32 devices in a mesh: grp: 2 (over y), ep: 4 (over z), tp: 4 (over x, core).
Axes of the slice: x: 2, y: 2, z: 4, core: 2. Of those that a mesh axis runs over, the one named last changes fastest.
Arguments:
- mixer_tokens: bfloat16 [4096, 2048], P(('grp', 'ep', 'tp')), parts along dimension 0, may hold values from -6 to 6
- mixer_gain: bfloat16 [2048], replicated, may hold values from 0.099609375 to 1.8984375
- in_weight: bfloat16 [2048, 2048], P(None, 'tp'), may hold values from -0.125 to 0.125
- group_weight: bfloat16 [4, 512, 512], P('tp'), may hold values from -0.25 to 0.25
- channel_scale: bfloat16 [2048], P('tp'), may hold values from 0.099609375 to 1.8984375
- out_weight: bfloat16 [2048, 2048], P('tp'), may hold values from -0.125 to 0.125
- expert_tokens: bfloat16 [4096, 2048], P(('grp', 'ep', 'tp')), parts along dimension 0, may hold values from -6 to 6
- expert_gain: bfloat16 [2048], replicated, may hold values from 0.099609375 to 1.8984375
- route_ids: int32 [4096, 2], P(('grp', 'ep', 'tp')), parts along dimension 0, may hold values from 0 to 3, all different within a row; in each aligned block of 128 rows (0 to 127, 128 to 255, ...) at most 128 rows name the same one
- route_weights: float32 [4096, 2], P(('grp', 'ep', 'tp')), parts along dimension 0, may hold values from 0.1 to 1
- gate_weight: bfloat16 [4, 2048, 1024], P('ep', None, 'tp'), may hold values from -0.125 to 0.125
- up_weight: bfloat16 [4, 2048, 1024], P('ep', None, 'tp'), may hold values from -0.125 to 0.125
- down_weight: bfloat16 [4, 1024, 2048], P('ep', 'tp'), may hold values from -0.1875 to 0.1875
Outputs:
- mixed_tokens: bfloat16 [4096, 2048], P(('grp', 'ep', 'tp')), parts along dimension 0
- expert_mix: bfloat16 [4096, 2048], P(('grp', 'ep', 'tp')), parts along dimension 0
The draws below stay inside these ranges and needn't reach their ends.
There are 2 independent parts, one for each index of `grp`. The reference program is written for one: setup_inputs(seed, part) draws one part's arguments, and reference() takes and returns one part's arrays. A program takes and returns all parts, laid end to end along the dimension named above; an argument that names none is the same for every part. Nothing has to cross between parts.
Inputs may be any that keep to these rules, and one draw needn't show every extreme that they name: `route_ids`: each row names 2 different experts; in the rows of one device no expert is named more than 128 times, and one expert exactly 128 times in the rows of some device.
All inputs are finite; a program needn't handle non-finite values.
Results may differ from the reference program's by a relative error of at most 0.015.
Values may be sent and summed in bfloat16 or wider, within the bound.
A program may use at most 128 MiB of HBM per device.

```python
import math
import jax
import jax.numpy as jnp
import numpy as np
from jax import lax

D = 2048
GROUPS = 4
GW = 512
FF = 1024
FF_DEV = 256
TOP = 2
TOK_DEV = 128
TOKENS = 2048
EXPERTS = 4
CAP = 128
N_EP = 4
N_TP = 4


def block_levels(key, dims, split, least, high):
    def one(position, shards_of):
        heights = jax.random.uniform(jax.random.fold_in(jax.random.fold_in(key, 6), position), (shards_of,), jnp.float32, least / len(split), high / len(split))
        return jnp.repeat(jnp.exp(heights), dims[position] // shards_of).reshape((-1,) + (1,) * (len(dims) - position - 1))

    level = one(*split[0])
    for cut in split[1:]:
        level = level * one(*cut)
    return level


def routed_block(own_key, own, number, rows, number_of, top, bound, lean):
    order = jax.random.permutation(own_key, number_of)
    heavy_load, ordinary = portions_of(number_of, rows * top, bound, lean, True), portions_of(number_of, rows * top, bound, lean, False)
    places = jnp.arange(number_of)

    def named(lengths, rotation):
        used = int((lengths > 0).sum())
        fixed = max(1, used // 4)
        moved = fixed + (places - fixed + rotation * (used - fixed)) % max(1, number_of - fixed)
        return jnp.zeros((number_of,), jnp.int32).at[order[jnp.where(places < fixed, places, moved)]].set(jnp.asarray(lengths, jnp.int32))

    lengths = jnp.where(number % 4 == 0, named(heavy_load, number // 4), named(ordinary, number - number // 4 - 1))
    mixed = jax.random.permutation(jax.random.fold_in(own, 3), number_of)
    source_of, taker = mixed[0:number_of // 2 * 2:2], mixed[1:number_of // 2 * 2:2]
    room = jnp.minimum(lengths[source_of] - 1, bound - lengths[taker]) // 2
    room = jnp.where((source_of == order[0]) | (taker == order[0]) | (lengths[taker] == 0), 0, jnp.maximum(room, 0))
    moved = jax.random.randint(jax.random.fold_in(own, 4), (number_of // 2,), 0, 1 << 20) % (room + 1)
    lengths = lengths.at[source_of].add(-moved).at[taker].add(moved)
    labels = jnp.searchsorted(jnp.cumsum(lengths), jnp.arange(rows * top), side="right").astype(jnp.int32)
    listing = labels.reshape(top, rows).T
    listing = listing[jax.random.permutation(jax.random.fold_in(own, 1), rows)]
    rotation = jax.random.randint(jax.random.fold_in(own, 2), (rows, 1), 0, top)
    return jnp.take_along_axis(listing, (jnp.arange(top)[None, :] + rotation) % top, axis=1)


def portions_of(number_of, total, most, lean, full):
    loads = [(1 << 20) // math.isqrt(rank ** lean) + 1 for rank in range(1, number_of + 1)]
    largest = most if full else min(most, max(-(-total // number_of), total * loads[0] // sum(loads)))
    least = 1 if total - largest >= number_of - 1 else 0
    holding, spare = [largest] + [least] * (number_of - 1), total - largest - least * (number_of - 1)
    while spare > 0:
        free = [i for i in range(1, number_of) if holding[i] < largest] or [i for i in range(1, number_of) if holding[i] < most]
        pool, budget = sum([loads[i] for i in free]), spare
        for i in free:
            more = min(most - holding[i], max(1, budget * loads[i] // pool), spare)
            holding[i] = holding[i] + more
            spare = spare - more
    return np.array(holding)


def bell_draw(key, shape, scale, bound, split=(), kind=jnp.bfloat16):
    entries = jax.random.normal(key, shape, jnp.float32) * scale
    if len(split) > 0:
        entries = block_levels(key, shape, split, -0.22, 0.18) * entries
    return jnp.clip(entries, min=-bound, max=bound).astype(kind)


def setup_inputs(seed: int = 0, part: int = 0) -> dict:
    splits = jax.random.split(jax.random.key(seed), 14)
    part_keys = jax.random.split(jax.random.fold_in(splits[13], part), 14)
    mixer_tokens = bell_draw(part_keys[0], (TOKENS, D), 1.0, 6.0, ((0, 16),))
    mixer_gain = jnp.clip(1.0 + 0.18 * jax.random.normal(splits[1], (D,), jnp.float32), 0.099609375, 1.8984375).astype(jnp.bfloat16)
    in_weight = bell_draw(splits[2], (D, D), D ** -0.5, 0.125, ((1, 4),))
    group_weight = bell_draw(splits[3], (GROUPS, GW, GW), GW ** -0.5, 0.25, ((0, 4),))
    channel_scale = jnp.clip(1.0 + 0.18 * jax.random.normal(splits[4], (D,), jnp.float32), 0.099609375, 1.8984375).astype(jnp.bfloat16)
    out_weight = bell_draw(splits[5], (D, D), D ** -0.5, 0.125, ((0, 4),))
    expert_tokens = bell_draw(part_keys[6], (TOKENS, D), 1.0, 6.0, ((0, 16),))
    expert_gain = jnp.clip(1.0 + 0.18 * jax.random.normal(splits[7], (D,), jnp.float32), 0.099609375, 1.8984375).astype(jnp.bfloat16)
    route_ids_keys = jax.random.split(jax.random.fold_in(part_keys[8], 1), TOKENS // TOK_DEV)
    route_ids_turns = jax.random.permutation(jax.random.fold_in(part_keys[8], 3), TOKENS // TOK_DEV)
    route_ids = jax.vmap(lambda own, number: routed_block(jax.random.fold_in(part_keys[8], 2), own, number, TOK_DEV, EXPERTS, TOP, CAP, 2))(route_ids_keys, route_ids_turns).reshape((TOKENS, TOP))
    route_weights = jnp.clip(jnp.exp(math.log(1.0) - 2.3025851 * jax.random.uniform(part_keys[9], (TOKENS, TOP), jnp.float32) ** block_levels(part_keys[9], (TOKENS, TOP), ((0, 16),), -0.2, 0.2)), 0.1, 1.0)
    gate_weight = bell_draw(splits[10], (EXPERTS, D, FF), D ** -0.5, 0.125, ((0, 4), (2, 4)))
    up_weight = bell_draw(splits[11], (EXPERTS, D, FF), D ** -0.5, 0.125, ((0, 4), (2, 4)))
    down_weight = bell_draw(splits[12], (EXPERTS, FF, D), FF ** -0.5, 0.1875, ((0, 4), (1, 4)))
    return dict(mixer_tokens=mixer_tokens, mixer_gain=mixer_gain, in_weight=in_weight, group_weight=group_weight, channel_scale=channel_scale, out_weight=out_weight, expert_tokens=expert_tokens, expert_gain=expert_gain, route_ids=route_ids, route_weights=route_weights, gate_weight=gate_weight, up_weight=up_weight, down_weight=down_weight)


def rms_rows(rows, gain):
    values = rows.astype(jnp.float32)
    scaled = values * lax.rsqrt(lax.optimization_barrier(jnp.mean(values * values, axis=-1, keepdims=True)) + 1e-06)
    return (scaled * gain.astype(jnp.float32)).astype(jnp.bfloat16)

def expert_hidden(rows, w_gate, w_up):
    gate = jnp.dot(rows, w_gate, preferred_element_type=jnp.float32)
    upper = jnp.dot(rows, w_up, preferred_element_type=jnp.float32)
    return (jax.nn.silu(gate) * upper).astype(jnp.bfloat16)

def reference(mixer_tokens, mixer_gain, in_weight, group_weight, channel_scale, out_weight, expert_tokens, expert_gain, route_ids, route_weights, gate_weight, up_weight, down_weight):
    normed = rms_rows(mixer_tokens, mixer_gain)
    pooled_in = jnp.dot(normed, in_weight, preferred_element_type=jnp.float32).astype(jnp.bfloat16)
    values = pooled_in.astype(jnp.float32)
    length = values.shape[0]
    prefix = jnp.concatenate([jnp.zeros((1, D), jnp.float32), jnp.cumsum(values, axis=0)], axis=0)
    mixed = jnp.zeros((length, D), jnp.float32)
    for group in range(GROUPS):
        window = 2 ** (group + 1)
        low_col = group * GW
        upper = prefix[1:, low_col:low_col + GW]
        lower = jnp.concatenate([jnp.zeros((window - 1, GW), jnp.float32), prefix[:length - window + 1, low_col:low_col + GW]], axis=0)
        counts = jnp.minimum(jnp.arange(1, length + 1), window).astype(jnp.float32)
        trail = ((upper - lower) / counts[:, None] - values[:, low_col:low_col + GW]).astype(jnp.bfloat16)
        grouped = (jnp.dot(trail, group_weight[group], preferred_element_type=jnp.float32) * channel_scale[low_col:low_col + GW].astype(jnp.float32)).astype(jnp.bfloat16)
        partial_value = jnp.dot(grouped, out_weight[low_col:low_col + GW, :], preferred_element_type=jnp.float32)
        partial_value = lax.optimization_barrier(partial_value.astype(jnp.bfloat16))
        mixed = mixed + partial_value.astype(jnp.float32)
    mixed_tokens = mixed.astype(jnp.bfloat16)
    expert_in = rms_rows(expert_tokens, expert_gain)
    weights = route_weights.astype(jnp.float32)
    shares = weights / lax.optimization_barrier(jnp.sum(weights, axis=1, keepdims=True))
    count_tok = expert_in.shape[0]
    flat_ids = route_ids.reshape(count_tok * TOP).astype(jnp.int32)
    flat_tokens = jnp.concatenate([(jnp.arange(count_tok * TOP) // TOP).astype(jnp.int32), jnp.full((1,), count_tok, jnp.int32)])
    flat_shares = jnp.concatenate([shares.reshape(count_tok * TOP), jnp.zeros((1,), jnp.float32)])
    padded = jnp.concatenate([expert_in, jnp.zeros((1, D), jnp.bfloat16)], axis=0)
    most = N_EP * N_TP * CAP

    def one_expert(total, expert):
        chosen = jnp.nonzero(flat_ids == expert, size=most, fill_value=count_tok * TOP)[0].astype(jnp.int32)
        token_of = flat_tokens[chosen]
        rows = padded[token_of]
        hidden = expert_hidden(rows, gate_weight[expert], up_weight[expert])
        result = jnp.zeros((most, D), jnp.float32)
        for block in range(N_TP):
            part = jnp.dot(hidden[:, block * FF_DEV:(block + 1) * FF_DEV], down_weight[expert][block * FF_DEV:(block + 1) * FF_DEV, :], preferred_element_type=jnp.float32)
            part = lax.optimization_barrier(part.astype(jnp.bfloat16))
            result = result + part.astype(jnp.float32)
        total = total.at[token_of].add(result * flat_shares[chosen][:, None])
        return (total, None)
    total, _ = lax.scan(one_expert, jnp.zeros((count_tok + 1, D), jnp.float32), jnp.arange(EXPERTS).astype(jnp.int32))
    expert_mix = total[:count_tok].astype(jnp.bfloat16)
    return (mixed_tokens, expert_mix)
```

```python
import jax
import jax.numpy as jnp
from jax import lax
from jax.experimental import pallas as pl
from jax.experimental.pallas import tpu as pltpu
from jax.sharding import PartitionSpec as P

WINDOW_MAX = 16


def shifted(value, axis, by):
    devices = lax.axis_size(axis)
    pairs = [(i, i + by) for i in range(devices) if 0 <= i + by < devices]
    return lax.ppermute(value, axis, pairs)


def turned(value, axis, by):
    devices = lax.axis_size(axis)
    if by % devices == 0:
        return value
    return lax.ppermute(value, axis, [(i, (i + by) % devices) for i in range(devices)])


def rms_rows(rows, gain):
    values = rows.astype(jnp.float32)
    scaled = values * lax.rsqrt(jnp.mean(values * values, axis=-1, keepdims=True) + 1e-06)
    return (scaled * gain.astype(jnp.float32)).astype(jnp.bfloat16)


def expert_hidden(rows, w_gate, w_up):
    gate = jnp.dot(rows, w_gate, preferred_element_type=jnp.float32)
    upper = jnp.dot(rows, w_up, preferred_element_type=jnp.float32)
    return (jax.nn.silu(gate) * upper).astype(jnp.bfloat16)


def local(
    mixer_tokens,
    mixer_gain,
    in_weight,
    group_weight,
    channel_scale,
    out_weight,
    expert_tokens,
    expert_gain,
    route_ids,
    route_weights,
    gate_weight,
    up_weight,
    down_weight,
):
    normed = rms_rows(mixer_tokens, mixer_gain)
    expert_in = rms_rows(expert_tokens, expert_gain)
    shares = route_weights / jnp.sum(route_weights, axis=1, keepdims=True)
    rows_here, top_k = route_ids.shape
    width = expert_in.shape[1]
    n_experts = lax.axis_size("ep") * gate_weight.shape[0]
    capacity = 4 * rows_here // n_experts
    dense = capacity >= rows_here
    parts_tp = lax.axis_size("tp")
    if dense:
        both = lax.all_gather(jnp.concatenate([normed, expert_in], axis=0), "tp", axis=0, tiled=True)
        both = both.reshape(parts_tp, 2, rows_here, width)
        every = both[:, 0].reshape(parts_tp * rows_here, width)
        own = both[:, 1].reshape(parts_tp * rows_here, width)
    else:
        every = lax.all_gather(normed, "tp", axis=0, tiled=True)
    pooled_in = jnp.dot(
        every,
        in_weight,
        preferred_element_type=jnp.float32,
    ).astype(jnp.bfloat16)
    block_rows = pooled_in.shape[0]
    rim_rows = shifted(pooled_in[block_rows - WINDOW_MAX :], "ep", 1)
    values = pooled_in.astype(jnp.float32)
    extended = jnp.concatenate([rim_rows.astype(jnp.float32), values], axis=0)
    window = jnp.left_shift(jnp.int32(2), lax.axis_index("tp"))
    sums = extended
    span = 1
    total = jnp.zeros_like(values)
    for level in range(WINDOW_MAX.bit_length() - 1):
        sums = sums[span:] + sums[:-span]
        span = span * 2
        total = total + jnp.where(window == span, sums[sums.shape[0] - block_rows :], 0.0)
    positions = lax.axis_index("ep") * block_rows + lax.iota(jnp.int32, block_rows) + 1
    counts = jnp.minimum(positions, window).astype(jnp.float32)
    pooled = (total / counts[:, None] - values).astype(jnp.bfloat16)
    grouped = (
        jnp.dot(pooled, group_weight[0], preferred_element_type=jnp.float32)
        * channel_scale.astype(jnp.float32)
    ).astype(jnp.bfloat16)
    mixed_part = jnp.dot(grouped, out_weight, preferred_element_type=jnp.float32).astype(
        jnp.bfloat16
    )
    if dense:
        experts = jnp.arange(n_experts, dtype=jnp.int32)
        named = (route_ids[:, :, None] == experts[None, None, :]).astype(jnp.float32)
        coefs = jnp.sum(named * shares[:, :, None], axis=1)
        coefs = lax.all_gather(coefs, ("ep", "tp"), axis=0, tiled=True)
        blocks = lax.axis_size("ep")
        here = lax.axis_index("ep")
        mine = (experts == here).astype(jnp.float32)
        coef = jnp.sum(coefs * mine[None, :], axis=1).reshape(blocks, parts_tp, rows_here)
        order = list(range(1, blocks))

        def scale_of(k):
            return lax.dynamic_index_in_dim(coef, lax.rem(here - k + blocks, blocks), 0, False)

        def expert_part(rows, scale):
            hidden = expert_hidden(rows, gate_weight[0], up_weight[0])
            part = jnp.dot(hidden, down_weight[0], preferred_element_type=jnp.float32)
            return (part * scale.reshape(-1)[:, None]).astype(jnp.bfloat16)

        moved = jnp.concatenate([turned(expert_in, "ep", k) for k in order], axis=0)
        moved, own = lax.optimization_barrier((moved, own))
        own_part = expert_part(own, scale_of(0))
        others = lax.all_gather(moved, "tp", axis=0, tiled=True)
        part = expert_part(others, jnp.stack([scale_of(k) for k in order], axis=1))
        back = lax.psum_scatter(part, "tp", scatter_dimension=0, tiled=True)
        back = back.reshape(blocks - 1, rows_here, width)
        pair = jnp.stack(
            [value.reshape(parts_tp, rows_here, width) for value in (mixed_part, own_part)], axis=1
        ).reshape(2 * parts_tp * rows_here, width)
        pair = lax.psum_scatter(pair, "tp", scatter_dimension=0, tiled=True)
        total = pair[rows_here:].astype(jnp.float32)
        for i, k in enumerate(order):
            total = total + turned(back[i], "ep", -k).astype(jnp.float32)
        return (pair[:rows_here], total.astype(jnp.bfloat16))
    mixed_tokens = lax.psum_scatter(mixed_part, "tp", scatter_dimension=0, tiled=True)
    flat_ids = route_ids.reshape(rows_here * top_k)
    one_hot = (flat_ids[:, None] == jnp.arange(n_experts, dtype=jnp.int32)[None, :]).astype(
        jnp.int32
    )
    before = jnp.cumsum(one_hot, axis=0) - one_hot
    slots = jnp.sum(before * one_hot, axis=1)
    targets = flat_ids * capacity + slots
    placement = (
        targets.reshape(rows_here, top_k)[None, :, :]
        == jnp.arange(n_experts * capacity, dtype=jnp.int32)[:, None, None]
    )
    dispatch = jnp.any(placement, axis=2).astype(jnp.bfloat16)
    outgoing = jnp.dot(dispatch, expert_in, preferred_element_type=jnp.float32).astype(jnp.bfloat16)
    outgoing = outgoing.reshape(n_experts, capacity, width)
    arrived = lax.all_to_all(outgoing, "ep", split_axis=0, concat_axis=0, tiled=True)
    sources, held, _ = arrived.shape
    flat = arrived.reshape(sources * held, width)
    hidden = expert_hidden(
        lax.all_gather(flat, "tp", axis=0, tiled=True), gate_weight[0], up_weight[0]
    )
    rows = hidden
    summed = lax.psum_scatter(
        jnp.dot(rows, down_weight[0], preferred_element_type=jnp.float32).astype(jnp.bfloat16),
        "tp",
        scatter_dimension=0,
        tiled=True,
    ).astype(jnp.float32)
    expert_out = lax.all_to_all(
        summed.reshape(sources, held, width).astype(jnp.bfloat16),
        "ep",
        split_axis=0,
        concat_axis=0,
        tiled=True,
    ).astype(jnp.float32)
    flat_out = expert_out.reshape(n_experts * capacity, width)
    picked = jnp.take(flat_out, targets, axis=0).reshape(rows_here, top_k, width)
    expert_mix = jnp.sum(picked * shares[:, :, None], axis=1).astype(jnp.bfloat16)
    return (mixed_tokens, expert_mix)


MESH = pl.DeviceIdType.MESH
PIECES_GU = 8
PIECES_D = 4
PIECES = PIECES_GU + PIECES_D
WINDOW = 4
HALVES = 2


def fused_kernel(
    mixer_tokens,
    mixer_gain,
    in_weight,
    group_weight,
    channel_scale,
    out_weight,
    expert_tokens,
    expert_gain,
    route_ids,
    route_weights,
    gate_weight,
    up_weight,
    down_weight,
    mixed_out,
    expert_out,
    mix_raw,
    exp_raw,
    w_in,
    w_group,
    w_out,
    w_gu,
    w_d,
    tokens,
    coefs,
    scales,
    hid,
    acc,
    rs_in,
    rs_stage,
    mix_all,
    pooled_in,
    mix_part,
    mix_pair,
    mix_stage,
    mix_far,
    load_sem,
    x_send,
    x_recv,
    y_send,
    y_recv,
    own_send,
    own_recv,
    fx_send,
    fx_recv,
    fy_send,
    fy_recv,
    ag_send,
    ag_recv,
    coef_send,
    coef_recv,
    rs_send,
    rs_recv,
    mix_send,
    mix_recv,
):
    f32, bf16 = jnp.float32, jnp.bfloat16
    rows, width = exp_raw.shape
    half_rows = rows // HALVES
    group_width = w_group.shape[0]
    ff_half = w_d.shape[1] // 2
    blocks = tokens.shape[0]
    g = lax.axis_index("grp")
    e = lax.axis_index("ep")
    t = lax.axis_index("tp")
    x = t // 2
    c = t % 2
    t_c = 2 * x + 1 - c
    t_x = 2 * (1 - x) + c
    t_d = 2 * (1 - x) + 1 - c
    dev_c, dev_x, dev_y = (g, e, t_c), (g, e, t_x), (1 - g, e, t)
    hi = e // 2
    sign = 1 - 2 * hi
    last = blocks - 1

    def mirror(m):
        return hi * last + sign * m

    u = mirror(e)
    end = u == 0
    mid = u == 1
    far = (g, lax.rem(e + sign + blocks, blocks), t)
    near = (g, lax.rem(e - sign + blocks, blocks), t)
    third = mirror(1 - u)

    def rc(src, dst, send, recv, dev):
        return pltpu.make_async_remote_copy(
            src_ref=src, dst_ref=dst, send_sem=send, recv_sem=recv, device_id=dev, device_id_type=MESH
        )

    def loads():
        out = []
        for h in range(2):
            hh = g if h == 0 else 1 - g
            lane = pl.multiple_of(hh * ff_half, ff_half)
            out.append((gate_weight.at[0, :, pl.ds(lane, ff_half)], w_gu.at[t, hh, :, pl.ds(0, ff_half)]))
            out.append((up_weight.at[0, :, pl.ds(lane, ff_half)], w_gu.at[t, hh, :, pl.ds(ff_half, ff_half)]))
        out.append((expert_tokens, exp_raw))
        out.append((down_weight.at[0], w_d.at[t]))
        out.append((mixer_tokens, mix_raw))
        out.append((in_weight, w_in))
        out.append((group_weight.at[0], w_group))
        out.append((out_weight, w_out))
        return [pltpu.make_async_copy(a, b, load_sem.at[i]) for i, (a, b) in enumerate(out)]

    local = loads()
    for copy in local:
        copy.start()
    pooled_in[pl.ds(0, rows), :] = jnp.zeros((rows, group_width), bf16)

    barrier = pltpu.get_barrier_semaphore()
    greet = [dev_c, dev_x, dev_y] + [(g, lax.rem(e + k, blocks), t) for k in range(1, blocks)]
    for dev in greet:
        pl.semaphore_signal(barrier, inc=1, device_id=dev, device_id_type=MESH)
    pl.semaphore_wait(barrier, len(greet))

    def piece(q, h, s):
        if s < PIECES_GU:
            n = width // PIECES_GU
            return w_gu.at[q, h, pl.ds(s * n, n), :]
        n = ff_half // PIECES_D
        start = pl.multiple_of(h * ff_half + (s - PIECES_GU) * n, n)
        return w_d.at[q, pl.ds(start, n), :]

    def send_x(s):
        p = piece(t, g, s)
        return rc(p, p, x_send.at[s], x_recv.at[s], dev_x)

    def got_x(s):
        p = piece(t_x, g, s)
        return rc(p, p, x_send.at[s], x_recv.at[s], dev_x)

    def send_y(s):
        p = piece(t_x, g, s)
        return rc(p, p, y_send.at[s], y_recv.at[s], dev_y)

    def got_y(s):
        p = piece(t_x, 1 - g, s)
        return rc(p, p, y_send.at[s], y_recv.at[s], dev_y)

    def send_fx(s):
        p = piece(t_x, g, s)
        return rc(p, p, fx_send.at[s], fx_recv.at[s], dev_c)

    def got_fx(s):
        p = piece(t_d, g, s)
        return rc(p, p, fx_send.at[s], fx_recv.at[s], dev_c)

    def send_fy(s):
        p = piece(t_x, 1 - g, s)
        return rc(p, p, fy_send.at[s], fy_recv.at[s], dev_c)

    def got_fy(s):
        p = piece(t_d, 1 - g, s)
        return rc(p, p, fy_send.at[s], fy_recv.at[s], dev_c)

    def own_gu(q):
        return rc(w_gu.at[q], w_gu.at[q], own_send.at[0], own_recv.at[0], dev_c)

    def own_d(q):
        return rc(w_d.at[q], w_d.at[q], own_send.at[1], own_recv.at[1], dev_c)

    def norm(raw, gain, dst, start, count):
        step = 16

        @pl.loop(0, count // step)
        def _(i):
            at = pl.ds(pl.multiple_of(start + i * step, step), step)
            values = raw[at, :].astype(f32)
            scaled = values * lax.rsqrt(jnp.mean(values * values, axis=-1, keepdims=True) + 1e-06)
            dst[at, :] = (scaled * gain[...].astype(f32)).astype(bf16)

    def chunk(home, j):
        return tokens.at[home, pl.ds(j * half_rows, half_rows), :]

    def ag_far(home, j, f):
        p = chunk(home, j)
        return rc(p, p, ag_send.at[f], ag_recv.at[f + 6 * (1 - u)], far)

    def ag_near(home, j, f):
        p = chunk(home, j)
        return rc(p, p, ag_send.at[4 + f], ag_recv.at[f], near)

    def ag_got(home, j, f):
        p = chunk(home, j)
        return rc(p, p, ag_send.at[0], ag_recv.at[f], far)

    local[0].wait()
    local[1].wait()
    for s in range(WINDOW):
        send_x(s).start()
    local[4].wait()
    for j in range(HALVES):
        norm(exp_raw, expert_gain, tokens.at[e], j * half_rows, half_rows)
        ag_far(e, j, j).start()

        @pl.when(mid)
        def _():
            ag_near(e, j, j).start()

    local[2].wait()
    local[3].wait()
    own_gu(t).start()
    local[5].wait()
    own_d(t).start()

    ids = route_ids[...]
    weights = route_weights[...]
    shares = weights / jnp.sum(weights, axis=1, keepdims=True)
    lanes = lax.broadcasted_iota(jnp.int32, (rows, rows), 1)
    coef = jnp.zeros((rows, rows), f32)
    for k in range(ids.shape[1]):
        coef = coef + jnp.where(ids[:, k : k + 1] == lanes, shares[:, k : k + 1], 0.0)
    coefs[e] = jnp.transpose(coef)[: coefs.shape[1], :]

    def coef_to(k):
        dev = (g, lax.rem(e + k, blocks), t)
        return rc(coefs.at[e], coefs.at[e], coef_send.at[k - 1], coef_recv.at[k - 1], dev)

    def coef_got(k):
        home = lax.rem(e - k + blocks, blocks)
        return rc(coefs.at[home], coefs.at[home], coef_send.at[k - 1], coef_recv.at[k - 1], dev_c)

    for k in range(1, blocks):
        coef_to(k).start()

    local[6].wait()
    norm(mix_raw, mixer_gain, mix_all.at[t], 0, rows)

    def mix_x(q, j):
        p = mix_all.at[q, pl.ds(j * half_rows, half_rows), :]
        return rc(p, p, mix_send.at[j], mix_recv.at[j], dev_x)

    def mix_fwd(q, j):
        p = mix_all.at[q, pl.ds(j * half_rows, half_rows), :]
        return rc(p, p, mix_send.at[2 + j], mix_recv.at[2 + j], dev_c)

    def mix_own(q):
        return rc(mix_all.at[q], mix_all.at[q], mix_send.at[4], mix_recv.at[4], dev_c)

    mix_own(t).start()

    def hidden(home, xq):
        @pl.loop(0, 4)
        def _(j):
            q = 2 * xq + j // 2
            h = j % 2
            both = jnp.dot(tokens[home], w_gu[q, h], preferred_element_type=f32)
            gate, upper = both[:, :ff_half], both[:, ff_half:]
            value = gate / (1.0 + jnp.exp(-gate)) * upper
            hid[home, xq, :, pl.ds(pl.multiple_of(j * ff_half, ff_half), ff_half)] = value.astype(bf16)

    col = 512

    def down(home, xq, first):
        @pl.loop(0, width // col)
        def _(n):
            at = pl.ds(pl.multiple_of(n * col, col), col)
            w = w_d[pl.ds(2 * xq, 2), :, at].reshape(4 * ff_half, col)
            part = jnp.dot(hid[home, xq], w, preferred_element_type=f32)
            if first:
                acc[home, :, at] = part
            else:
                scale = scales[home][:, :1]
                acc[home, :, at] = (acc[home, :, at] + part) * scale

    def pool_in(xq):
        @pl.loop(0, 2)
        def _(j):
            q = 2 * xq + j
            value = jnp.dot(mix_all[q], w_in[...], preferred_element_type=f32)
            pooled_in[pl.ds(pl.multiple_of(rows * (q + 1), rows), rows), :] = value.astype(bf16)

    def wait_fgu():
        for s in range(PIECES_GU):
            got_fx(s).wait_recv()
            got_fy(s).wait_recv()

    for s in range(PIECES):
        got_x(s).wait_recv()
        send_y(s).start()
        send_fx(s).start()
        if s + WINDOW < PIECES:
            send_x(s + WINDOW).start()
        elif s + WINDOW < PIECES + HALVES:
            mix_x(t, s + WINDOW - PIECES).start()
        if s >= 1:
            got_y(s - 1).wait_recv()
            send_fy(s - 1).start()
        if s % 2 == 1:
            f = s // 2

            @pl.when(end)
            def _():
                ag_got(mirror(1 + f // 2), f % 2, f).wait_recv()

            if f < 4:

                @pl.when(mid)
                def _():
                    home = mirror(2 + f // 2)
                    ag_got(home, f % 2, f).wait_recv()
                    ag_near(home, f % 2, f + 2).start()

            if f < 2:

                @pl.when(mid)
                def _():
                    home = mirror(0)
                    ag_got(home, f % 2, 6 + f).wait_recv()
                    ag_far(home, f % 2, 2 + f).start()

        if s == 1:
            for k in range(1, blocks):
                coef_got(k).wait_recv()
            for home in range(blocks):
                row = coefs[home, pl.ds(e, 1), :]
                scales[home] = jnp.transpose(jnp.broadcast_to(row, (rows, rows)))
        if s == 2:
            own_gu(t_c).wait_recv()
            own_d(t_c).wait_recv()
            hidden(e, x)
        if s == 3:
            down(e, x, True)
        if s == 4:
            hidden(third, x)
        if s == 5:
            down(third, x, True)
        if s == 6:
            mix_own(t_c).wait_recv()
            local[7].wait()
            pool_in(x)
        if s == 8:
            hidden(mirror(2), x)
            down(mirror(2), x, True)
        if s == 9:
            wait_fgu()
            hidden(mirror(2), 1 - x)
        if s == 10:
            hidden(third, 1 - x)
            hidden(e, 1 - x)

    got_y(PIECES - 1).wait_recv()
    send_fy(PIECES - 1).start()
    hidden(mirror(3), x)
    for s in range(PIECES_GU, PIECES):
        got_fx(s).wait_recv()
        got_fy(s).wait_recv()

    def rs_far(k):
        p = rs_stage.at[k]
        return rc(p, rs_in.at[k + 6 * u], rs_send.at[k], rs_recv.at[k + 6 * u], far)

    def rs_near(k):
        p = rs_stage.at[4 + k]
        return rc(p, rs_in.at[6 + k], rs_send.at[4 + k], rs_recv.at[6 + k], near)

    def rs_got(k):
        return rc(rs_in.at[k], rs_in.at[k], rs_send.at[0], rs_recv.at[k], far)

    def first_send(home, k):
        @pl.when(end)
        def _():
            for j in range(HALVES):
                at = pl.ds(j * half_rows, half_rows)
                rs_stage[k + j] = acc[home, at, :].astype(bf16)
                rs_far(k + j).start()

    def lead(k):
        @pl.when(mid)
        def _():
            rs_got(k).wait_recv()
            if k < 4:
                at = pl.ds((k % 2) * half_rows, half_rows)
                rs_stage[k] = (acc[mirror(2 + k // 2), at, :] + rs_in[k].astype(f32)).astype(bf16)
                rs_far(k).start()

    def lag(k):
        @pl.when(mid)
        def _():
            rs_got(6 + k).wait_recv()
            if k >= 2:
                at = pl.ds((k % 2) * half_rows, half_rows)
                rs_stage[4 + k - 2] = (acc[mirror(0), at, :] + rs_in[6 + k].astype(f32)).astype(bf16)
                rs_near(k - 2).start()

    down(mirror(2), 1 - x, False)
    first_send(mirror(2), 0)
    hidden(mirror(3), 1 - x)
    down(mirror(3), x, True)
    down(mirror(3), 1 - x, False)
    first_send(mirror(3), 2)
    down(third, 1 - x, False)
    first_send(third, 4)
    down(e, 1 - x, False)

    for j in range(HALVES):
        mix_x(t_x, j).wait_recv()
        mix_fwd(t_x, j).start()
    lead(0)

    def rim_to():
        return rc(
            pooled_in.at[pl.ds(rows * (blocks + 1) - 16, 16), :],
            pooled_in.at[pl.ds(rows - 16, 16), :],
            mix_send.at[5],
            mix_recv.at[5],
            (g, lax.rem(e + 1, blocks), t),
        )

    for j in range(HALVES):
        mix_fwd(t_d, j).wait_recv()
    pool_in(1 - x)

    @pl.when(e < last)
    def _():
        rim_to().start()

    lead(1)

    @pl.when(e > 0)
    def _():
        rim_to().wait_recv()

    local[8].wait()
    local[9].wait()
    window = 2 + 2 * jnp.minimum(t, 1) + 4 * (t // 2) + 8 * (t // 3)

    def mix_down(j):
        q = (2 * (1 - x) if j < 2 else 2 * x) + (1 - c if j % 2 == 0 else c)
        start = pl.multiple_of(q * rows, rows)
        seg = pooled_in[pl.ds(start, 2 * rows), :]
        i = lax.broadcasted_iota(jnp.int32, (rows, 2 * rows), 0) + rows
        k = lax.broadcasted_iota(jnp.int32, (rows, 2 * rows), 1)
        band = jnp.where((k <= i) & (k > i - window), 1.0, 0.0).astype(bf16)
        sums = jnp.dot(band, seg, preferred_element_type=f32)
        place = lax.broadcasted_iota(jnp.int32, (rows, 1), 0) + (e * blocks + q) * rows + 1
        counts = jnp.minimum(place, window).astype(f32)
        pooled = (sums / counts - seg[rows:, :].astype(f32)).astype(bf16)
        grouped = jnp.dot(pooled, w_group[...], preferred_element_type=f32)
        grouped = (grouped * channel_scale[...].astype(f32)).astype(bf16)

        @pl.loop(0, width // col)
        def _(n):
            at = pl.ds(pl.multiple_of(n * col, col), col)
            mix_part[j, :, at] = jnp.dot(grouped, w_out[:, at], preferred_element_type=f32).astype(bf16)

    def pair_to(j):
        return rc(mix_part.at[2 * j], mix_pair.at[j], mix_send.at[6 + j], mix_recv.at[6 + j], dev_c)

    def cross(j):
        at = pl.ds(j * half_rows, half_rows)
        return rc(mix_stage.at[at, :], mix_far.at[at, :], mix_send.at[8 + j], mix_recv.at[8 + j], dev_x)

    mix_down(0)
    pair_to(0).start()
    mix_down(1)
    pair_to(0).wait_recv()
    for j in range(HALVES):
        at = pl.ds(j * half_rows, half_rows)
        mix_stage[at, :] = (mix_part[1, at, :].astype(f32) + mix_pair[0, at, :].astype(f32)).astype(bf16)
        cross(j).start()
    lag(0)
    lead(2)
    mix_down(2)
    pair_to(1).start()
    mix_down(3)
    lag(1)
    lead(3)
    lag(2)
    lead(4)
    lag(3)
    pair_to(1).wait_recv()
    for j in range(HALVES):
        at = pl.ds(j * half_rows, half_rows)
        cross(j).wait_recv()
        mixed_out[at, :] = (
            mix_part[3, at, :].astype(f32) + mix_pair[1, at, :].astype(f32) + mix_far[at, :].astype(f32)
        ).astype(bf16)
    lead(5)
    for j in range(HALVES):
        at = pl.ds(j * half_rows, half_rows)

        @pl.when(mid)
        def _():
            expert_out[at, :] = (acc[e, at, :] + rs_in[4 + j].astype(f32) + rs_in[6 + j].astype(f32)).astype(bf16)

        @pl.when(end)
        def _():
            rs_got(6 + j).wait_recv()
            expert_out[at, :] = (acc[e, at, :] + rs_in[6 + j].astype(f32)).astype(bf16)

    for s in range(PIECES):
        send_x(s).wait_send()
        send_y(s).wait_send()
        send_fx(s).wait_send()
        send_fy(s).wait_send()
    own_gu(t).wait_send()
    own_d(t).wait_send()
    for k in range(1, blocks):
        coef_to(k).wait_send()
    for j in range(HALVES):
        ag_far(e, j, j).wait_send()
        mix_x(t, j).wait_send()
        mix_fwd(t_x, j).wait_send()
        pair_to(j).wait_send()
        cross(j).wait_send()
    mix_own(t).wait_send()

    @pl.when(e < last)
    def _():
        rim_to().wait_send()

    @pl.when(end)
    def _():
        for k in range(6):
            rs_far(k).wait_send()

    @pl.when(mid)
    def _():
        for f in range(6):
            ag_near(e, f % 2, f).wait_send()
        for f in range(2):
            ag_far(e, f, 2 + f).wait_send()
        for k in range(4):
            rs_far(k).wait_send()
        for k in range(2):
            rs_near(k).wait_send()


def fused(*args):
    (mixer_tokens, _, in_weight, group_weight, _, out_weight, _, _, route_ids, _, gate_weight, _, _) = args
    rows, width = mixer_tokens.shape
    group_width = in_weight.shape[1]
    ff = gate_weight.shape[2]
    blocks = lax.axis_size("ep")
    parts = lax.axis_size("tp")
    half = rows // HALVES
    bf16, f32 = jnp.bfloat16, jnp.float32
    vmem = pltpu.VMEM
    dma = pltpu.SemaphoreType.DMA
    anyspace = pl.BlockSpec(memory_space=pl.ANY)
    local_spec = pl.BlockSpec(memory_space=pltpu.VMEM)
    args = list(args)
    for i in (1, 4, 7):
        args[i] = args[i].reshape(1, -1)
    small = (1, 4, 7, 8, 9)
    scratch = [
        vmem((rows, width), bf16),
        vmem((rows, width), bf16),
        vmem((width, group_width), bf16),
        vmem((group_width, group_width), bf16),
        vmem((group_width, width), bf16),
        vmem((parts, 2, width, ff), bf16),
        vmem((parts, ff, width), bf16),
        vmem((blocks, rows, width), bf16),
        vmem((blocks, 8, rows), f32),
        vmem((blocks, rows, rows), f32),
        vmem((blocks, 2, rows, 2 * ff), bf16),
        vmem((blocks, rows, width), f32),
        vmem((10, half, width), bf16),
        vmem((6, half, width), bf16),
        vmem((parts, rows, width), bf16),
        vmem((rows * (parts + 1), group_width), bf16),
        vmem((parts, rows, width), bf16),
        vmem((2, rows, width), bf16),
        vmem((rows, width), bf16),
        vmem((rows, width), bf16),
        dma((10,)),
    ]
    for count in (PIECES, PIECES, PIECES, PIECES, 2, 2, PIECES, PIECES, PIECES, PIECES, 10, 8, 3, 3, 6, 10, 10, 10):
        scratch.append(dma((count,)))
    shape = jax.ShapeDtypeStruct((rows, width), bf16)
    return pl.pallas_call(
        fused_kernel,
        out_shape=(shape, shape),
        in_specs=[local_spec if i in small else anyspace for i in range(len(args))],
        out_specs=(local_spec, local_spec),
        scratch_shapes=scratch,
        compiler_params=pltpu.CompilerParams(
            collective_id=0, has_side_effects=True, vmem_limit_bytes=60 << 20
        ),
        name="fused",
    )(*args)


def fits(mesh):
    sizes = dict(mesh.shape)
    return sizes["grp"] == 2 and sizes["ep"] == 4 and sizes["tp"] == 4


def solution(mesh):
    placed = (
        P(("grp", "ep", "tp"), None),
        P(),
        P(None, "tp"),
        P("tp", None, None),
        P("tp"),
        P("tp", None),
        P(("grp", "ep", "tp"), None),
        P(),
        P(("grp", "ep", "tp"), None),
        P(("grp", "ep", "tp"), None),
        P("ep", None, "tp"),
        P("ep", None, "tp"),
        P("ep", "tp", None),
    )
    return jax.shard_map(
        fused if fits(mesh) else local,
        mesh=mesh,
        in_specs=placed,
        out_specs=(P(("grp", "ep", "tp"), None), P(("grp", "ep", "tp"), None)),
        check_vma=False,
    )
```

```python
import jax
import jax.numpy as jnp
from jax import lax
from jax.experimental import pallas as pl
from jax.experimental.pallas import tpu as pltpu
from jax.sharding import PartitionSpec as P

WINDOW_MAX = 16


def shifted(value, axis, by):
    devices = lax.axis_size(axis)
    pairs = [(i, i + by) for i in range(devices) if 0 <= i + by < devices]
    return lax.ppermute(value, axis, pairs)


def turned(value, axis, by):
    devices = lax.axis_size(axis)
    if by % devices == 0:
        return value
    return lax.ppermute(value, axis, [(i, (i + by) % devices) for i in range(devices)])


def rms_rows(rows, gain):
    values = rows.astype(jnp.float32)
    scaled = values * lax.rsqrt(jnp.mean(values * values, axis=-1, keepdims=True) + 1e-06)
    return (scaled * gain.astype(jnp.float32)).astype(jnp.bfloat16)


def expert_hidden(rows, w_gate, w_up):
    gate = jnp.dot(rows, w_gate, preferred_element_type=jnp.float32)
    upper = jnp.dot(rows, w_up, preferred_element_type=jnp.float32)
    return (jax.nn.silu(gate) * upper).astype(jnp.bfloat16)


def local(
    mixer_tokens,
    mixer_gain,
    in_weight,
    group_weight,
    channel_scale,
    out_weight,
    expert_tokens,
    expert_gain,
    route_ids,
    route_weights,
    gate_weight,
    up_weight,
    down_weight,
):
    normed = rms_rows(mixer_tokens, mixer_gain)
    expert_in = rms_rows(expert_tokens, expert_gain)
    shares = route_weights / jnp.sum(route_weights, axis=1, keepdims=True)
    rows_here, top_k = route_ids.shape
    width = expert_in.shape[1]
    n_experts = lax.axis_size("ep") * gate_weight.shape[0]
    capacity = 4 * rows_here // n_experts
    dense = capacity >= rows_here
    parts_tp = lax.axis_size("tp")
    if dense:
        both = lax.all_gather(jnp.concatenate([normed, expert_in], axis=0), "tp", axis=0, tiled=True)
        both = both.reshape(parts_tp, 2, rows_here, width)
        every = both[:, 0].reshape(parts_tp * rows_here, width)
        own = both[:, 1].reshape(parts_tp * rows_here, width)
    else:
        every = lax.all_gather(normed, "tp", axis=0, tiled=True)
    pooled_in = jnp.dot(
        every,
        in_weight,
        preferred_element_type=jnp.float32,
    ).astype(jnp.bfloat16)
    block_rows = pooled_in.shape[0]
    rim_rows = shifted(pooled_in[block_rows - WINDOW_MAX :], "ep", 1)
    values = pooled_in.astype(jnp.float32)
    extended = jnp.concatenate([rim_rows.astype(jnp.float32), values], axis=0)
    window = jnp.left_shift(jnp.int32(2), lax.axis_index("tp"))
    sums = extended
    span = 1
    total = jnp.zeros_like(values)
    for level in range(WINDOW_MAX.bit_length() - 1):
        sums = sums[span:] + sums[:-span]
        span = span * 2
        total = total + jnp.where(window == span, sums[sums.shape[0] - block_rows :], 0.0)
    positions = lax.axis_index("ep") * block_rows + lax.iota(jnp.int32, block_rows) + 1
    counts = jnp.minimum(positions, window).astype(jnp.float32)
    pooled = (total / counts[:, None] - values).astype(jnp.bfloat16)
    grouped = (
        jnp.dot(pooled, group_weight[0], preferred_element_type=jnp.float32)
        * channel_scale.astype(jnp.float32)
    ).astype(jnp.bfloat16)
    mixed_part = jnp.dot(grouped, out_weight, preferred_element_type=jnp.float32).astype(
        jnp.bfloat16
    )
    if dense:
        experts = jnp.arange(n_experts, dtype=jnp.int32)
        named = (route_ids[:, :, None] == experts[None, None, :]).astype(jnp.float32)
        coefs = jnp.sum(named * shares[:, :, None], axis=1)
        coefs = lax.all_gather(coefs, ("ep", "tp"), axis=0, tiled=True)
        blocks = lax.axis_size("ep")
        here = lax.axis_index("ep")
        mine = (experts == here).astype(jnp.float32)
        coef = jnp.sum(coefs * mine[None, :], axis=1).reshape(blocks, parts_tp, rows_here)
        order = list(range(1, blocks))

        def scale_of(k):
            return lax.dynamic_index_in_dim(coef, lax.rem(here - k + blocks, blocks), 0, False)

        def expert_part(rows, scale):
            hidden = expert_hidden(rows, gate_weight[0], up_weight[0])
            part = jnp.dot(hidden, down_weight[0], preferred_element_type=jnp.float32)
            return (part * scale.reshape(-1)[:, None]).astype(jnp.bfloat16)

        moved = jnp.concatenate([turned(expert_in, "ep", k) for k in order], axis=0)
        moved, own = lax.optimization_barrier((moved, own))
        own_part = expert_part(own, scale_of(0))
        others = lax.all_gather(moved, "tp", axis=0, tiled=True)
        part = expert_part(others, jnp.stack([scale_of(k) for k in order], axis=1))
        back = lax.psum_scatter(part, "tp", scatter_dimension=0, tiled=True)
        back = back.reshape(blocks - 1, rows_here, width)
        pair = jnp.stack(
            [value.reshape(parts_tp, rows_here, width) for value in (mixed_part, own_part)], axis=1
        ).reshape(2 * parts_tp * rows_here, width)
        pair = lax.psum_scatter(pair, "tp", scatter_dimension=0, tiled=True)
        total = pair[rows_here:].astype(jnp.float32)
        for i, k in enumerate(order):
            total = total + turned(back[i], "ep", -k).astype(jnp.float32)
        return (pair[:rows_here], total.astype(jnp.bfloat16))
    mixed_tokens = lax.psum_scatter(mixed_part, "tp", scatter_dimension=0, tiled=True)
    flat_ids = route_ids.reshape(rows_here * top_k)
    one_hot = (flat_ids[:, None] == jnp.arange(n_experts, dtype=jnp.int32)[None, :]).astype(
        jnp.int32
    )
    before = jnp.cumsum(one_hot, axis=0) - one_hot
    slots = jnp.sum(before * one_hot, axis=1)
    targets = flat_ids * capacity + slots
    placement = (
        targets.reshape(rows_here, top_k)[None, :, :]
        == jnp.arange(n_experts * capacity, dtype=jnp.int32)[:, None, None]
    )
    dispatch = jnp.any(placement, axis=2).astype(jnp.bfloat16)
    outgoing = jnp.dot(dispatch, expert_in, preferred_element_type=jnp.float32).astype(jnp.bfloat16)
    outgoing = outgoing.reshape(n_experts, capacity, width)
    arrived = lax.all_to_all(outgoing, "ep", split_axis=0, concat_axis=0, tiled=True)
    sources, held, _ = arrived.shape
    flat = arrived.reshape(sources * held, width)
    hidden = expert_hidden(
        lax.all_gather(flat, "tp", axis=0, tiled=True), gate_weight[0], up_weight[0]
    )
    rows = hidden
    summed = lax.psum_scatter(
        jnp.dot(rows, down_weight[0], preferred_element_type=jnp.float32).astype(jnp.bfloat16),
        "tp",
        scatter_dimension=0,
        tiled=True,
    ).astype(jnp.float32)
    expert_out = lax.all_to_all(
        summed.reshape(sources, held, width).astype(jnp.bfloat16),
        "ep",
        split_axis=0,
        concat_axis=0,
        tiled=True,
    ).astype(jnp.float32)
    flat_out = expert_out.reshape(n_experts * capacity, width)
    picked = jnp.take(flat_out, targets, axis=0).reshape(rows_here, top_k, width)
    expert_mix = jnp.sum(picked * shares[:, :, None], axis=1).astype(jnp.bfloat16)
    return (mixed_tokens, expert_mix)


MESH = pl.DeviceIdType.MESH
PIECES_GU = 8
PIECES_D = 4
PIECES = PIECES_GU + PIECES_D
WINDOW = 4
LAG = 3
HALVES = 2


def fused_kernel(
    mixer_tokens,
    mixer_gain,
    in_weight,
    group_weight,
    channel_scale,
    out_weight,
    expert_tokens,
    expert_gain,
    route_ids,
    route_weights,
    gate_weight,
    up_weight,
    down_weight,
    mixed_out,
    expert_out,
    mix_raw,
    exp_raw,
    w_in,
    w_group,
    w_out,
    w_gu,
    w_d,
    tokens,
    coefs,
    scales,
    hid,
    acc,
    rs_in,
    rs_stage,
    mix_all,
    pooled_in,
    mix_part,
    mix_pair,
    mix_stage,
    mix_far,
    rim_rows,
    load_sem,
    x_send,
    x_recv,
    y_send,
    y_recv,
    own_send,
    own_recv,
    fx_send,
    fx_recv,
    fy_send,
    fy_recv,
    ag_send,
    ag_recv,
    coef_send,
    coef_recv,
    rs_send,
    rs_recv,
    mix_send,
    mix_recv,
    rim_send,
    rim_recv,
):
    f32, bf16 = jnp.float32, jnp.bfloat16
    rows, width = exp_raw.shape
    half_rows = rows // HALVES
    group_width = w_group.shape[0]
    ff_half = w_d.shape[1] // 2
    blocks = tokens.shape[0]
    parts = mix_all.shape[0]
    g = lax.axis_index("grp")
    e = lax.axis_index("ep")
    t = lax.axis_index("tp")
    x = t // 2
    c = t % 2
    t_c = 2 * x + 1 - c
    t_x = 2 * (1 - x) + c
    t_d = 2 * (1 - x) + 1 - c
    dev_c, dev_x, dev_y = (g, e, t_c), (g, e, t_x), (1 - g, e, t)
    hi = e // 2
    sign = 1 - 2 * hi
    last = blocks - 1

    def mirror(m):
        return hi * last + sign * m

    u = mirror(e)
    end = u == 0
    mid = u == 1
    far = (g, lax.rem(e + sign + blocks, blocks), t)
    near = (g, lax.rem(e - sign + blocks, blocks), t)
    third = mirror(1 - u)

    def rc(src, dst, send, recv, dev):
        return pltpu.make_async_remote_copy(
            src_ref=src, dst_ref=dst, send_sem=send, recv_sem=recv, device_id=dev, device_id_type=MESH
        )

    barrier = pltpu.get_barrier_semaphore()
    greet = [dev_c, dev_x, dev_y] + [(g, lax.rem(e + k, blocks), t) for k in range(1, blocks)]
    for dev in greet:
        pl.semaphore_signal(barrier, inc=1, device_id=dev, device_id_type=MESH)

    def loads():
        out = []
        for h in range(2):
            hh = g if h == 0 else 1 - g
            lane = pl.multiple_of(hh * ff_half, ff_half)
            out.append((gate_weight.at[0, :, pl.ds(lane, ff_half)], w_gu.at[t, hh, :, pl.ds(0, ff_half)]))
            out.append((up_weight.at[0, :, pl.ds(lane, ff_half)], w_gu.at[t, hh, :, pl.ds(ff_half, ff_half)]))
        out.append((expert_tokens, exp_raw))
        out.append((down_weight.at[0], w_d.at[t]))
        out.append((mixer_tokens, mix_raw))
        out.append((in_weight, w_in))
        out.append((group_weight.at[0], w_group))
        out.append((out_weight, w_out))
        return [pltpu.make_async_copy(a, b, load_sem.at[i]) for i, (a, b) in enumerate(out)]

    local = loads()
    for copy in local:
        copy.start()
    def norm(raw, gain, dst, start, count):
        step = 16
        gain_row = gain[...].astype(f32).reshape(1, width)

        @pl.loop(0, count // step)
        def _(i):
            at = pl.ds(pl.multiple_of(start + i * step, step), step)
            values = raw[at, :].astype(f32)
            scaled = values * lax.rsqrt(jnp.mean(values * values, axis=-1, keepdims=True) + 1e-06)
            dst[at, :] = (scaled * gain_row).astype(bf16)

    local[4].wait()
    norm(exp_raw, expert_gain, tokens.at[e], 0, rows)
    ids = route_ids[...]
    weights = route_weights[...]
    shares = weights / jnp.sum(weights, axis=0, keepdims=True)
    numbers = lax.broadcasted_iota(jnp.int32, coefs.shape[1:], 0)
    coef = jnp.zeros(coefs.shape[1:], f32)
    for k in range(ids.shape[0]):
        coef = coef + jnp.where(ids[k : k + 1, :] == numbers, shares[k : k + 1, :], 0.0)
    coefs[e] = coef

    def piece(q, h, s):
        if s < PIECES_GU:
            n = width // PIECES_GU
            return w_gu.at[q, h, pl.ds(s * n, n), :]
        n = ff_half // PIECES_D
        start = pl.multiple_of(h * ff_half + (s - PIECES_GU) * n, n)
        return w_d.at[q, pl.ds(start, n), :]

    def send_x(s):
        p = piece(t, g, s)
        return rc(p, p, x_send.at[s], x_recv.at[s], dev_x)

    def got_x(s):
        p = piece(t_x, g, s)
        return rc(p, p, x_send.at[s], x_recv.at[s], dev_x)

    def send_y(s):
        p = piece(t_x, g, s)
        return rc(p, p, y_send.at[s], y_recv.at[s], dev_y)

    def got_y(s):
        p = piece(t_x, 1 - g, s)
        return rc(p, p, y_send.at[s], y_recv.at[s], dev_y)

    def send_fx(s):
        p = piece(t_x, g, s)
        return rc(p, p, fx_send.at[s], fx_recv.at[s], dev_c)

    def got_fx(s):
        p = piece(t_d, g, s)
        return rc(p, p, fx_send.at[s], fx_recv.at[s], dev_c)

    def send_fy(s):
        p = piece(t_x, 1 - g, s)
        return rc(p, p, fy_send.at[s], fy_recv.at[s], dev_c)

    def got_fy(s):
        p = piece(t_d, 1 - g, s)
        return rc(p, p, fy_send.at[s], fy_recv.at[s], dev_c)

    def own_gu(q):
        return rc(w_gu.at[q], w_gu.at[q], own_send.at[0], own_recv.at[0], dev_c)

    def own_d(q):
        return rc(w_d.at[q], w_d.at[q], own_send.at[1], own_recv.at[1], dev_c)

    def chunk(home, j):
        return tokens.at[home, pl.ds(j * half_rows, half_rows), :]

    def ag_far(home, j, f):
        p = chunk(home, j)
        return rc(p, p, ag_send.at[f], ag_recv.at[f + 6 * (1 - u)], far)

    def ag_near(home, j, f):
        p = chunk(home, j)
        return rc(p, p, ag_send.at[4 + f], ag_recv.at[f], near)

    def ag_got(home, j, f):
        p = chunk(home, j)
        return rc(p, p, ag_send.at[0], ag_recv.at[f], far)

    rim_source = (t == parts - 1) & (e < last)
    rim_mine = (t == parts - 1) & (e > 0)
    rim_relay = (t == parts // 2 - 1) & (e > 0)
    rim_last = (c == 0) & (e > 0)

    def rim_to(k):
        src = mix_all.at[t, pl.ds(rows - rim_rows.shape[0], rim_rows.shape[0]), :] if k == 0 else rim_rows
        dev = ((g, lax.rem(e + 1, blocks), t), dev_x, dev_c)[k]
        return rc(src, rim_rows, rim_send.at[k], rim_recv.at[k], dev)

    def coef_to(k):
        dev = (g, lax.rem(e + k, blocks), t)
        return rc(coefs.at[e], coefs.at[e], coef_send.at[k - 1], coef_recv.at[k - 1], dev)

    def coef_got(k):
        home = lax.rem(e - k + blocks, blocks)
        return rc(coefs.at[home], coefs.at[home], coef_send.at[k - 1], coef_recv.at[k - 1], dev_c)

    def mix_x(q, j):
        p = mix_all.at[q, pl.ds(j * half_rows, half_rows), :]
        return rc(p, p, mix_send.at[j], mix_recv.at[j], dev_x)

    def mix_fwd(q, j):
        p = mix_all.at[q, pl.ds(j * half_rows, half_rows), :]
        return rc(p, p, mix_send.at[2 + j], mix_recv.at[2 + j], dev_c)

    def mix_own(q):
        return rc(mix_all.at[q], mix_all.at[q], mix_send.at[4], mix_recv.at[4], dev_c)

    local[0].wait()
    local[1].wait()
    pl.semaphore_wait(barrier, len(greet))
    for s in range(WINDOW):
        send_x(s).start()
    for k in range(1, blocks):
        coef_to(k).start()
    for j in range(HALVES):
        ag_far(e, j, j).start()

        @pl.when(mid)
        def _():
            ag_near(e, j, j).start()

    local[2].wait()
    local[3].wait()
    own_gu(t).start()
    local[5].wait()
    own_d(t).start()
    local[6].wait()
    norm(mix_raw, mixer_gain, mix_all.at[t], 0, rows)

    @pl.when(rim_source)
    def _():
        rim_to(0).start()

    mix_own(t).start()

    def hidden(home, xq):
        @pl.loop(0, 4)
        def _(j):
            q = 2 * xq + j // 2
            h = j % 2
            both = jnp.dot(tokens[home], w_gu[q, h], preferred_element_type=f32)
            gate, upper = both[:, :ff_half], both[:, ff_half:]
            value = gate / (1.0 + jnp.exp(-gate)) * upper
            hid[home, xq, :, pl.ds(pl.multiple_of(j * ff_half, ff_half), ff_half)] = value.astype(bf16)

    col = 512

    def down(home, xq, first):
        @pl.loop(0, width // col)
        def _(n):
            at = pl.ds(pl.multiple_of(n * col, col), col)
            w = w_d[pl.ds(2 * xq, 2), :, at].reshape(4 * ff_half, col)
            part = jnp.dot(hid[home, xq], w, preferred_element_type=f32)
            if first:
                acc[home, :, at] = part
            else:
                scale = scales[home][:, :1]
                acc[home, :, at] = (acc[home, :, at] + part) * scale

    def pool_in(xq):
        @pl.loop(0, 2)
        def _(j):
            q = 2 * xq + j
            value = jnp.dot(mix_all[q], w_in[...], preferred_element_type=f32)
            pooled_in[pl.ds(pl.multiple_of(rows * (q + 1), rows), rows), :] = value.astype(bf16)

    def wait_fgu():
        for s in range(PIECES_GU):
            got_fx(s).wait_recv()
            got_fy(s).wait_recv()

    def relay_y(s):
        got_y(s).wait_recv()
        send_fy(s).start()

    def gather(f):
        @pl.when(end)
        def _():
            ag_got(mirror(1 + f // 2), f % 2, f).wait_recv()

        if f < 4:

            @pl.when(mid)
            def _():
                home = mirror(2 + f // 2)
                ag_got(home, f % 2, f).wait_recv()
                ag_near(home, f % 2, f + 2).start()

        if f < 2:

            @pl.when(mid)
            def _():
                home = mirror(0)
                ag_got(home, f % 2, 6 + f).wait_recv()
                ag_far(home, f % 2, 2 + f).start()

    for s in range(PIECES):
        got_x(s).wait_recv()
        send_y(s).start()
        send_fx(s).start()
        if s + WINDOW < PIECES:
            send_x(s + WINDOW).start()
        elif s + WINDOW < PIECES + HALVES:
            mix_x(t, s + WINDOW - PIECES).start()
        if s >= LAG:
            relay_y(s - LAG)
        if s >= 2 and s % 2 == 0:
            gather(s // 2 - 1)
        if s == 1:
            for k in range(1, blocks):
                coef_got(k).wait_recv()
            for home in range(blocks):
                row = coefs[home, pl.ds(e, 1), :]
                scales[home] = jnp.transpose(jnp.broadcast_to(row, (rows, rows)))
        if s == 2:
            own_gu(t_c).wait_recv()
            hidden(e, x)
        if s == 5:

            @pl.when(rim_mine)
            def _():
                rim_to(0).wait_recv()
                rim_to(1).start()
                rim_to(2).start()

        if s == 3:
            own_d(t_c).wait_recv()
            down(e, x, True)
        if s == 4:
            pooled_in[pl.ds(0, rows), :] = jnp.zeros((rows, group_width), bf16)
        if s == 5:
            hidden(third, x)
        if s == 6:
            down(third, x, True)
        if s == 7:
            mix_own(t_c).wait_recv()
            local[7].wait()
            pool_in(x)
        if s == 11:

            @pl.when(rim_relay)
            def _():
                rim_to(1).wait_recv()
                rim_to(2).start()

        if s == 9:
            hidden(mirror(2), x)
            down(mirror(2), x, True)
        if s == 10:
            wait_fgu()
            hidden(mirror(2), 1 - x)
        if s == 11:
            hidden(third, 1 - x)

    for s in range(PIECES - LAG, PIECES - 1):
        relay_y(s)
    hidden(e, 1 - x)
    gather(5)
    hidden(mirror(3), x)
    down(mirror(3), x, True)
    hidden(mirror(3), 1 - x)
    relay_y(PIECES - 1)
    for s in range(PIECES_GU, PIECES):
        got_fx(s).wait_recv()
        got_fy(s).wait_recv()

    def rs_far(k):
        p = rs_stage.at[k]
        return rc(p, rs_in.at[k + 6 * u], rs_send.at[k], rs_recv.at[k + 6 * u], far)

    def rs_near(k):
        p = rs_stage.at[4 + k]
        return rc(p, rs_in.at[6 + k], rs_send.at[4 + k], rs_recv.at[6 + k], near)

    def rs_got(k):
        return rc(rs_in.at[k], rs_in.at[k], rs_send.at[0], rs_recv.at[k], far)

    def first_send(home, k):
        @pl.when(end)
        def _():
            for j in range(HALVES):
                at = pl.ds(j * half_rows, half_rows)
                rs_stage[k + j] = acc[home, at, :].astype(bf16)
                rs_far(k + j).start()

    def lead(k):
        @pl.when(mid)
        def _():
            rs_got(k).wait_recv()
            if k < 4:
                at = pl.ds((k % 2) * half_rows, half_rows)
                rs_stage[k] = (acc[mirror(3 - k // 2), at, :] + rs_in[k].astype(f32)).astype(bf16)
                rs_far(k).start()

    def lag(k):
        @pl.when(mid)
        def _():
            rs_got(6 + k).wait_recv()
            if k < 2:
                at = pl.ds((k % 2) * half_rows, half_rows)
                rs_stage[4 + k] = (acc[mirror(0), at, :] + rs_in[6 + k].astype(f32)).astype(bf16)
                rs_near(k).start()

    down(mirror(3), 1 - x, False)
    first_send(mirror(3), 0)
    down(mirror(2), 1 - x, False)
    first_send(mirror(2), 2)
    down(third, 1 - x, False)
    first_send(third, 4)
    down(e, 1 - x, False)

    for j in range(HALVES):
        mix_x(t_x, j).wait_recv()
        mix_fwd(t_x, j).start()
    lead(0)

    for j in range(HALVES):
        mix_fwd(t_d, j).wait_recv()
    pool_in(1 - x)

    @pl.when(rim_last)
    def _():
        rim_to(2).wait_recv()

    @pl.when(e > 0)
    def _():
        value = jnp.dot(rim_rows[...], w_in[...], preferred_element_type=f32)
        pooled_in[pl.ds(rows - rim_rows.shape[0], rim_rows.shape[0]), :] = value.astype(bf16)

    lead(1)
    local[8].wait()
    local[9].wait()
    window = 2 + 2 * jnp.minimum(t, 1) + 4 * (t // 2) + 8 * (t // 3)

    def mix_down(j):
        q = (2 * (1 - x) if j < 2 else 2 * x) + (1 - c if j % 2 == 0 else c)
        start = pl.multiple_of(q * rows, rows)
        seg = pooled_in[pl.ds(start, 2 * rows), :]
        i = lax.broadcasted_iota(jnp.int32, (rows, 2 * rows), 0) + rows
        k = lax.broadcasted_iota(jnp.int32, (rows, 2 * rows), 1)
        band = jnp.where((k <= i) & (k > i - window), 1.0, 0.0).astype(bf16)
        sums = jnp.dot(band, seg, preferred_element_type=f32)
        place = lax.broadcasted_iota(jnp.int32, (rows, 1), 0) + (e * blocks + q) * rows + 1
        counts = jnp.minimum(place, window).astype(f32)
        pooled = (sums / counts - seg[rows:, :].astype(f32)).astype(bf16)
        grouped = jnp.dot(pooled, w_group[...], preferred_element_type=f32)
        grouped = (grouped * channel_scale[...].astype(f32).reshape(1, group_width)).astype(bf16)

        @pl.loop(0, width // col)
        def _(n):
            at = pl.ds(pl.multiple_of(n * col, col), col)
            mix_part[j, :, at] = jnp.dot(grouped, w_out[:, at], preferred_element_type=f32).astype(bf16)

    def pair_to(j):
        return rc(mix_part.at[2 * j], mix_pair.at[j], mix_send.at[6 + j], mix_recv.at[6 + j], dev_c)

    def cross(j):
        at = pl.ds(j * half_rows, half_rows)
        return rc(mix_stage.at[at, :], mix_far.at[at, :], mix_send.at[8 + j], mix_recv.at[8 + j], dev_x)

    mix_down(0)
    pair_to(0).start()
    mix_down(1)
    pair_to(0).wait_recv()
    for j in range(HALVES):
        at = pl.ds(j * half_rows, half_rows)
        mix_stage[at, :] = (mix_part[1, at, :].astype(f32) + mix_pair[0, at, :].astype(f32)).astype(bf16)
        cross(j).start()
    lag(0)
    lead(2)
    mix_down(2)
    pair_to(1).start()
    mix_down(3)
    lag(1)
    lead(3)
    lag(2)
    lead(4)
    lag(3)
    pair_to(1).wait_recv()
    for j in range(HALVES):
        at = pl.ds(j * half_rows, half_rows)
        cross(j).wait_recv()
        mixed_out[at, :] = (
            mix_part[3, at, :].astype(f32) + mix_pair[1, at, :].astype(f32) + mix_far[at, :].astype(f32)
        ).astype(bf16)
    lead(5)
    for j in range(HALVES):
        at = pl.ds(j * half_rows, half_rows)

        @pl.when(mid)
        def _():
            expert_out[at, :] = (acc[e, at, :] + rs_in[4 + j].astype(f32) + rs_in[8 + j].astype(f32)).astype(bf16)

        @pl.when(end)
        def _():
            rs_got(6 + j).wait_recv()
            expert_out[at, :] = (acc[e, at, :] + rs_in[6 + j].astype(f32)).astype(bf16)

    for s in range(PIECES):
        send_x(s).wait_send()
        send_y(s).wait_send()
        send_fx(s).wait_send()
        send_fy(s).wait_send()
    own_gu(t).wait_send()
    own_d(t).wait_send()
    for k in range(1, blocks):
        coef_to(k).wait_send()
    for j in range(HALVES):
        ag_far(e, j, j).wait_send()
        mix_x(t, j).wait_send()
        mix_fwd(t_x, j).wait_send()
        pair_to(j).wait_send()
        cross(j).wait_send()
    mix_own(t).wait_send()

    @pl.when(rim_source)
    def _():
        rim_to(0).wait_send()

    @pl.when(rim_mine)
    def _():
        rim_to(1).wait_send()
        rim_to(2).wait_send()

    @pl.when(rim_relay)
    def _():
        rim_to(2).wait_send()

    @pl.when(end)
    def _():
        for k in range(6):
            rs_far(k).wait_send()

    @pl.when(mid)
    def _():
        for f in range(6):
            ag_near(e, f % 2, f).wait_send()
        for f in range(2):
            ag_far(e, f, 2 + f).wait_send()
        for k in range(4):
            rs_far(k).wait_send()
        for k in range(2):
            rs_near(k).wait_send()


def fused(*args):
    (mixer_tokens, _, in_weight, group_weight, _, out_weight, _, _, route_ids, _, gate_weight, _, _) = args
    rows, width = mixer_tokens.shape
    group_width = in_weight.shape[1]
    ff = gate_weight.shape[2]
    blocks = lax.axis_size("ep")
    parts = lax.axis_size("tp")
    half = rows // HALVES
    bf16, f32 = jnp.bfloat16, jnp.float32
    vmem = pltpu.VMEM
    dma = pltpu.SemaphoreType.DMA
    anyspace = pl.BlockSpec(memory_space=pl.ANY)
    local_spec = pl.BlockSpec(memory_space=pltpu.VMEM)
    args = list(args)
    for i in (8, 9):
        args[i] = args[i].T
    small = (1, 4, 7, 8, 9)
    scratch = [
        vmem((rows, width), bf16),
        vmem((rows, width), bf16),
        vmem((width, group_width), bf16),
        vmem((group_width, group_width), bf16),
        vmem((group_width, width), bf16),
        vmem((parts, 2, width, ff), bf16),
        vmem((parts, ff, width), bf16),
        vmem((blocks, rows, width), bf16),
        vmem((blocks, 8, rows), f32),
        vmem((blocks, rows, rows), f32),
        vmem((blocks, 2, rows, 2 * ff), bf16),
        vmem((blocks, rows, width), f32),
        vmem((10, half, width), bf16),
        vmem((6, half, width), bf16),
        vmem((parts, rows, width), bf16),
        vmem((rows * (parts + 1), group_width), bf16),
        vmem((parts, rows, width), bf16),
        vmem((2, rows, width), bf16),
        vmem((rows, width), bf16),
        vmem((rows, width), bf16),
        vmem((WINDOW_MAX, width), bf16),
        dma((10,)),
    ]
    for count in (PIECES, PIECES, PIECES, PIECES, 2, 2, PIECES, PIECES, PIECES, PIECES, 10, 8, 3, 3, 6, 10, 10, 10, 3, 3):
        scratch.append(dma((count,)))
    shape = vmem((rows, width), bf16)
    return pl.pallas_call(
        fused_kernel,
        out_shape=(shape, shape),
        in_specs=[local_spec if i in small else anyspace for i in range(len(args))],
        out_specs=(local_spec, local_spec),
        scratch_shapes=scratch,
        compiler_params=pltpu.CompilerParams(
            collective_id=0, has_side_effects=True, vmem_limit_bytes=60 << 20
        ),
        name="fused",
    )(*args)


def fits(mesh):
    sizes = dict(mesh.shape)
    return sizes["grp"] == 2 and sizes["ep"] == 4 and sizes["tp"] == 4


def solution(mesh):
    placed = (
        P(("grp", "ep", "tp"), None),
        P(),
        P(None, "tp"),
        P("tp", None, None),
        P("tp"),
        P("tp", None),
        P(("grp", "ep", "tp"), None),
        P(),
        P(("grp", "ep", "tp"), None),
        P(("grp", "ep", "tp"), None),
        P("ep", None, "tp"),
        P("ep", None, "tp"),
        P("ep", "tp", None),
    )
    return jax.shard_map(
        fused if fits(mesh) else local,
        mesh=mesh,
        in_specs=placed,
        out_specs=(P(("grp", "ep", "tp"), None), P(("grp", "ep", "tp"), None)),
        check_vma=False,
    )
```

```python
import jax
import jax.numpy as jnp
from jax import lax
from jax.experimental import pallas as pl
from jax.experimental.pallas import tpu as pltpu
from jax.sharding import PartitionSpec as P

WINDOW_MAX = 16


def shifted(value, axis, by):
    devices = lax.axis_size(axis)
    pairs = [(i, i + by) for i in range(devices) if 0 <= i + by < devices]
    return lax.ppermute(value, axis, pairs)


def turned(value, axis, by):
    devices = lax.axis_size(axis)
    if by % devices == 0:
        return value
    return lax.ppermute(value, axis, [(i, (i + by) % devices) for i in range(devices)])


def rms_rows(rows, gain):
    values = rows.astype(jnp.float32)
    scaled = values * lax.rsqrt(jnp.mean(values * values, axis=-1, keepdims=True) + 1e-06)
    return (scaled * gain.astype(jnp.float32)).astype(jnp.bfloat16)


def expert_hidden(rows, w_gate, w_up):
    gate = jnp.dot(rows, w_gate, preferred_element_type=jnp.float32)
    upper = jnp.dot(rows, w_up, preferred_element_type=jnp.float32)
    return (jax.nn.silu(gate) * upper).astype(jnp.bfloat16)


def local(
    mixer_tokens,
    mixer_gain,
    in_weight,
    group_weight,
    channel_scale,
    out_weight,
    expert_tokens,
    expert_gain,
    route_ids,
    route_weights,
    gate_weight,
    up_weight,
    down_weight,
):
    normed = rms_rows(mixer_tokens, mixer_gain)
    expert_in = rms_rows(expert_tokens, expert_gain)
    shares = route_weights / jnp.sum(route_weights, axis=1, keepdims=True)
    rows_here, top_k = route_ids.shape
    width = expert_in.shape[1]
    n_experts = lax.axis_size("ep") * gate_weight.shape[0]
    capacity = 4 * rows_here // n_experts
    dense = capacity >= rows_here
    parts_tp = lax.axis_size("tp")
    if dense:
        both = lax.all_gather(jnp.concatenate([normed, expert_in], axis=0), "tp", axis=0, tiled=True)
        both = both.reshape(parts_tp, 2, rows_here, width)
        every = both[:, 0].reshape(parts_tp * rows_here, width)
        own = both[:, 1].reshape(parts_tp * rows_here, width)
    else:
        every = lax.all_gather(normed, "tp", axis=0, tiled=True)
    pooled_in = jnp.dot(
        every,
        in_weight,
        preferred_element_type=jnp.float32,
    ).astype(jnp.bfloat16)
    block_rows = pooled_in.shape[0]
    rim_rows = shifted(pooled_in[block_rows - WINDOW_MAX :], "ep", 1)
    values = pooled_in.astype(jnp.float32)
    extended = jnp.concatenate([rim_rows.astype(jnp.float32), values], axis=0)
    window = jnp.left_shift(jnp.int32(2), lax.axis_index("tp"))
    sums = extended
    span = 1
    total = jnp.zeros_like(values)
    for level in range(WINDOW_MAX.bit_length() - 1):
        sums = sums[span:] + sums[:-span]
        span = span * 2
        total = total + jnp.where(window == span, sums[sums.shape[0] - block_rows :], 0.0)
    positions = lax.axis_index("ep") * block_rows + lax.iota(jnp.int32, block_rows) + 1
    counts = jnp.minimum(positions, window).astype(jnp.float32)
    pooled = (total / counts[:, None] - values).astype(jnp.bfloat16)
    grouped = (
        jnp.dot(pooled, group_weight[0], preferred_element_type=jnp.float32)
        * channel_scale.astype(jnp.float32)
    ).astype(jnp.bfloat16)
    mixed_part = jnp.dot(grouped, out_weight, preferred_element_type=jnp.float32).astype(
        jnp.bfloat16
    )
    if dense:
        experts = jnp.arange(n_experts, dtype=jnp.int32)
        named = (route_ids[:, :, None] == experts[None, None, :]).astype(jnp.float32)
        coefs = jnp.sum(named * shares[:, :, None], axis=1)
        coefs = lax.all_gather(coefs, ("ep", "tp"), axis=0, tiled=True)
        blocks = lax.axis_size("ep")
        here = lax.axis_index("ep")
        mine = (experts == here).astype(jnp.float32)
        coef = jnp.sum(coefs * mine[None, :], axis=1).reshape(blocks, parts_tp, rows_here)
        order = list(range(1, blocks))

        def scale_of(k):
            return lax.dynamic_index_in_dim(coef, lax.rem(here - k + blocks, blocks), 0, False)

        def expert_part(rows, scale):
            hidden = expert_hidden(rows, gate_weight[0], up_weight[0])
            part = jnp.dot(hidden, down_weight[0], preferred_element_type=jnp.float32)
            return (part * scale.reshape(-1)[:, None]).astype(jnp.bfloat16)

        moved = jnp.concatenate([turned(expert_in, "ep", k) for k in order], axis=0)
        moved, own = lax.optimization_barrier((moved, own))
        own_part = expert_part(own, scale_of(0))
        others = lax.all_gather(moved, "tp", axis=0, tiled=True)
        part = expert_part(others, jnp.stack([scale_of(k) for k in order], axis=1))
        back = lax.psum_scatter(part, "tp", scatter_dimension=0, tiled=True)
        back = back.reshape(blocks - 1, rows_here, width)
        pair = jnp.stack(
            [value.reshape(parts_tp, rows_here, width) for value in (mixed_part, own_part)], axis=1
        ).reshape(2 * parts_tp * rows_here, width)
        pair = lax.psum_scatter(pair, "tp", scatter_dimension=0, tiled=True)
        total = pair[rows_here:].astype(jnp.float32)
        for i, k in enumerate(order):
            total = total + turned(back[i], "ep", -k).astype(jnp.float32)
        return (pair[:rows_here], total.astype(jnp.bfloat16))
    mixed_tokens = lax.psum_scatter(mixed_part, "tp", scatter_dimension=0, tiled=True)
    flat_ids = route_ids.reshape(rows_here * top_k)
    one_hot = (flat_ids[:, None] == jnp.arange(n_experts, dtype=jnp.int32)[None, :]).astype(
        jnp.int32
    )
    before = jnp.cumsum(one_hot, axis=0) - one_hot
    slots = jnp.sum(before * one_hot, axis=1)
    targets = flat_ids * capacity + slots
    placement = (
        targets.reshape(rows_here, top_k)[None, :, :]
        == jnp.arange(n_experts * capacity, dtype=jnp.int32)[:, None, None]
    )
    dispatch = jnp.any(placement, axis=2).astype(jnp.bfloat16)
    outgoing = jnp.dot(dispatch, expert_in, preferred_element_type=jnp.float32).astype(jnp.bfloat16)
    outgoing = outgoing.reshape(n_experts, capacity, width)
    arrived = lax.all_to_all(outgoing, "ep", split_axis=0, concat_axis=0, tiled=True)
    sources, held, _ = arrived.shape
    flat = arrived.reshape(sources * held, width)
    hidden = expert_hidden(
        lax.all_gather(flat, "tp", axis=0, tiled=True), gate_weight[0], up_weight[0]
    )
    rows = hidden
    summed = lax.psum_scatter(
        jnp.dot(rows, down_weight[0], preferred_element_type=jnp.float32).astype(jnp.bfloat16),
        "tp",
        scatter_dimension=0,
        tiled=True,
    ).astype(jnp.float32)
    expert_out = lax.all_to_all(
        summed.reshape(sources, held, width).astype(jnp.bfloat16),
        "ep",
        split_axis=0,
        concat_axis=0,
        tiled=True,
    ).astype(jnp.float32)
    flat_out = expert_out.reshape(n_experts * capacity, width)
    picked = jnp.take(flat_out, targets, axis=0).reshape(rows_here, top_k, width)
    expert_mix = jnp.sum(picked * shares[:, :, None], axis=1).astype(jnp.bfloat16)
    return (mixed_tokens, expert_mix)


MESH = pl.DeviceIdType.MESH
GU_CUTS = (0, 1, 2, 4, 6, 8, 10, 12, 14, 16)
PIECES_GU = len(GU_CUTS) - 1
D_CUTS = (0, 2, 4, 6, 7, 8)
PIECES = PIECES_GU + len(D_CUTS) - 1
WINDOW = 5
LAG = 3
HALVES = 2
CUTS = ((0, 1, 2, 4, 6, 8), (0, 2, 4, 6, 7, 8))
CHUNKS = len(CUTS[0]) - 1


def fused_kernel(
    mixer_tokens,
    mixer_gain,
    in_weight,
    group_weight,
    channel_scale,
    out_weight,
    expert_tokens,
    expert_gain,
    route_ids,
    route_weights,
    gate_weight,
    up_weight,
    down_weight,
    mixed_out,
    expert_out,
    mix_raw,
    exp_raw,
    w_in,
    w_group,
    w_out,
    w_gu,
    w_d,
    tokens,
    coefs,
    scales,
    hid,
    acc,
    rs_in,
    rs_stage,
    mix_all,
    pooled_in,
    mix_part,
    mix_pair,
    mix_stage,
    mix_far,
    rim_rows,
    w_d2,
    hid_far,
    load_sem,
    x_send,
    x_recv,
    y_send,
    y_recv,
    own_send,
    own_recv,
    fx_send,
    fx_recv,
    fy_send,
    fy_recv,
    ag_send,
    ag_recv,
    coef_send,
    coef_recv,
    rs_send,
    rs_recv,
    mix_send,
    mix_recv,
    rim_send,
    rim_recv,
    d2_send,
    d2_recv,
):
    f32, bf16 = jnp.float32, jnp.bfloat16
    rows, width = exp_raw.shape
    half_rows = rows // HALVES
    group_width = w_group.shape[0]
    ff_half = w_d.shape[1] // 2
    blocks = tokens.shape[0]
    parts = mix_all.shape[0]
    g = lax.axis_index("grp")
    e = lax.axis_index("ep")
    t = lax.axis_index("tp")
    x = t // 2
    c = t % 2
    t_c = 2 * x + 1 - c
    t_x = 2 * (1 - x) + c
    t_d = 2 * (1 - x) + 1 - c
    dev_c, dev_x, dev_y = (g, e, t_c), (g, e, t_x), (1 - g, e, t)
    hi = e // 2
    sign = 1 - 2 * hi
    last = blocks - 1

    def mirror(m):
        return hi * last + sign * m

    u = mirror(e)
    end = u == 0
    mid = u == 1
    far = (g, lax.rem(e + sign + blocks, blocks), t)
    near = (g, lax.rem(e - sign + blocks, blocks), t)
    third = mirror(1 - u)

    def rc(src, dst, send, recv, dev):
        return pltpu.make_async_remote_copy(
            src_ref=src, dst_ref=dst, send_sem=send, recv_sem=recv, device_id=dev, device_id_type=MESH
        )

    barrier = pltpu.get_barrier_semaphore()
    greet = [dev_c, dev_x, dev_y] + [(g, lax.rem(e + k, blocks), t) for k in range(1, blocks)]
    for dev in greet:
        pl.semaphore_signal(barrier, inc=1, device_id=dev, device_id_type=MESH)

    def loads():
        out = []
        for h in range(2):
            hh = g if h == 0 else 1 - g
            lane = pl.multiple_of(hh * ff_half, ff_half)
            out.append((gate_weight.at[0, :, pl.ds(lane, ff_half)], w_gu.at[t, hh, :, pl.ds(0, ff_half)]))
            out.append((up_weight.at[0, :, pl.ds(lane, ff_half)], w_gu.at[t, hh, :, pl.ds(ff_half, ff_half)]))
        out.append((expert_tokens, exp_raw))
        out.append((down_weight.at[0], w_d.at[t]))
        out.append((mixer_tokens, mix_raw))
        out.append((in_weight, w_in))
        out.append((group_weight.at[0], w_group))
        out.append((out_weight, w_out))
        return [pltpu.make_async_copy(a, b, load_sem.at[i]) for i, (a, b) in enumerate(out)]

    local = loads()
    for copy in local:
        copy.start()
    def norm(raw, gain, dst, start, count):
        step = 16
        gain_row = gain[...].astype(f32).reshape(1, width)

        @pl.loop(0, count // step)
        def _(i):
            at = pl.ds(pl.multiple_of(start + i * step, step), step)
            values = raw[at, :].astype(f32)
            scaled = values * lax.rsqrt(jnp.mean(values * values, axis=-1, keepdims=True) + 1e-06)
            dst[at, :] = (scaled * gain_row).astype(bf16)

    local[4].wait()
    norm(exp_raw, expert_gain, tokens.at[e], 0, rows)
    ids = route_ids[...]
    weights = route_weights[...]
    shares = weights / jnp.sum(weights, axis=0, keepdims=True)
    numbers = lax.broadcasted_iota(jnp.int32, coefs.shape[1:], 0)
    coef = jnp.zeros(coefs.shape[1:], f32)
    for k in range(ids.shape[0]):
        coef = coef + jnp.where(ids[k : k + 1, :] == numbers, shares[k : k + 1, :], 0.0)
    coefs[e] = coef

    def d_cut(s):
        unit = ff_half // D_CUTS[-1]
        low, high = D_CUTS[s - PIECES_GU], D_CUTS[s - PIECES_GU + 1]
        return low * unit, (high - low) * unit

    def piece(q, h, s):
        if s < PIECES_GU:
            unit = width // GU_CUTS[-1]
            low, high = GU_CUTS[s], GU_CUTS[s + 1]
            return w_gu.at[q, h, pl.ds(low * unit, (high - low) * unit), :]
        start, n = d_cut(s)
        return w_d.at[q, pl.ds(pl.multiple_of(h * ff_half + start, 16), n), :]

    def send_x(s):
        p = piece(t, g, s)
        return rc(p, p, x_send.at[s], x_recv.at[s], dev_x)

    def got_x(s):
        p = piece(t_x, g, s)
        return rc(p, p, x_send.at[s], x_recv.at[s], dev_x)

    def send_y(s):
        p = piece(t_x, g, s)
        return rc(p, p, y_send.at[s], y_recv.at[s], dev_y)

    def got_y(s):
        p = piece(t_x, 1 - g, s)
        return rc(p, p, y_send.at[s], y_recv.at[s], dev_y)

    def send_fx(s):
        p = piece(t_x, g, s)
        return rc(p, p, fx_send.at[s], fx_recv.at[s], dev_c)

    def got_fx(s):
        p = piece(t_d, g, s)
        return rc(p, p, fx_send.at[s], fx_recv.at[s], dev_c)

    def send_fy(s):
        p = piece(t_x, 1 - g, s)
        return rc(p, p, fy_send.at[s], fy_recv.at[s], dev_c)

    def got_fy(s):
        p = piece(t_d, 1 - g, s)
        return rc(p, p, fy_send.at[s], fy_recv.at[s], dev_c)

    def own_gu(q):
        return rc(w_gu.at[q], w_gu.at[q], own_send.at[0], own_recv.at[0], dev_c)

    def own_d(q):
        return rc(w_d.at[q], w_d.at[q], own_send.at[1], own_recv.at[1], dev_c)

    def chunk(home, j):
        return tokens.at[home, pl.ds(j * half_rows, half_rows), :]

    def ag_far(home, j, f):
        p = chunk(home, j)
        return rc(p, p, ag_send.at[f], ag_recv.at[f + 6 * (1 - u)], far)

    def ag_near(home, j, f):
        p = chunk(home, j)
        return rc(p, p, ag_send.at[4 + f], ag_recv.at[f], near)

    def ag_got(home, j, f):
        p = chunk(home, j)
        return rc(p, p, ag_send.at[0], ag_recv.at[f], far)

    rim_source = (t == parts - 1) & (e < last)
    rim_mine = (t == parts - 1) & (e > 0)
    rim_relay = (t == parts // 2 - 1) & (e > 0)
    rim_last = (c == 0) & (e > 0)

    def rim_to(k):
        src = mix_all.at[t, pl.ds(rows - rim_rows.shape[0], rim_rows.shape[0]), :] if k == 0 else rim_rows
        dev = ((g, lax.rem(e + 1, blocks), t), dev_x, dev_c)[k]
        return rc(src, rim_rows, rim_send.at[k], rim_recv.at[k], dev)

    def coef_to(k):
        dev = (g, lax.rem(e + k, blocks), t)
        return rc(coefs.at[e], coefs.at[e], coef_send.at[k - 1], coef_recv.at[k - 1], dev)

    def coef_got(k):
        home = lax.rem(e - k + blocks, blocks)
        return rc(coefs.at[home], coefs.at[home], coef_send.at[k - 1], coef_recv.at[k - 1], dev_c)

    def d2_half(ref, q, h):
        return ref.at[q, pl.ds(pl.multiple_of(h * ff_half, ff_half), ff_half), :]

    def d2_piece(ref, s):
        start, n = d_cut(s)
        return ref.at[t_x, pl.ds(pl.multiple_of(g * ff_half + start, 16), n), :]

    def d2_own():
        return rc(d2_half(w_d, t, g), d2_half(w_d2, t, g), d2_send.at[0], d2_recv.at[0], far)

    def d2_relay(s):
        k = 1 + s - PIECES_GU
        return rc(d2_piece(w_d, s), d2_piece(w_d2, s), d2_send.at[k], d2_recv.at[k], far)

    def d2_hid(xq, k):
        return rc(hid.at[third, xq], hid_far.at[xq], d2_send.at[6 + k], d2_recv.at[6 + k], far)

    def d2_y(k, mine):
        p = d2_half(w_d2, t if k == 0 else t_x, g if mine else 1 - g)
        return rc(p, p, d2_send.at[8 + k], d2_recv.at[8 + k], dev_y)

    def d2_c(k, mine):
        q = (t if k % 2 == 0 else t_x) if mine else (t_c if k % 2 == 0 else t_d)
        p = d2_half(w_d2, q, g if k < 2 else 1 - g)
        return rc(p, p, d2_send.at[10 + k], d2_recv.at[10 + k], dev_c)

    def mix_x(q, j):
        p = mix_all.at[q, pl.ds(j * half_rows, half_rows), :]
        return rc(p, p, mix_send.at[j], mix_recv.at[j], dev_x)

    def mix_fwd(q, j):
        p = mix_all.at[q, pl.ds(j * half_rows, half_rows), :]
        return rc(p, p, mix_send.at[2 + j], mix_recv.at[2 + j], dev_c)

    def mix_own(q):
        return rc(mix_all.at[q], mix_all.at[q], mix_send.at[4], mix_recv.at[4], dev_c)

    local[0].wait()
    local[1].wait()
    pl.semaphore_wait(barrier, len(greet))
    for s in range(WINDOW):
        send_x(s).start()
    for k in range(1, blocks):
        coef_to(k).start()
    for j in range(HALVES):
        ag_far(e, j, j).start()

        @pl.when(mid)
        def _():
            ag_near(e, j, j).start()

    local[2].wait()
    local[3].wait()
    own_gu(t).start()
    local[5].wait()
    own_d(t).start()

    @pl.when(end)
    def _():
        d2_own().start()

    local[6].wait()
    norm(mix_raw, mixer_gain, mix_all.at[t], 0, rows)

    @pl.when(rim_source)
    def _():
        rim_to(0).start()

    mix_own(t).start()

    def hidden(home, xq):
        @pl.loop(0, 4)
        def _(j):
            q = 2 * xq + j // 2
            h = j % 2
            both = jnp.dot(tokens[home], w_gu[q, h], preferred_element_type=f32)
            gate, upper = both[:, :ff_half], both[:, ff_half:]
            value = gate / (1.0 + jnp.exp(-gate)) * upper
            hid[home, xq, :, pl.ds(pl.multiple_of(j * ff_half, ff_half), ff_half)] = value.astype(bf16)

    col = 512

    def down(home, xq, first):
        @pl.loop(0, width // col)
        def _(n):
            at = pl.ds(pl.multiple_of(n * col, col), col)
            w = w_d[pl.ds(2 * xq, 2), :, at].reshape(4 * ff_half, col)
            part = jnp.dot(hid[home, xq], w, preferred_element_type=f32)
            if first:
                acc[home, :, at] = part
            else:
                scale = scales[home][:, :1]
                acc[home, :, at] = (acc[home, :, at] + part) * scale

    def pool_in(xq):
        @pl.loop(0, 2)
        def _(j):
            q = 2 * xq + j
            value = jnp.dot(mix_all[q], w_in[...], preferred_element_type=f32)
            pooled_in[pl.ds(pl.multiple_of(rows * (q + 1), rows), rows), :] = value.astype(bf16)

    def wait_fgu():
        for s in range(PIECES_GU):
            got_fx(s).wait_recv()
            got_fy(s).wait_recv()

    def relay_y(s):
        got_y(s).wait_recv()
        send_fy(s).start()

    def gather(f):
        @pl.when(end)
        def _():
            ag_got(mirror(1 + f // 2), f % 2, f).wait_recv()

        if f < 4:

            @pl.when(mid)
            def _():
                home = mirror(2 + f // 2)
                ag_got(home, f % 2, f).wait_recv()
                ag_near(home, f % 2, f + 2).start()

        if f < 2:

            @pl.when(mid)
            def _():
                home = mirror(0)
                ag_got(home, f % 2, 6 + f).wait_recv()
                ag_far(home, f % 2, 2 + f).start()

    for s in range(PIECES):
        got_x(s).wait_recv()
        send_y(s).start()
        send_fx(s).start()
        if s >= PIECES_GU:

            @pl.when(end)
            def _():
                d2_relay(s).start()

        if s + WINDOW == PIECES:

            @pl.when(rim_mine)
            def _():
                rim_to(1).start()

        if s + WINDOW < PIECES:
            send_x(s + WINDOW).start()
        elif s + WINDOW < PIECES + HALVES:
            mix_x(t, s + WINDOW - PIECES).start()
        if s >= LAG:
            relay_y(s - LAG)
        if s in (3, 5, 7, 9, 11):
            gather(s // 2 - 1)
        if s == 2:
            for k in range(1, blocks):
                coef_got(k).wait_recv()
            for home in range(blocks):
                row = coefs[home, pl.ds(e, 1), :]
                scales[home] = jnp.transpose(jnp.broadcast_to(row, (rows, rows)))
        if s == 3:
            own_gu(t_c).wait_recv()
            hidden(e, x)
        if s == 6:

            @pl.when(rim_mine)
            def _():
                rim_to(0).wait_recv()
                rim_to(2).start()

        if s == 4:
            own_d(t_c).wait_recv()
            down(e, x, True)
        if s == 5:
            pooled_in[pl.ds(0, rows), :] = jnp.zeros((rows, group_width), bf16)
        if s == 6:
            hidden(third, x)

            @pl.when(end)
            def _():
                d2_hid(x, 0).start()

        if s == 7:

            @pl.when(mid)
            def _():
                down(third, x, True)

        if s == 8:
            mix_own(t_c).wait_recv()
            local[7].wait()
            pool_in(x)
        if s == 10:
            hidden(mirror(2), x)
            down(mirror(2), x, True)
        if s == 11:
            wait_fgu()
            hidden(third, 1 - x)

            @pl.when(end)
            def _():
                d2_hid(1 - x, 1).start()

    gather(5)
    hidden(mirror(3), x)
    relay_y(PIECES - 3)
    down(mirror(3), x, True)
    relay_y(PIECES - 2)
    hidden(mirror(3), 1 - x)
    relay_y(PIECES - 1)

    @pl.when(mid)
    def _():
        d2_own().wait_recv()
        d2_y(0, True).start()
        d2_c(0, True).start()

    for s in range(PIECES_GU, PIECES):
        got_fx(s).wait_recv()
        got_fy(s).wait_recv()

    def cut(k):
        slot, j = divmod(k, CHUNKS)
        unit = rows // CUTS[slot][-1]
        low, high = CUTS[slot][j], CUTS[slot][j + 1]
        return slot, pl.ds(low * unit, (high - low) * unit)

    def rs_far(k):
        slot, at = cut(k)
        sem = k + 2 * CHUNKS * u
        return rc(rs_stage.at[slot, at, :], rs_in.at[slot + 2 * u, at, :], rs_send.at[k], rs_recv.at[sem], far)

    def rs_near(k):
        slot, at = cut(k)
        sem = 2 * CHUNKS + k
        return rc(rs_stage.at[2, at, :], rs_in.at[2, at, :], rs_send.at[sem], rs_recv.at[sem], near)

    def rs_got(k, base):
        slot, at = cut(k)
        p = rs_in.at[slot + base, at, :]
        return rc(p, p, rs_send.at[0], rs_recv.at[k + base * CHUNKS], far)

    def first_send(home, first):
        @pl.when(end)
        def _():
            for k in range(first, first + CHUNKS):
                slot, at = cut(k)
                rs_stage[slot, at, :] = acc[home, at, :].astype(bf16)
                rs_far(k).start()

    def lead(k):
        @pl.when(mid)
        def _():
            rs_got(k, 0).wait_recv()
            slot, at = cut(k)
            rs_stage[slot, at, :] = (acc[mirror(3 - slot), at, :] + rs_in[slot, at, :].astype(f32)).astype(bf16)
            rs_far(k).start()

    def lag(k):
        @pl.when(mid)
        def _():
            rs_got(k, 2).wait_recv()
            if k < CHUNKS:
                slot, at = cut(k)
                rs_stage[2, at, :] = (acc[mirror(0), at, :] + rs_in[2, at, :].astype(f32)).astype(bf16)
                rs_near(k).start()

    local[8].wait()
    local[9].wait()
    window = 2 + 2 * jnp.minimum(t, 1) + 4 * (t // 2) + 8 * (t // 3)

    def mix_down(j):
        q = (2 * (1 - x) if j < 2 else 2 * x) + (1 - c if j % 2 == 0 else c)
        start = pl.multiple_of(q * rows, rows)
        seg = pooled_in[pl.ds(start, 2 * rows), :]
        i = lax.broadcasted_iota(jnp.int32, (rows, 2 * rows), 0) + rows
        k = lax.broadcasted_iota(jnp.int32, (rows, 2 * rows), 1)
        band = jnp.where((k <= i) & (k > i - window), 1.0, 0.0).astype(bf16)
        sums = jnp.dot(band, seg, preferred_element_type=f32)
        place = lax.broadcasted_iota(jnp.int32, (rows, 1), 0) + (e * blocks + q) * rows + 1
        counts = jnp.minimum(place, window).astype(f32)
        pooled = (sums / counts - seg[rows:, :].astype(f32)).astype(bf16)
        grouped = jnp.dot(pooled, w_group[...], preferred_element_type=f32)
        grouped = (grouped * channel_scale[...].astype(f32).reshape(1, group_width)).astype(bf16)

        @pl.loop(0, width // col)
        def _(n):
            at = pl.ds(pl.multiple_of(n * col, col), col)
            mix_part[j, :, at] = jnp.dot(grouped, w_out[:, at], preferred_element_type=f32).astype(bf16)

    def pair_to(j):
        return rc(mix_part.at[2 * j], mix_pair.at[j], mix_send.at[6 + j], mix_recv.at[6 + j], dev_c)

    def cross(j):
        at = pl.ds(j * half_rows, half_rows)
        return rc(mix_stage.at[at, :], mix_far.at[at, :], mix_send.at[8 + j], mix_recv.at[8 + j], dev_x)

    def mix_relay(j):
        mix_x(t_x, j).wait_recv()
        mix_fwd(t_x, j).start()

    def final(k):
        @pl.when(mid)
        def _():
            _, at = cut(CHUNKS + k)
            expert_out[at, :] = (acc[e, at, :] + rs_in[3, at, :].astype(f32)).astype(bf16)

        @pl.when(end)
        def _():
            _, at = cut(k)
            rs_got(k, 2).wait_recv()
            expert_out[at, :] = (acc[e, at, :] + rs_in[2, at, :].astype(f32)).astype(bf16)

    down(mirror(3), 1 - x, False)
    first_send(mirror(3), 0)
    hidden(mirror(2), 1 - x)
    lead(0)
    down(mirror(2), 1 - x, False)
    first_send(mirror(2), CHUNKS)
    mix_relay(0)
    lead(1)

    @pl.when(mid)
    def _():
        down(third, 1 - x, False)
        for s in range(PIECES_GU, PIECES):
            d2_relay(s).wait_recv()
        d2_y(1, True).start()
        d2_c(1, True).start()

    @pl.when(rim_relay)
    def _():
        rim_to(1).wait_recv()
        rim_to(2).start()

    mix_relay(1)
    lead(2)
    for j in range(HALVES):
        mix_fwd(t_d, j).wait_recv()
    pool_in(1 - x)

    @pl.when(rim_last)
    def _():
        rim_to(2).wait_recv()

    @pl.when(e > 0)
    def _():
        value = jnp.dot(rim_rows[...], w_in[...], preferred_element_type=f32)
        pooled_in[pl.ds(rows - rim_rows.shape[0], rim_rows.shape[0]), :] = value.astype(bf16)

    mix_down(0)
    pair_to(0).start()
    lead(3)
    mix_down(1)
    pair_to(0).wait_recv()
    for j in range(HALVES):
        at = pl.ds(j * half_rows, half_rows)
        mix_stage[at, :] = (mix_part[1, at, :].astype(f32) + mix_pair[0, at, :].astype(f32)).astype(bf16)
        cross(j).start()
    lag(0)
    lag(1)
    lag(2)
    lead(4)

    @pl.when(mid)
    def _():
        d2_y(0, False).wait_recv()
        d2_c(2, True).start()

    lag(3)
    hidden(e, 1 - x)
    lead(5)
    down(e, 1 - x, False)
    lag(4)
    mix_down(2)
    pair_to(1).start()
    lead(6)
    lag(5)
    mix_down(3)
    lead(7)
    lag(6)

    @pl.when(mid)
    def _():
        d2_y(1, False).wait_recv()
        d2_c(3, True).start()

    lead(8)
    lead(9)

    @pl.when(mid)
    def _():
        scales[0] = jnp.transpose(jnp.broadcast_to(coefs[e, pl.ds(mirror(0), 1), :], (rows, rows)))
        d2_hid(x, 0).wait_recv()
        d2_hid(1 - x, 1).wait_recv()
        for k in range(4):
            d2_c(k, False).wait_recv()

        @pl.loop(0, width // col)
        def _(n):
            at = pl.ds(pl.multiple_of(n * col, col), col)
            part = acc[e, :, at]
            scale = scales[0][:, :1]
            for xq in range(2):
                w = w_d2[pl.ds(2 * xq, 2), :, at].reshape(4 * ff_half, col)
                part = part + jnp.dot(hid_far[xq], w, preferred_element_type=f32) * scale
            acc[e, :, at] = part

    final(0)
    final(1)
    lag(7)
    final(2)
    pair_to(1).wait_recv()
    for j in range(HALVES):
        at = pl.ds(j * half_rows, half_rows)
        cross(j).wait_recv()
        mixed_out[at, :] = (
            mix_part[3, at, :].astype(f32) + mix_pair[1, at, :].astype(f32) + mix_far[at, :].astype(f32)
        ).astype(bf16)
    for s in range(PIECES):
        send_x(s).wait_send()
        send_y(s).wait_send()
        send_fx(s).wait_send()
        send_fy(s).wait_send()
    own_gu(t).wait_send()
    own_d(t).wait_send()
    for k in range(1, blocks):
        coef_to(k).wait_send()
    for j in range(HALVES):
        ag_far(e, j, j).wait_send()
        mix_x(t, j).wait_send()
        mix_fwd(t_x, j).wait_send()
        pair_to(j).wait_send()
        cross(j).wait_send()
    mix_own(t).wait_send()

    @pl.when(rim_source)
    def _():
        rim_to(0).wait_send()

    @pl.when(rim_mine)
    def _():
        rim_to(1).wait_send()
        rim_to(2).wait_send()

    @pl.when(rim_relay)
    def _():
        rim_to(2).wait_send()

    @pl.when(end)
    def _():
        d2_own().wait_send()
        d2_hid(x, 0).wait_send()
        d2_hid(1 - x, 1).wait_send()
        for s in range(PIECES_GU, PIECES):
            d2_relay(s).wait_send()

    @pl.when(mid)
    def _():
        for f in range(6):
            ag_near(e, f % 2, f).wait_send()
        for f in range(2):
            ag_far(e, f, 2 + f).wait_send()
        for k in range(2):
            d2_y(k, True).wait_send()
        for k in range(4):
            d2_c(k, True).wait_send()

    lag(8)
    final(3)
    lag(9)
    final(4)
    for k in range(2 * CHUNKS):
        rs_far(k).wait_send()

    @pl.when(mid)
    def _():
        for k in range(CHUNKS):
            rs_near(k).wait_send()


def fused(*args):
    (mixer_tokens, _, in_weight, group_weight, _, out_weight, _, _, route_ids, _, gate_weight, _, _) = args
    rows, width = mixer_tokens.shape
    group_width = in_weight.shape[1]
    ff = gate_weight.shape[2]
    blocks = lax.axis_size("ep")
    parts = lax.axis_size("tp")
    half = rows // HALVES
    bf16, f32 = jnp.bfloat16, jnp.float32
    vmem = pltpu.VMEM
    dma = pltpu.SemaphoreType.DMA
    anyspace = pl.BlockSpec(memory_space=pl.ANY)
    local_spec = pl.BlockSpec(memory_space=pltpu.VMEM)
    args = list(args)
    for i in (8, 9):
        args[i] = args[i].T
    small = (1, 4, 7, 8, 9)
    scratch = [
        vmem((rows, width), bf16),
        vmem((rows, width), bf16),
        vmem((width, group_width), bf16),
        vmem((group_width, group_width), bf16),
        vmem((group_width, width), bf16),
        vmem((parts, 2, width, ff), bf16),
        vmem((parts, ff, width), bf16),
        vmem((blocks, rows, width), bf16),
        vmem((blocks, 8, rows), f32),
        vmem((blocks, rows, rows), f32),
        vmem((blocks, 2, rows, 2 * ff), bf16),
        vmem((blocks, rows, width), f32),
        vmem((4, rows, width), bf16),
        vmem((3, rows, width), bf16),
        vmem((parts, rows, width), bf16),
        vmem((rows * (parts + 1), group_width), bf16),
        vmem((parts, rows, width), bf16),
        vmem((2, rows, width), bf16),
        vmem((rows, width), bf16),
        vmem((rows, width), bf16),
        vmem((WINDOW_MAX, width), bf16),
        vmem((parts, ff, width), bf16),
        vmem((2, rows, 2 * ff), bf16),
        dma((10,)),
    ]
    for count in (PIECES, PIECES, PIECES, PIECES, 2, 2, PIECES, PIECES, PIECES, PIECES, 10, 8, 3, 3, 3 * CHUNKS, 4 * CHUNKS, 10, 10, 3, 3, 14, 14):
        scratch.append(dma((count,)))
    shape = vmem((rows, width), bf16)
    return pl.pallas_call(
        fused_kernel,
        out_shape=(shape, shape),
        in_specs=[local_spec if i in small else anyspace for i in range(len(args))],
        out_specs=(local_spec, local_spec),
        scratch_shapes=scratch,
        compiler_params=pltpu.CompilerParams(
            collective_id=0, has_side_effects=True, vmem_limit_bytes=60 << 20
        ),
        name="fused",
    )(*args)


def fits(mesh):
    sizes = dict(mesh.shape)
    return sizes["grp"] == 2 and sizes["ep"] == 4 and sizes["tp"] == 4


def solution(mesh):
    placed = (
        P(("grp", "ep", "tp"), None),
        P(),
        P(None, "tp"),
        P("tp", None, None),
        P("tp"),
        P("tp", None),
        P(("grp", "ep", "tp"), None),
        P(),
        P(("grp", "ep", "tp"), None),
        P(("grp", "ep", "tp"), None),
        P("ep", None, "tp"),
        P("ep", None, "tp"),
        P("ep", "tp", None),
    )
    return jax.shard_map(
        fused if fits(mesh) else local,
        mesh=mesh,
        in_specs=placed,
        out_specs=(P(("grp", "ep", "tp"), None), P(("grp", "ep", "tp"), None)),
        check_vma=False,
    )
```

```python
import jax
import jax.numpy as jnp
from jax import lax
from jax.experimental import pallas as pl
from jax.experimental.pallas import tpu as pltpu
from jax.sharding import PartitionSpec as P

WINDOW_MAX = 16


def shifted(value, axis, by):
    devices = lax.axis_size(axis)
    pairs = [(i, i + by) for i in range(devices) if 0 <= i + by < devices]
    return lax.ppermute(value, axis, pairs)


def turned(value, axis, by):
    devices = lax.axis_size(axis)
    if by % devices == 0:
        return value
    return lax.ppermute(value, axis, [(i, (i + by) % devices) for i in range(devices)])


def rms_rows(rows, gain):
    values = rows.astype(jnp.float32)
    scaled = values * lax.rsqrt(jnp.mean(values * values, axis=-1, keepdims=True) + 1e-06)
    return (scaled * gain.astype(jnp.float32)).astype(jnp.bfloat16)


def expert_hidden(rows, w_gate, w_up):
    gate = jnp.dot(rows, w_gate, preferred_element_type=jnp.float32)
    upper = jnp.dot(rows, w_up, preferred_element_type=jnp.float32)
    return (jax.nn.silu(gate) * upper).astype(jnp.bfloat16)


def local(
    mixer_tokens,
    mixer_gain,
    in_weight,
    group_weight,
    channel_scale,
    out_weight,
    expert_tokens,
    expert_gain,
    route_ids,
    route_weights,
    gate_weight,
    up_weight,
    down_weight,
):
    normed = rms_rows(mixer_tokens, mixer_gain)
    expert_in = rms_rows(expert_tokens, expert_gain)
    shares = route_weights / jnp.sum(route_weights, axis=1, keepdims=True)
    rows_here, top_k = route_ids.shape
    width = expert_in.shape[1]
    n_experts = lax.axis_size("ep") * gate_weight.shape[0]
    capacity = 4 * rows_here // n_experts
    dense = capacity >= rows_here
    parts_tp = lax.axis_size("tp")
    if dense:
        both = lax.all_gather(jnp.concatenate([normed, expert_in], axis=0), "tp", axis=0, tiled=True)
        both = both.reshape(parts_tp, 2, rows_here, width)
        every = both[:, 0].reshape(parts_tp * rows_here, width)
        own = both[:, 1].reshape(parts_tp * rows_here, width)
    else:
        every = lax.all_gather(normed, "tp", axis=0, tiled=True)
    pooled_in = jnp.dot(
        every,
        in_weight,
        preferred_element_type=jnp.float32,
    ).astype(jnp.bfloat16)
    block_rows = pooled_in.shape[0]
    rim_rows = shifted(pooled_in[block_rows - WINDOW_MAX :], "ep", 1)
    values = pooled_in.astype(jnp.float32)
    extended = jnp.concatenate([rim_rows.astype(jnp.float32), values], axis=0)
    window = jnp.left_shift(jnp.int32(2), lax.axis_index("tp"))
    sums = extended
    span = 1
    total = jnp.zeros_like(values)
    for level in range(WINDOW_MAX.bit_length() - 1):
        sums = sums[span:] + sums[:-span]
        span = span * 2
        total = total + jnp.where(window == span, sums[sums.shape[0] - block_rows :], 0.0)
    positions = lax.axis_index("ep") * block_rows + lax.iota(jnp.int32, block_rows) + 1
    counts = jnp.minimum(positions, window).astype(jnp.float32)
    pooled = (total / counts[:, None] - values).astype(jnp.bfloat16)
    grouped = (
        jnp.dot(pooled, group_weight[0], preferred_element_type=jnp.float32)
        * channel_scale.astype(jnp.float32)
    ).astype(jnp.bfloat16)
    mixed_part = jnp.dot(grouped, out_weight, preferred_element_type=jnp.float32).astype(
        jnp.bfloat16
    )
    if dense:
        experts = jnp.arange(n_experts, dtype=jnp.int32)
        named = (route_ids[:, :, None] == experts[None, None, :]).astype(jnp.float32)
        coefs = jnp.sum(named * shares[:, :, None], axis=1)
        coefs = lax.all_gather(coefs, ("ep", "tp"), axis=0, tiled=True)
        blocks = lax.axis_size("ep")
        here = lax.axis_index("ep")
        mine = (experts == here).astype(jnp.float32)
        coef = jnp.sum(coefs * mine[None, :], axis=1).reshape(blocks, parts_tp, rows_here)
        order = list(range(1, blocks))

        def scale_of(k):
            return lax.dynamic_index_in_dim(coef, lax.rem(here - k + blocks, blocks), 0, False)

        def expert_part(rows, scale):
            hidden = expert_hidden(rows, gate_weight[0], up_weight[0])
            part = jnp.dot(hidden, down_weight[0], preferred_element_type=jnp.float32)
            return (part * scale.reshape(-1)[:, None]).astype(jnp.bfloat16)

        moved = jnp.concatenate([turned(expert_in, "ep", k) for k in order], axis=0)
        moved, own = lax.optimization_barrier((moved, own))
        own_part = expert_part(own, scale_of(0))
        others = lax.all_gather(moved, "tp", axis=0, tiled=True)
        part = expert_part(others, jnp.stack([scale_of(k) for k in order], axis=1))
        back = lax.psum_scatter(part, "tp", scatter_dimension=0, tiled=True)
        back = back.reshape(blocks - 1, rows_here, width)
        pair = jnp.stack(
            [value.reshape(parts_tp, rows_here, width) for value in (mixed_part, own_part)], axis=1
        ).reshape(2 * parts_tp * rows_here, width)
        pair = lax.psum_scatter(pair, "tp", scatter_dimension=0, tiled=True)
        total = pair[rows_here:].astype(jnp.float32)
        for i, k in enumerate(order):
            total = total + turned(back[i], "ep", -k).astype(jnp.float32)
        return (pair[:rows_here], total.astype(jnp.bfloat16))
    mixed_tokens = lax.psum_scatter(mixed_part, "tp", scatter_dimension=0, tiled=True)
    flat_ids = route_ids.reshape(rows_here * top_k)
    one_hot = (flat_ids[:, None] == jnp.arange(n_experts, dtype=jnp.int32)[None, :]).astype(
        jnp.int32
    )
    before = jnp.cumsum(one_hot, axis=0) - one_hot
    slots = jnp.sum(before * one_hot, axis=1)
    targets = flat_ids * capacity + slots
    placement = (
        targets.reshape(rows_here, top_k)[None, :, :]
        == jnp.arange(n_experts * capacity, dtype=jnp.int32)[:, None, None]
    )
    dispatch = jnp.any(placement, axis=2).astype(jnp.bfloat16)
    outgoing = jnp.dot(dispatch, expert_in, preferred_element_type=jnp.float32).astype(jnp.bfloat16)
    outgoing = outgoing.reshape(n_experts, capacity, width)
    arrived = lax.all_to_all(outgoing, "ep", split_axis=0, concat_axis=0, tiled=True)
    sources, held, _ = arrived.shape
    flat = arrived.reshape(sources * held, width)
    hidden = expert_hidden(
        lax.all_gather(flat, "tp", axis=0, tiled=True), gate_weight[0], up_weight[0]
    )
    rows = hidden
    summed = lax.psum_scatter(
        jnp.dot(rows, down_weight[0], preferred_element_type=jnp.float32).astype(jnp.bfloat16),
        "tp",
        scatter_dimension=0,
        tiled=True,
    ).astype(jnp.float32)
    expert_out = lax.all_to_all(
        summed.reshape(sources, held, width).astype(jnp.bfloat16),
        "ep",
        split_axis=0,
        concat_axis=0,
        tiled=True,
    ).astype(jnp.float32)
    flat_out = expert_out.reshape(n_experts * capacity, width)
    picked = jnp.take(flat_out, targets, axis=0).reshape(rows_here, top_k, width)
    expert_mix = jnp.sum(picked * shares[:, :, None], axis=1).astype(jnp.bfloat16)
    return (mixed_tokens, expert_mix)


MESH = pl.DeviceIdType.MESH
GU_CUTS = (0, 1, 2, 4, 6, 8, 10, 12, 14, 16)
PIECES_GU = len(GU_CUTS) - 1
D_CUTS = (0, 2, 4, 5, 6, 8)
PIECES = PIECES_GU + len(D_CUTS) - 1
X_PIECES = PIECES + 1
Y_PIECES = PIECES - 1
WINDOW = 5
LAG = 3
HALVES = 2
CHUNKS = 8


def fused_kernel(
    mixer_tokens,
    mixer_gain,
    in_weight,
    group_weight,
    channel_scale,
    out_weight,
    expert_tokens,
    expert_gain,
    route_ids,
    route_weights,
    gate_weight,
    up_weight,
    down_weight,
    mixed_out,
    expert_out,
    mix_raw,
    exp_raw,
    w_in,
    w_group,
    w_out,
    w_gu,
    w_d,
    tokens,
    coefs,
    scales,
    hid,
    acc,
    rs_in,
    rs_stage,
    mix_all,
    pooled_in,
    mix_part,
    mix_pair,
    mix_stage,
    mix_far,
    rim_rows,
    w_d2,
    hid_far,
    load_sem,
    x_send,
    x_recv,
    y_send,
    y_recv,
    own_send,
    own_recv,
    fx_send,
    fx_recv,
    fy_send,
    fy_recv,
    ag_send,
    ag_recv,
    coef_send,
    coef_recv,
    rs_send,
    rs_recv,
    mix_send,
    mix_recv,
    rim_send,
    rim_recv,
    d2_send,
    d2_recv,
):
    f32, bf16 = jnp.float32, jnp.bfloat16
    rows, width = exp_raw.shape
    half_rows = rows // HALVES
    group_width = w_group.shape[0]
    ff_half = w_d.shape[1] // 2
    blocks = tokens.shape[0]
    parts = mix_all.shape[0]
    g = lax.axis_index("grp")
    e = lax.axis_index("ep")
    t = lax.axis_index("tp")
    x = t // 2
    c = t % 2
    t_c = 2 * x + 1 - c
    t_x = 2 * (1 - x) + c
    t_d = 2 * (1 - x) + 1 - c
    dev_c, dev_x, dev_y = (g, e, t_c), (g, e, t_x), (1 - g, e, t)
    hi = e // 2
    sign = 1 - 2 * hi
    last = blocks - 1

    def mirror(m):
        return hi * last + sign * m

    u = mirror(e)
    end = u == 0
    mid = u == 1
    far = (g, lax.rem(e + sign + blocks, blocks), t)
    near = (g, lax.rem(e - sign + blocks, blocks), t)
    third = mirror(1 - u)

    def rc(src, dst, send, recv, dev):
        return pltpu.make_async_remote_copy(
            src_ref=src, dst_ref=dst, send_sem=send, recv_sem=recv, device_id=dev, device_id_type=MESH
        )

    barrier = pltpu.get_barrier_semaphore()
    for dev in (dev_c, dev_x, dev_y):
        pl.semaphore_signal(barrier, inc=1, device_id=dev, device_id_type=MESH)

    @pl.when(e < last)
    def _():
        dev = (g, lax.rem(e + 1, blocks), t)
        pl.semaphore_signal(barrier, inc=1, device_id=dev, device_id_type=MESH)

    @pl.when(e > 0)
    def _():
        dev = (g, lax.rem(e - 1 + blocks, blocks), t)
        pl.semaphore_signal(barrier, inc=1, device_id=dev, device_id_type=MESH)

    def loads():
        out = []
        for h in range(2):
            hh = g if h == 0 else 1 - g
            lane = pl.multiple_of(hh * ff_half, ff_half)
            out.append((gate_weight.at[0, :, pl.ds(lane, ff_half)], w_gu.at[t, hh, :, pl.ds(0, ff_half)]))
            out.append((up_weight.at[0, :, pl.ds(lane, ff_half)], w_gu.at[t, hh, :, pl.ds(ff_half, ff_half)]))
            if h == 0:
                out.append((expert_tokens, exp_raw))
        out.append((down_weight.at[0], w_d.at[t]))
        out.append((mixer_tokens, mix_raw))
        out.append((in_weight, w_in))
        out.append((group_weight.at[0], w_group))
        out.append((out_weight, w_out))
        return [pltpu.make_async_copy(a, b, load_sem.at[i]) for i, (a, b) in enumerate(out)]

    local = loads()
    for copy in local:
        copy.start()
    def norm(raw, gain, dst, start, count):
        step = 32
        gain_row = gain[...].astype(f32).reshape(1, width)

        @pl.loop(0, count // step)
        def _(i):
            at = pl.ds(pl.multiple_of(start + i * step, step), step)
            values = raw[at, :].astype(f32)
            scaled = values * lax.rsqrt(jnp.mean(values * values, axis=-1, keepdims=True) + 1e-06)
            dst[at, :] = (scaled * gain_row).astype(bf16)

    ids = route_ids[...]
    weights = route_weights[...]
    shares = weights / jnp.sum(weights, axis=0, keepdims=True)
    numbers = lax.broadcasted_iota(jnp.int32, coefs.shape[1:], 0)
    coef = jnp.zeros(coefs.shape[1:], f32)
    for k in range(ids.shape[0]):
        coef = coef + jnp.where(ids[k : k + 1, :] == numbers, shares[k : k + 1, :], 0.0)
    coefs[e] = coef

    def d_cut(s):
        unit = ff_half // D_CUTS[-1]
        low, high = D_CUTS[s - PIECES_GU], D_CUTS[s - PIECES_GU + 1]
        return low * unit, (high - low) * unit

    def piece(q, h, s):
        if s < PIECES_GU:
            unit = width // GU_CUTS[-1]
            low, high = GU_CUTS[s], GU_CUTS[s + 1]
            return w_gu.at[q, h, pl.ds(low * unit, (high - low) * unit), :]
        start, n = d_cut(s)
        return w_d.at[q, pl.ds(pl.multiple_of(h * ff_half + start, 16), n), :]

    def x_piece(q, s):
        return piece(q, g, s) if s < PIECES else piece(q, 1 - g, PIECES - 1)

    def kind(s):
        return 0 if s < PIECES_GU else 1

    def send_x(s):
        p = x_piece(t, s)
        return rc(p, p, x_send.at[kind(s)], x_recv.at[s], dev_x)

    def got_x(s):
        p = x_piece(t_x, s)
        return rc(p, p, x_send.at[0], x_recv.at[s], dev_x)

    def send_y(s):
        p = piece(t_x, g, s)
        return rc(p, p, y_send.at[kind(s)], y_recv.at[s], dev_y)

    def got_y(s):
        p = piece(t_x, 1 - g, s)
        return rc(p, p, y_send.at[0], y_recv.at[s], dev_y)

    def send_fx(s):
        p = x_piece(t_x, s)
        return rc(p, p, fx_send.at[kind(s)], fx_recv.at[kind(s)], dev_c)

    def send_fy(s):
        p = piece(t_x, 1 - g, s)
        return rc(p, p, fy_send.at[kind(s)], fy_recv.at[kind(s)], dev_c)

    d_last = d_cut(PIECES - 1)
    x_rows, y_rows = ff_half + d_last[1], d_last[0]

    def all_gu(send, recv):
        return rc(w_gu.at[t, g], w_gu.at[t, g], send.at[0], recv.at[0], dev_c)

    def all_d(send, recv, count):
        p = w_d.at[t, pl.ds(0, count), :]
        return rc(p, p, send.at[1], recv.at[1], dev_c)

    def own_gu(q):
        return rc(w_gu.at[q], w_gu.at[q], own_send.at[0], own_recv.at[0], dev_c)

    def own_d(q):
        return rc(w_d.at[q], w_d.at[q], own_send.at[1], own_recv.at[1], dev_c)

    def chunk(home, j):
        return tokens.at[home, pl.ds(j * half_rows, half_rows), :]

    def ag_far(home, j, f):
        p = chunk(home, j)
        return rc(p, p, ag_send.at[0], ag_recv.at[f + 6 * (1 - u)], far)

    def ag_near(home, j, f):
        p = chunk(home, j)
        return rc(p, p, ag_send.at[1], ag_recv.at[f], near)

    def ag_got(home, j, f):
        p = chunk(home, j)
        return rc(p, p, ag_send.at[0], ag_recv.at[f], far)

    rim_source = (t == parts - 1) & (e < last)
    rim_mine = (t == parts - 1) & (e > 0)
    rim_relay = (t == parts // 2 - 1) & (e > 0)
    rim_last = (c == 0) & (e > 0)

    def rim_to(k):
        src = mix_all.at[t, pl.ds(rows - rim_rows.shape[0], rim_rows.shape[0]), :] if k == 0 else rim_rows
        dev = ((g, lax.rem(e + 1, blocks), t), dev_x, dev_c)[k]
        return rc(src, rim_rows, rim_send.at[k], rim_recv.at[k], dev)

    def coef_far(home, k):
        return rc(coefs.at[home], coefs.at[home], coef_send.at[0], coef_recv.at[k + 3 * (1 - u)], far)

    def coef_near(home, k):
        return rc(coefs.at[home], coefs.at[home], coef_send.at[1], coef_recv.at[k], near)

    def coef_got(home, k):
        return rc(coefs.at[home], coefs.at[home], coef_send.at[0], coef_recv.at[k], far)

    def d2_half(ref, q, h):
        return ref.at[q, pl.ds(pl.multiple_of(h * ff_half, ff_half), ff_half), :]

    def d2_piece(ref, s):
        start, n = d_cut(s)
        return ref.at[t_x, pl.ds(pl.multiple_of(g * ff_half + start, 16), n), :]

    def d2_own():
        return rc(d2_half(w_d, t, g), d2_half(w_d2, t, g), d2_send.at[0], d2_recv.at[0], far)

    def d2_relay(s):
        return rc(d2_piece(w_d, s), d2_piece(w_d2, s), d2_send.at[1], d2_recv.at[1], far)

    def d2_hid(xq):
        return rc(hid.at[third, xq], hid_far.at[xq], d2_send.at[2], d2_recv.at[2], far)

    def d2_y(k, mine):
        p = d2_half(w_d2, t if k == 0 else t_x, g if mine else 1 - g)
        return rc(p, p, d2_send.at[3], d2_recv.at[3 + k], dev_y)

    def d2_c(k):
        p = d2_half(w_d2, t if k % 2 == 0 else t_x, g if k < 2 else 1 - g)
        return rc(p, p, d2_send.at[4], d2_recv.at[5], dev_c)

    def d2_all(k, p):
        return rc(p, p, d2_send.at[k], d2_recv.at[min(k, 2) if k < 4 else 5], dev_c)

    def mix_x(q, j):
        p = mix_all.at[q, pl.ds(j * half_rows, half_rows), :]
        return rc(p, p, mix_send.at[0], mix_recv.at[j], dev_x)

    def mix_fwd(q, j):
        p = mix_all.at[q, pl.ds(j * half_rows, half_rows), :]
        return rc(p, p, mix_send.at[1], mix_recv.at[2], dev_c)

    def mix_own(q):
        return rc(mix_all.at[q], mix_all.at[q], mix_send.at[2], mix_recv.at[3], dev_c)

    local[0].wait()
    local[1].wait()
    @pl.when(end)
    def _():
        pl.semaphore_wait(barrier, 4)

    @pl.when(mid)
    def _():
        pl.semaphore_wait(barrier, 5)

    for s in range(WINDOW):
        send_x(s).start()
    local[2].wait()
    norm(exp_raw, expert_gain, tokens.at[e], 0, rows)
    for j in range(HALVES):
        ag_far(e, j, j).start()
    coef_far(e, 0).start()

    @pl.when(mid)
    def _():
        for j in range(HALVES):
            ag_near(e, j, j).start()
        coef_near(e, 0).start()

    local[3].wait()
    local[4].wait()
    own_gu(t).start()
    local[5].wait()
    own_d(t).start()

    local[6].wait()
    norm(mix_raw, mixer_gain, mix_all.at[t], 0, rows)

    @pl.when(rim_source)
    def _():
        rim_to(0).start()

    @pl.when(end)
    def _():
        d2_own().start()

    mix_own(t).start()

    whole = pl.ds(0, rows)
    part_of = [pl.ds(j * half_rows, half_rows) for j in range(HALVES)]

    def hidden(home, xq, at=whole):
        @pl.loop(0, 4)
        def _(j):
            q = 2 * xq + j // 2
            h = j % 2
            both = jnp.dot(tokens[home, at, :], w_gu[q, h], preferred_element_type=f32)
            gate, upper = both[:, :ff_half], both[:, ff_half:]
            value = gate / (1.0 + jnp.exp(-gate)) * upper
            hid[home, xq, at, pl.ds(pl.multiple_of(j * ff_half, ff_half), ff_half)] = value.astype(bf16)

    col = 512

    def down(home, xq, first, at=whole):
        @pl.loop(0, width // col)
        def _(n):
            cols = pl.ds(pl.multiple_of(n * col, col), col)
            w = w_d[pl.ds(2 * xq, 2), :, cols].reshape(4 * ff_half, col)
            part = jnp.dot(hid[home, xq, at, :], w, preferred_element_type=f32)
            if first:
                acc[home, at, cols] = part
            else:
                scale = scales[home, at, :][:, :1]
                acc[home, at, cols] = (acc[home, at, cols] + part) * scale

    def pool_in(xq):
        @pl.loop(0, 2)
        def _(j):
            q = 2 * xq + j
            value = jnp.dot(mix_all[q], w_in[...], preferred_element_type=f32)
            pooled_in[pl.ds(pl.multiple_of(rows * (q + 1), rows), rows), :] = value.astype(bf16)

    def wait_fgu():
        all_gu(fx_send, fx_recv).wait_recv()
        all_gu(fy_send, fy_recv).wait_recv()

    def relay_y(s):
        got_y(s).wait_recv()
        send_fy(s).start()

    def gather(f):
        @pl.when(end)
        def _():
            home = mirror(1 + f // 2)
            ag_got(home, f % 2, f).wait_recv()
            if f % 2 == 1:
                coef_got(home, f // 2).wait_recv()

        if f < 4:

            @pl.when(mid)
            def _():
                home = mirror(2 + f // 2)
                ag_got(home, f % 2, f).wait_recv()
                ag_near(home, f % 2, f + 2).start()
                if f % 2 == 1:
                    coef_got(home, f // 2).wait_recv()
                    coef_near(home, f // 2 + 1).start()

        if f < 2:

            @pl.when(mid)
            def _():
                home = mirror(0)
                ag_got(home, f % 2, 6 + f).wait_recv()
                ag_far(home, f % 2, 2 + f).start()
                if f % 2 == 1:
                    coef_got(home, 3).wait_recv()
                    coef_far(home, 1).start()

    def scale_of(home):
        scales[home] = jnp.transpose(jnp.broadcast_to(coefs[home, pl.ds(e, 1), :], (rows, rows)))

    for s in range(X_PIECES):
        got_x(s).wait_recv()
        if s < Y_PIECES:
            send_y(s).start()
        send_fx(s).start()
        if PIECES_GU <= s < PIECES:

            @pl.when(end)
            def _():
                d2_relay(s).start()

        if s + WINDOW == X_PIECES:

            @pl.when(rim_mine)
            def _():
                rim_to(1).start()

        if s + WINDOW < X_PIECES:
            send_x(s + WINDOW).start()
        elif s + WINDOW < X_PIECES + HALVES:
            mix_x(t, s + WINDOW - X_PIECES).start()
        if s >= LAG:
            relay_y(s - LAG)
        if s in (3, 5, 7, 9, 11):
            gather(s // 2 - 1)
        if s == 3:
            own_gu(t_c).wait_recv()
            hidden(e, x)
        if s == 8:

            @pl.when(rim_mine)
            def _():
                rim_to(0).wait_recv()
                rim_to(2).start()

        if s == 4:
            own_d(t_c).wait_recv()
            down(e, x, True)
        if s == 5:
            pooled_in[pl.ds(0, rows), :] = jnp.zeros((rows, group_width), bf16)
        if s == 6:
            hidden(third, x)

            @pl.when(end)
            def _():
                d2_hid(x).start()

        if s == 7:

            @pl.when(mid)
            def _():
                down(third, x, True)

        if s == 8:
            mix_own(t_c).wait_recv()
            local[7].wait()
            pool_in(x)
        if s == 10:
            hidden(mirror(2), x)
            down(mirror(2), x, True)
        if s == 11:
            hidden(mirror(3), x, part_of[0])
        if s == 12:
            wait_fgu()
            hidden(third, 1 - x)

            @pl.when(end)
            def _():
                d2_hid(1 - x).start()

        if s == Y_PIECES:

            @pl.when(mid)
            def _():
                d2_own().wait_recv()
                d2_y(0, True).start()
                d2_c(0).start()

            hidden(mirror(3), 1 - x, part_of[0])

    for s in range(X_PIECES - LAG, Y_PIECES):
        relay_y(s)
    down(mirror(3), x, True, part_of[0])
    gather(5)
    for home in range(blocks):
        scale_of(home)
    all_d(fx_send, fx_recv, x_rows).wait_recv()
    all_d(fy_send, fy_recv, y_rows).wait_recv()

    def cut(k):
        slot, j = divmod(k, CHUNKS)
        return slot, pl.ds(j * (rows // CHUNKS), rows // CHUNKS)

    def rs_far(k):
        slot, at = cut(k)
        sem = k + 2 * CHUNKS * u
        return rc(rs_stage.at[slot, at, :], rs_in.at[slot + 2 * u, at, :], rs_send.at[0], rs_recv.at[sem], far)

    def rs_near(k):
        slot, at = cut(k)
        sem = 2 * CHUNKS + k
        return rc(rs_stage.at[2, at, :], rs_in.at[2, at, :], rs_send.at[1], rs_recv.at[sem], near)

    def rs_got(k, base):
        slot, at = cut(k)
        p = rs_in.at[slot + base, at, :]
        return rc(p, p, rs_send.at[0], rs_recv.at[k + base * CHUNKS], far)

    def first_send(home, first, count=CHUNKS):
        @pl.when(end)
        def _():
            for k in range(first, first + count):
                slot, at = cut(k)
                rs_stage[slot, at, :] = acc[home, at, :].astype(bf16)
                rs_far(k).start()

    def lead(k):
        @pl.when(mid)
        def _():
            rs_got(k, 0).wait_recv()
            slot, at = cut(k)
            rs_stage[slot, at, :] = (acc[mirror(3 - slot), at, :] + rs_in[slot, at, :].astype(f32)).astype(bf16)
            rs_far(k).start()

    def lag(k):
        @pl.when(mid)
        def _():
            rs_got(k, 2).wait_recv()
            if k < CHUNKS:
                slot, at = cut(k)
                rs_stage[2, at, :] = (acc[mirror(0), at, :] + rs_in[2, at, :].astype(f32)).astype(bf16)
                rs_near(k).start()

    local[8].wait()
    local[9].wait()
    window = 2 + 2 * jnp.minimum(t, 1) + 4 * (t // 2) + 8 * (t // 3)

    def mix_down(j):
        q = (2 * (1 - x) if j < 2 else 2 * x) + (1 - c if j % 2 == 0 else c)
        start = pl.multiple_of(q * rows, rows)
        seg = pooled_in[pl.ds(start, 2 * rows), :]
        i = lax.broadcasted_iota(jnp.int32, (rows, 2 * rows), 0) + rows
        k = lax.broadcasted_iota(jnp.int32, (rows, 2 * rows), 1)
        band = jnp.where((k <= i) & (k > i - window), 1.0, 0.0).astype(bf16)
        sums = jnp.dot(band, seg, preferred_element_type=f32)
        place = lax.broadcasted_iota(jnp.int32, (rows, 1), 0) + (e * blocks + q) * rows + 1
        counts = jnp.minimum(place, window).astype(f32)
        pooled = (sums / counts - seg[rows:, :].astype(f32)).astype(bf16)
        grouped = jnp.dot(pooled, w_group[...], preferred_element_type=f32)
        grouped = (grouped * channel_scale[...].astype(f32).reshape(1, group_width)).astype(bf16)

        @pl.loop(0, width // col)
        def _(n):
            at = pl.ds(pl.multiple_of(n * col, col), col)
            mix_part[j, :, at] = jnp.dot(grouped, w_out[:, at], preferred_element_type=f32).astype(bf16)

    def pair_to(j):
        return rc(mix_part.at[2 * j], mix_pair.at[j], mix_send.at[3], mix_recv.at[4 + j], dev_c)

    def cross(j):
        at = pl.ds(j * half_rows, half_rows)
        return rc(mix_stage.at[at, :], mix_far.at[at, :], mix_send.at[4], mix_recv.at[6 + j], dev_x)

    def mix_relay(j):
        mix_x(t_x, j).wait_recv()
        mix_fwd(t_x, j).start()

    def final(k):
        @pl.when(mid)
        def _():
            _, at = cut(CHUNKS + k)
            expert_out[at, :] = (acc[e, at, :] + rs_in[3, at, :].astype(f32)).astype(bf16)

        @pl.when(end)
        def _():
            _, at = cut(k)
            rs_got(k, 2).wait_recv()
            expert_out[at, :] = (acc[e, at, :] + rs_in[2, at, :].astype(f32)).astype(bf16)

    down(mirror(3), 1 - x, False, part_of[0])
    first_send(mirror(3), 0, CHUNKS // 2)
    hidden(mirror(3), x, part_of[1])
    hidden(mirror(3), 1 - x, part_of[1])
    lead(0)
    down(mirror(3), x, True, part_of[1])
    lead(1)
    down(mirror(3), 1 - x, False, part_of[1])
    first_send(mirror(3), CHUNKS // 2, CHUNKS // 2)

    @pl.when(mid)
    def _():
        d2_all(1, d2_half(w_d2, t_x, g)).wait_recv()
        d2_y(1, True).start()
        d2_c(1).start()

    mix_relay(0)
    lead(2)
    hidden(mirror(2), 1 - x)

    @pl.when(rim_relay)
    def _():
        rim_to(1).wait_recv()
        rim_to(2).start()

    lead(3)
    down(mirror(2), 1 - x, False)
    first_send(mirror(2), CHUNKS)
    lead(4)
    mix_relay(1)

    @pl.when(mid)
    def _():
        down(third, 1 - x, False)

    mix_all_in = rc(mix_all.at[t_d], mix_all.at[t_d], mix_send.at[1], mix_recv.at[2], dev_c)
    mix_all_in.wait_recv()
    pool_in(1 - x)

    @pl.when(rim_last)
    def _():
        rim_to(2).wait_recv()

    @pl.when(e > 0)
    def _():
        value = jnp.dot(rim_rows[...], w_in[...], preferred_element_type=f32)
        pooled_in[pl.ds(rows - rim_rows.shape[0], rim_rows.shape[0]), :] = value.astype(bf16)

    lead(5)
    lag(0)
    mix_down(0)
    pair_to(0).start()
    lead(6)
    lag(1)
    mix_down(1)
    lead(7)
    lag(2)
    pair_to(0).wait_recv()
    for j in range(HALVES):
        at = pl.ds(j * half_rows, half_rows)
        mix_stage[at, :] = (mix_part[1, at, :].astype(f32) + mix_pair[0, at, :].astype(f32)).astype(bf16)
        cross(j).start()
    lead(8)
    lag(3)

    hidden(e, 1 - x)
    lead(9)
    lag(4)

    @pl.when(mid)
    def _():
        d2_y(0, False).wait_recv()
        d2_c(2).start()

    down(e, 1 - x, False)
    lead(10)
    lag(5)
    lead(11)
    lag(6)
    mix_down(2)
    pair_to(1).start()
    lead(12)
    lag(7)
    lead(13)
    mix_down(3)
    lead(14)

    @pl.when(mid)
    def _():
        d2_y(1, False).wait_recv()
        d2_c(3).start()

    lead(15)

    @pl.when(mid)
    def _():
        scales[0] = jnp.transpose(jnp.broadcast_to(coefs[e, pl.ds(mirror(0), 1), :], (rows, rows)))
        d2_all(2, hid_far).wait_recv()
        d2_all(4, w_d2.at[pl.ds(0, 2)]).wait_recv()

        @pl.loop(0, width // col)
        def _(n):
            at = pl.ds(pl.multiple_of(n * col, col), col)
            part = acc[e, :, at]
            scale = scales[0][:, :1]
            for xq in range(2):
                w = w_d2[pl.ds(2 * xq, 2), :, at].reshape(4 * ff_half, col)
                part = part + jnp.dot(hid_far[xq], w, preferred_element_type=f32) * scale
            acc[e, :, at] = part

    for k in range(4):
        lag(CHUNKS + k)
        final(k)
    pair_to(1).wait_recv()
    for j in range(HALVES):
        at = pl.ds(j * half_rows, half_rows)
        cross(j).wait_recv()
        mixed_out[at, :] = (
            mix_part[3, at, :].astype(f32) + mix_pair[1, at, :].astype(f32) + mix_far[at, :].astype(f32)
        ).astype(bf16)

    all_gu(x_send, fx_recv).wait_send()
    all_d(x_send, fx_recv, x_rows).wait_send()
    all_gu(y_send, fx_recv).wait_send()
    all_d(y_send, fx_recv, y_rows).wait_send()
    all_gu(fx_send, fx_recv).wait_send()
    all_d(fx_send, fx_recv, x_rows).wait_send()
    all_gu(fy_send, fx_recv).wait_send()
    all_d(fy_send, fx_recv, y_rows).wait_send()
    own_gu(t).wait_send()
    own_d(t).wait_send()

    def sent(sems, k, p):
        rc(p, p, sems.at[k], mix_recv.at[0], dev_c).wait_send()

    sent(mix_send, 0, mix_all.at[t])
    sent(mix_send, 1, mix_all.at[t])
    sent(mix_send, 2, mix_all.at[t])
    sent(mix_send, 3, mix_part.at[pl.ds(0, 2)])
    sent(mix_send, 4, mix_stage)

    @pl.when(rim_source)
    def _():
        rim_to(0).wait_send()

    @pl.when(rim_mine)
    def _():
        rim_to(1).wait_send()
        rim_to(2).wait_send()

    @pl.when(rim_relay)
    def _():
        rim_to(2).wait_send()

    @pl.when(end)
    def _():
        sent(ag_send, 0, tokens.at[e])
        sent(coef_send, 0, coefs.at[e])
        d2_own().wait_send()
        sent(d2_send, 1, d2_half(w_d, t_x, g))
        sent(d2_send, 2, hid_far)

    @pl.when(mid)
    def _():
        sent(ag_send, 0, tokens.at[pl.ds(0, 2)])
        sent(ag_send, 1, tokens.at[pl.ds(0, 3)])
        sent(coef_send, 0, coefs.at[pl.ds(0, 2)])
        sent(coef_send, 1, coefs.at[pl.ds(0, 3)])
        sent(d2_send, 3, w_d2.at[0])
        sent(d2_send, 4, w_d2.at[pl.ds(0, 2)])
        sent(rs_send, 1, rs_stage.at[2])

    for k in range(4, CHUNKS):
        lag(CHUNKS + k)
        final(k)
    sent(rs_send, 0, rs_stage.at[pl.ds(0, 2)])


def fused(*args):
    (mixer_tokens, _, in_weight, group_weight, _, out_weight, _, _, route_ids, _, gate_weight, _, _) = args
    rows, width = mixer_tokens.shape
    group_width = in_weight.shape[1]
    ff = gate_weight.shape[2]
    blocks = lax.axis_size("ep")
    parts = lax.axis_size("tp")
    half = rows // HALVES
    bf16, f32 = jnp.bfloat16, jnp.float32
    vmem = pltpu.VMEM
    dma = pltpu.SemaphoreType.DMA
    anyspace = pl.BlockSpec(memory_space=pl.ANY)
    local_spec = pl.BlockSpec(memory_space=pltpu.VMEM)
    args = list(args)
    for i in (8, 9):
        args[i] = args[i].T
    small = (1, 4, 7, 8, 9)
    scratch = [
        vmem((rows, width), bf16),
        vmem((rows, width), bf16),
        vmem((width, group_width), bf16),
        vmem((group_width, group_width), bf16),
        vmem((group_width, width), bf16),
        vmem((parts, 2, width, ff), bf16),
        vmem((parts, ff, width), bf16),
        vmem((blocks, rows, width), bf16),
        vmem((blocks, 8, rows), f32),
        vmem((blocks, rows, rows), f32),
        vmem((blocks, 2, rows, 2 * ff), bf16),
        vmem((blocks, rows, width), f32),
        vmem((4, rows, width), bf16),
        vmem((3, rows, width), bf16),
        vmem((parts, rows, width), bf16),
        vmem((rows * (parts + 1), group_width), bf16),
        vmem((parts, rows, width), bf16),
        vmem((2, rows, width), bf16),
        vmem((rows, width), bf16),
        vmem((rows, width), bf16),
        vmem((WINDOW_MAX, width), bf16),
        vmem((parts, ff, width), bf16),
        vmem((2, rows, 2 * ff), bf16),
        dma((10,)),
    ]
    for count in (2, X_PIECES, 2, Y_PIECES, 2, 2, 2, 2, 2, 2, 2, 8, 2, 4, 2, 4 * CHUNKS, 5, 8, 3, 3, 5, 6):
        scratch.append(dma((count,)))
    shape = vmem((rows, width), bf16)
    return pl.pallas_call(
        fused_kernel,
        out_shape=(shape, shape),
        in_specs=[local_spec if i in small else anyspace for i in range(len(args))],
        out_specs=(local_spec, local_spec),
        scratch_shapes=scratch,
        compiler_params=pltpu.CompilerParams(
            collective_id=0, has_side_effects=True, vmem_limit_bytes=60 << 20
        ),
        name="fused",
    )(*args)


def fits(mesh):
    sizes = dict(mesh.shape)
    return sizes["grp"] == 2 and sizes["ep"] == 4 and sizes["tp"] == 4


def solution(mesh):
    placed = (
        P(("grp", "ep", "tp"), None),
        P(),
        P(None, "tp"),
        P("tp", None, None),
        P("tp"),
        P("tp", None),
        P(("grp", "ep", "tp"), None),
        P(),
        P(("grp", "ep", "tp"), None),
        P(("grp", "ep", "tp"), None),
        P("ep", None, "tp"),
        P("ep", None, "tp"),
        P("ep", "tp", None),
    )
    return jax.shard_map(
        fused if fits(mesh) else local,
        mesh=mesh,
        in_specs=placed,
        out_specs=(P(("grp", "ep", "tp"), None), P(("grp", "ep", "tp"), None)),
        check_vma=False,
    )
```

```python
import jax
import jax.numpy as jnp
from jax import lax
from jax.experimental import pallas as pl
from jax.experimental.pallas import tpu as pltpu
from jax.sharding import PartitionSpec as P

WINDOW_MAX = 16


def shifted(value, axis, by):
    devices = lax.axis_size(axis)
    pairs = [(i, i + by) for i in range(devices) if 0 <= i + by < devices]
    return lax.ppermute(value, axis, pairs)


def turned(value, axis, by):
    devices = lax.axis_size(axis)
    if by % devices == 0:
        return value
    return lax.ppermute(value, axis, [(i, (i + by) % devices) for i in range(devices)])


def rms_rows(rows, gain):
    values = rows.astype(jnp.float32)
    scaled = values * lax.rsqrt(jnp.mean(values * values, axis=-1, keepdims=True) + 1e-06)
    return (scaled * gain.astype(jnp.float32)).astype(jnp.bfloat16)


def expert_hidden(rows, w_gate, w_up):
    gate = jnp.dot(rows, w_gate, preferred_element_type=jnp.float32)
    upper = jnp.dot(rows, w_up, preferred_element_type=jnp.float32)
    return (jax.nn.silu(gate) * upper).astype(jnp.bfloat16)


def local(
    mixer_tokens,
    mixer_gain,
    in_weight,
    group_weight,
    channel_scale,
    out_weight,
    expert_tokens,
    expert_gain,
    route_ids,
    route_weights,
    gate_weight,
    up_weight,
    down_weight,
):
    normed = rms_rows(mixer_tokens, mixer_gain)
    expert_in = rms_rows(expert_tokens, expert_gain)
    shares = route_weights / jnp.sum(route_weights, axis=1, keepdims=True)
    rows_here, top_k = route_ids.shape
    width = expert_in.shape[1]
    n_experts = lax.axis_size("ep") * gate_weight.shape[0]
    capacity = 4 * rows_here // n_experts
    dense = capacity >= rows_here
    parts_tp = lax.axis_size("tp")
    if dense:
        both = lax.all_gather(jnp.concatenate([normed, expert_in], axis=0), "tp", axis=0, tiled=True)
        both = both.reshape(parts_tp, 2, rows_here, width)
        every = both[:, 0].reshape(parts_tp * rows_here, width)
        own = both[:, 1].reshape(parts_tp * rows_here, width)
    else:
        every = lax.all_gather(normed, "tp", axis=0, tiled=True)
    pooled_in = jnp.dot(
        every,
        in_weight,
        preferred_element_type=jnp.float32,
    ).astype(jnp.bfloat16)
    block_rows = pooled_in.shape[0]
    rim_rows = shifted(pooled_in[block_rows - WINDOW_MAX :], "ep", 1)
    values = pooled_in.astype(jnp.float32)
    extended = jnp.concatenate([rim_rows.astype(jnp.float32), values], axis=0)
    window = jnp.left_shift(jnp.int32(2), lax.axis_index("tp"))
    sums = extended
    span = 1
    total = jnp.zeros_like(values)
    for level in range(WINDOW_MAX.bit_length() - 1):
        sums = sums[span:] + sums[:-span]
        span = span * 2
        total = total + jnp.where(window == span, sums[sums.shape[0] - block_rows :], 0.0)
    positions = lax.axis_index("ep") * block_rows + lax.iota(jnp.int32, block_rows) + 1
    counts = jnp.minimum(positions, window).astype(jnp.float32)
    pooled = (total / counts[:, None] - values).astype(jnp.bfloat16)
    grouped = (
        jnp.dot(pooled, group_weight[0], preferred_element_type=jnp.float32)
        * channel_scale.astype(jnp.float32)
    ).astype(jnp.bfloat16)
    mixed_part = jnp.dot(grouped, out_weight, preferred_element_type=jnp.float32).astype(
        jnp.bfloat16
    )
    if dense:
        experts = jnp.arange(n_experts, dtype=jnp.int32)
        named = (route_ids[:, :, None] == experts[None, None, :]).astype(jnp.float32)
        coefs = jnp.sum(named * shares[:, :, None], axis=1)
        coefs = lax.all_gather(coefs, ("ep", "tp"), axis=0, tiled=True)
        blocks = lax.axis_size("ep")
        here = lax.axis_index("ep")
        mine = (experts == here).astype(jnp.float32)
        coef = jnp.sum(coefs * mine[None, :], axis=1).reshape(blocks, parts_tp, rows_here)
        order = list(range(1, blocks))

        def scale_of(k):
            return lax.dynamic_index_in_dim(coef, lax.rem(here - k + blocks, blocks), 0, False)

        def expert_part(rows, scale):
            hidden = expert_hidden(rows, gate_weight[0], up_weight[0])
            part = jnp.dot(hidden, down_weight[0], preferred_element_type=jnp.float32)
            return (part * scale.reshape(-1)[:, None]).astype(jnp.bfloat16)

        moved = jnp.concatenate([turned(expert_in, "ep", k) for k in order], axis=0)
        moved, own = lax.optimization_barrier((moved, own))
        own_part = expert_part(own, scale_of(0))
        others = lax.all_gather(moved, "tp", axis=0, tiled=True)
        part = expert_part(others, jnp.stack([scale_of(k) for k in order], axis=1))
        back = lax.psum_scatter(part, "tp", scatter_dimension=0, tiled=True)
        back = back.reshape(blocks - 1, rows_here, width)
        pair = jnp.stack(
            [value.reshape(parts_tp, rows_here, width) for value in (mixed_part, own_part)], axis=1
        ).reshape(2 * parts_tp * rows_here, width)
        pair = lax.psum_scatter(pair, "tp", scatter_dimension=0, tiled=True)
        total = pair[rows_here:].astype(jnp.float32)
        for i, k in enumerate(order):
            total = total + turned(back[i], "ep", -k).astype(jnp.float32)
        return (pair[:rows_here], total.astype(jnp.bfloat16))
    mixed_tokens = lax.psum_scatter(mixed_part, "tp", scatter_dimension=0, tiled=True)
    flat_ids = route_ids.reshape(rows_here * top_k)
    one_hot = (flat_ids[:, None] == jnp.arange(n_experts, dtype=jnp.int32)[None, :]).astype(
        jnp.int32
    )
    before = jnp.cumsum(one_hot, axis=0) - one_hot
    slots = jnp.sum(before * one_hot, axis=1)
    targets = flat_ids * capacity + slots
    placement = (
        targets.reshape(rows_here, top_k)[None, :, :]
        == jnp.arange(n_experts * capacity, dtype=jnp.int32)[:, None, None]
    )
    dispatch = jnp.any(placement, axis=2).astype(jnp.bfloat16)
    outgoing = jnp.dot(dispatch, expert_in, preferred_element_type=jnp.float32).astype(jnp.bfloat16)
    outgoing = outgoing.reshape(n_experts, capacity, width)
    arrived = lax.all_to_all(outgoing, "ep", split_axis=0, concat_axis=0, tiled=True)
    sources, held, _ = arrived.shape
    flat = arrived.reshape(sources * held, width)
    hidden = expert_hidden(
        lax.all_gather(flat, "tp", axis=0, tiled=True), gate_weight[0], up_weight[0]
    )
    rows = hidden
    summed = lax.psum_scatter(
        jnp.dot(rows, down_weight[0], preferred_element_type=jnp.float32).astype(jnp.bfloat16),
        "tp",
        scatter_dimension=0,
        tiled=True,
    ).astype(jnp.float32)
    expert_out = lax.all_to_all(
        summed.reshape(sources, held, width).astype(jnp.bfloat16),
        "ep",
        split_axis=0,
        concat_axis=0,
        tiled=True,
    ).astype(jnp.float32)
    flat_out = expert_out.reshape(n_experts * capacity, width)
    picked = jnp.take(flat_out, targets, axis=0).reshape(rows_here, top_k, width)
    expert_mix = jnp.sum(picked * shares[:, :, None], axis=1).astype(jnp.bfloat16)
    return (mixed_tokens, expert_mix)


MESH = pl.DeviceIdType.MESH
GU_CUTS = (0, 1, 2, 4, 6, 8, 10, 12, 14, 16)
PIECES_GU = len(GU_CUTS) - 1
D_CUTS = (0, 2, 4, 5, 6, 8)
PIECES = PIECES_GU + len(D_CUTS) - 1
X_PIECES = PIECES + 1
Y_PIECES = PIECES - 1
WINDOW = 5
LAG = 3
HALVES = 2
CHUNKS = 8


def fused_kernel(
    mixer_tokens,
    mixer_gain,
    in_weight,
    group_weight,
    channel_scale,
    out_weight,
    expert_tokens,
    expert_gain,
    route_ids,
    route_weights,
    gate_weight,
    up_weight,
    down_weight,
    mixed_out,
    expert_out,
    mix_raw,
    exp_raw,
    w_in,
    w_group,
    w_out,
    w_gu,
    w_d,
    tokens,
    coefs,
    scales,
    hid,
    acc,
    rs_in,
    rs_stage,
    mix_all,
    pooled_in,
    mix_part,
    mix_pair,
    mix_stage,
    mix_far,
    rim_rows,
    w_d2,
    hid_far,
    load_sem,
    x_send,
    x_recv,
    y_send,
    y_recv,
    own_send,
    own_recv,
    fx_send,
    fx_recv,
    fy_send,
    fy_recv,
    ag_send,
    ag_recv,
    coef_send,
    coef_recv,
    rs_send,
    rs_recv,
    mix_send,
    mix_recv,
    rim_send,
    rim_recv,
    d2_send,
    d2_recv,
):
    f32, bf16 = jnp.float32, jnp.bfloat16
    rows, width = exp_raw.shape
    half_rows = rows // HALVES
    group_width = w_group.shape[0]
    ff_half = w_d.shape[1] // 2
    blocks = tokens.shape[0]
    parts = mix_all.shape[0]
    g = lax.axis_index("grp")
    e = lax.axis_index("ep")
    t = lax.axis_index("tp")
    x = t // 2
    c = t % 2
    t_c = 2 * x + 1 - c
    t_x = 2 * (1 - x) + c
    t_d = 2 * (1 - x) + 1 - c
    dev_c, dev_x, dev_y = (g, e, t_c), (g, e, t_x), (1 - g, e, t)
    hi = e // 2
    sign = 1 - 2 * hi
    last = blocks - 1

    def mirror(m):
        return hi * last + sign * m

    u = mirror(e)
    end = u == 0
    mid = u == 1
    far = (g, lax.rem(e + sign + blocks, blocks), t)
    near = (g, lax.rem(e - sign + blocks, blocks), t)
    third = mirror(1 - u)

    def rc(src, dst, send, recv, dev):
        return pltpu.make_async_remote_copy(
            src_ref=src, dst_ref=dst, send_sem=send, recv_sem=recv, device_id=dev, device_id_type=MESH
        )

    barrier = pltpu.get_barrier_semaphore()
    for dev in (dev_c, dev_x, dev_y):
        pl.semaphore_signal(barrier, inc=1, device_id=dev, device_id_type=MESH)

    @pl.when(e < last)
    def _():
        dev = (g, lax.rem(e + 1, blocks), t)
        pl.semaphore_signal(barrier, inc=1, device_id=dev, device_id_type=MESH)

    @pl.when(e > 0)
    def _():
        dev = (g, lax.rem(e - 1 + blocks, blocks), t)
        pl.semaphore_signal(barrier, inc=1, device_id=dev, device_id_type=MESH)

    def loads():
        out = []
        for h in range(2):
            hh = g if h == 0 else 1 - g
            lane = pl.multiple_of(hh * ff_half, ff_half)
            out.append((gate_weight.at[0, :, pl.ds(lane, ff_half)], w_gu.at[t, hh, :, pl.ds(0, ff_half)]))
            out.append((up_weight.at[0, :, pl.ds(lane, ff_half)], w_gu.at[t, hh, :, pl.ds(ff_half, ff_half)]))
            if h == 0:
                out.append((expert_tokens, exp_raw))
        out.append((down_weight.at[0], w_d.at[t]))
        out.append((mixer_tokens, mix_raw))
        out.append((in_weight, w_in))
        out.append((group_weight.at[0], w_group))
        out.append((out_weight, w_out))
        return [pltpu.make_async_copy(a, b, load_sem.at[i]) for i, (a, b) in enumerate(out)]

    local = loads()
    for copy in local[:3]:
        copy.start()
    def norm(raw, gain, dst, start, count):
        step = 32
        gain_row = gain[...].astype(f32).reshape(1, width)

        @pl.loop(0, count // step)
        def _(i):
            at = pl.ds(pl.multiple_of(start + i * step, step), step)
            values = raw[at, :].astype(f32)
            scaled = values * lax.rsqrt(jnp.mean(values * values, axis=-1, keepdims=True) + 1e-06)
            dst[at, :] = (scaled * gain_row).astype(bf16)

    ids = route_ids[...]
    weights = route_weights[...]
    shares = weights / jnp.sum(weights, axis=0, keepdims=True)
    numbers = lax.broadcasted_iota(jnp.int32, coefs.shape[1:], 0)
    coef = jnp.zeros(coefs.shape[1:], f32)
    for k in range(ids.shape[0]):
        coef = coef + jnp.where(ids[k : k + 1, :] == numbers, shares[k : k + 1, :], 0.0)
    coefs[e] = coef

    def d_cut(s):
        unit = ff_half // D_CUTS[-1]
        low, high = D_CUTS[s - PIECES_GU], D_CUTS[s - PIECES_GU + 1]
        return low * unit, (high - low) * unit

    def piece(q, h, s):
        if s < PIECES_GU:
            unit = width // GU_CUTS[-1]
            low, high = GU_CUTS[s], GU_CUTS[s + 1]
            return w_gu.at[q, h, pl.ds(low * unit, (high - low) * unit), :]
        start, n = d_cut(s)
        return w_d.at[q, pl.ds(pl.multiple_of(h * ff_half + start, 16), n), :]

    def x_piece(q, s):
        return piece(q, g, s) if s < PIECES else piece(q, 1 - g, PIECES - 1)

    def kind(s):
        return 0 if s < PIECES_GU else 1

    def send_x(s):
        p = x_piece(t, s)
        return rc(p, p, x_send.at[kind(s)], x_recv.at[s], dev_x)

    def got_x(s):
        p = x_piece(t_x, s)
        return rc(p, p, x_send.at[0], x_recv.at[s], dev_x)

    def send_y(s):
        p = piece(t_x, g, s)
        return rc(p, p, y_send.at[kind(s)], y_recv.at[s], dev_y)

    def got_y(s):
        p = piece(t_x, 1 - g, s)
        return rc(p, p, y_send.at[0], y_recv.at[s], dev_y)

    def send_fx(s):
        p = x_piece(t_x, s)
        return rc(p, p, fx_send.at[kind(s)], fx_recv.at[kind(s)], dev_c)

    def send_fy(s):
        p = piece(t_x, 1 - g, s)
        return rc(p, p, fy_send.at[kind(s)], fy_recv.at[kind(s)], dev_c)

    d_last = d_cut(PIECES - 1)
    x_rows, y_rows = ff_half + d_last[1], d_last[0]

    def all_gu(send, recv):
        return rc(w_gu.at[t, g], w_gu.at[t, g], send.at[0], recv.at[0], dev_c)

    def all_d(send, recv, count):
        p = w_d.at[t, pl.ds(0, count), :]
        return rc(p, p, send.at[1], recv.at[1], dev_c)

    def own_gu(q):
        return rc(w_gu.at[q], w_gu.at[q], own_send.at[0], own_recv.at[0], dev_c)

    def own_d(q):
        return rc(w_d.at[q], w_d.at[q], own_send.at[1], own_recv.at[1], dev_c)

    def chunk(home, j):
        return tokens.at[home, pl.ds(j * half_rows, half_rows), :]

    def ag_far(home, j, f):
        p = chunk(home, j)
        return rc(p, p, ag_send.at[0], ag_recv.at[f + 6 * (1 - u)], far)

    def ag_near(home, j, f):
        p = chunk(home, j)
        return rc(p, p, ag_send.at[1], ag_recv.at[f], near)

    def ag_got(home, j, f):
        p = chunk(home, j)
        return rc(p, p, ag_send.at[0], ag_recv.at[f], far)

    rim_source = (t == parts - 1) & (e < last)
    rim_mine = (t == parts - 1) & (e > 0)
    rim_relay = (t == parts // 2 - 1) & (e > 0)
    rim_last = (c == 0) & (e > 0)

    def rim_to(k):
        src = mix_all.at[t, pl.ds(rows - rim_rows.shape[0], rim_rows.shape[0]), :] if k == 0 else rim_rows
        dev = ((g, lax.rem(e + 1, blocks), t), dev_x, dev_c)[k]
        return rc(src, rim_rows, rim_send.at[k], rim_recv.at[k], dev)

    def coef_far(home, k):
        return rc(coefs.at[home], coefs.at[home], coef_send.at[0], coef_recv.at[k + 3 * (1 - u)], far)

    def coef_near(home, k):
        return rc(coefs.at[home], coefs.at[home], coef_send.at[1], coef_recv.at[k], near)

    def coef_got(home, k):
        return rc(coefs.at[home], coefs.at[home], coef_send.at[0], coef_recv.at[k], far)

    def d2_half(ref, q, h):
        return ref.at[q, pl.ds(pl.multiple_of(h * ff_half, ff_half), ff_half), :]

    def d2_piece(ref, s):
        start, n = d_cut(s)
        return ref.at[t_x, pl.ds(pl.multiple_of(g * ff_half + start, 16), n), :]

    def d2_own():
        return rc(d2_half(w_d, t, g), d2_half(w_d2, t, g), d2_send.at[0], d2_recv.at[0], far)

    def d2_relay(s):
        return rc(d2_piece(w_d, s), d2_piece(w_d2, s), d2_send.at[1], d2_recv.at[1], far)

    def d2_hid(xq):
        return rc(hid.at[third, xq], hid_far.at[xq], d2_send.at[2], d2_recv.at[2], far)

    def d2_y(k, mine):
        p = d2_half(w_d2, t if k == 0 else t_x, g if mine else 1 - g)
        return rc(p, p, d2_send.at[3], d2_recv.at[3 + k], dev_y)

    def d2_c(k):
        p = d2_half(w_d2, t if k % 2 == 0 else t_x, g if k < 2 else 1 - g)
        return rc(p, p, d2_send.at[4], d2_recv.at[5], dev_c)

    def d2_all(k, p):
        return rc(p, p, d2_send.at[k], d2_recv.at[min(k, 2) if k < 4 else 5], dev_c)

    def mix_x(q, j):
        p = mix_all.at[q, pl.ds(j * half_rows, half_rows), :]
        return rc(p, p, mix_send.at[0], mix_recv.at[j], dev_x)

    def mix_fwd(q, j):
        p = mix_all.at[q, pl.ds(j * half_rows, half_rows), :]
        return rc(p, p, mix_send.at[1], mix_recv.at[2], dev_c)

    def mix_own(q):
        return rc(mix_all.at[q], mix_all.at[q], mix_send.at[2], mix_recv.at[3], dev_c)

    local[0].wait()
    local[1].wait()
    @pl.when(end)
    def _():
        pl.semaphore_wait(barrier, 4)

    @pl.when(mid)
    def _():
        pl.semaphore_wait(barrier, 5)

    for s in range(WINDOW):
        send_x(s).start()
    for copy in local[3:]:
        copy.start()
    local[2].wait()
    norm(exp_raw, expert_gain, tokens.at[e], 0, rows)
    coef_far(e, 0).start()
    for j in range(HALVES):
        ag_far(e, j, j).start()

    @pl.when(mid)
    def _():
        coef_near(e, 0).start()
        for j in range(HALVES):
            ag_near(e, j, j).start()

    local[3].wait()
    local[4].wait()
    own_gu(t).start()
    local[5].wait()
    own_d(t).start()

    local[6].wait()
    norm(mix_raw, mixer_gain, mix_all.at[t], 0, rows)

    @pl.when(rim_source)
    def _():
        rim_to(0).start()

    @pl.when(end)
    def _():
        d2_own().start()

    mix_own(t).start()

    whole = pl.ds(0, rows)
    part_of = [pl.ds(j * half_rows, half_rows) for j in range(HALVES)]

    def hidden(home, xq, at=whole):
        @pl.loop(0, 4)
        def _(j):
            q = 2 * xq + j // 2
            h = j % 2
            both = jnp.dot(tokens[home, at, :], w_gu[q, h], preferred_element_type=f32)
            gate, upper = both[:, :ff_half], both[:, ff_half:]
            value = gate / (1.0 + jnp.exp(-gate)) * upper
            hid[home, xq, at, pl.ds(pl.multiple_of(j * ff_half, ff_half), ff_half)] = value.astype(bf16)

    col = 512

    def down(home, xq, first, at=whole):
        @pl.loop(0, width // col)
        def _(n):
            cols = pl.ds(pl.multiple_of(n * col, col), col)
            w = w_d[pl.ds(2 * xq, 2), :, cols].reshape(4 * ff_half, col)
            part = jnp.dot(hid[home, xq, at, :], w, preferred_element_type=f32)
            if first:
                acc[home, at, cols] = part
            else:
                scale = scales[home, at, :][:, :1]
                acc[home, at, cols] = (acc[home, at, cols] + part) * scale

    def pool_in(xq):
        @pl.loop(0, 2)
        def _(j):
            q = 2 * xq + j
            value = jnp.dot(mix_all[q], w_in[...], preferred_element_type=f32)
            pooled_in[pl.ds(pl.multiple_of(rows * (q + 1), rows), rows), :] = value.astype(bf16)

    def wait_fgu():
        all_gu(fx_send, fx_recv).wait_recv()
        all_gu(fy_send, fy_recv).wait_recv()

    def relay_y(s):
        got_y(s).wait_recv()
        send_fy(s).start()

    def gather(f):
        @pl.when(end)
        def _():
            home = mirror(1 + f // 2)
            ag_got(home, f % 2, f).wait_recv()
            if f % 2 == 0:
                coef_got(home, f // 2).wait_recv()

        if f < 4:

            @pl.when(mid)
            def _():
                home = mirror(2 + f // 2)
                ag_got(home, f % 2, f).wait_recv()
                ag_near(home, f % 2, f + 2).start()
                if f % 2 == 0:
                    coef_got(home, f // 2).wait_recv()
                    coef_near(home, f // 2 + 1).start()

        if f < 2:

            @pl.when(mid)
            def _():
                home = mirror(0)
                ag_got(home, f % 2, 6 + f).wait_recv()
                ag_far(home, f % 2, 2 + f).start()
                if f % 2 == 0:
                    coef_got(home, 3).wait_recv()
                    coef_far(home, 1).start()

    def scale_of(home):
        scales[home] = jnp.transpose(jnp.broadcast_to(coefs[home, pl.ds(e, 1), :], (rows, rows)))

    for s in range(X_PIECES):
        got_x(s).wait_recv()
        if s < Y_PIECES:
            send_y(s).start()
        send_fx(s).start()
        if PIECES_GU <= s < PIECES:

            @pl.when(end)
            def _():
                d2_relay(s).start()

        if s + WINDOW == X_PIECES:

            @pl.when(rim_mine)
            def _():
                rim_to(1).start()

        if s + WINDOW < X_PIECES:
            send_x(s + WINDOW).start()
        elif s + WINDOW < X_PIECES + HALVES:
            mix_x(t, s + WINDOW - X_PIECES).start()
        if s >= LAG:
            relay_y(s - LAG)
        if s in (3, 5, 7, 9, 11):
            gather(s // 2 - 1)
        if s == 3:
            own_gu(t_c).wait_recv()
            hidden(e, x)
        if s == 8:

            @pl.when(rim_mine)
            def _():
                rim_to(0).wait_recv()
                rim_to(2).start()

        if s == 4:
            own_d(t_c).wait_recv()
            down(e, x, True)
        if s == 5:
            pooled_in[pl.ds(0, rows), :] = jnp.zeros((rows, group_width), bf16)
        if s == 6:
            hidden(third, x)

            @pl.when(end)
            def _():
                d2_hid(x).start()

        if s == 7:

            @pl.when(mid)
            def _():
                down(third, x, True)

        if s == 8:
            mix_own(t_c).wait_recv()
            local[7].wait()
            pool_in(x)
        if s == 10:
            hidden(mirror(2), x)
            down(mirror(2), x, True)
        if s == 11:
            hidden(mirror(3), x, part_of[0])
        if s == 12:
            wait_fgu()
            hidden(third, 1 - x)

            @pl.when(end)
            def _():
                d2_hid(1 - x).start()

        if s == Y_PIECES:

            @pl.when(mid)
            def _():
                d2_own().wait_recv()
                d2_y(0, True).start()
                d2_c(0).start()

            hidden(mirror(3), 1 - x, part_of[0])
            down(mirror(3), x, True, part_of[0])
            scale_of(mirror(3))

    for s in range(X_PIECES - LAG, Y_PIECES):
        relay_y(s)
    all_d(fx_send, fx_recv, x_rows).wait_recv()
    all_d(fy_send, fy_recv, y_rows).wait_recv()

    def cut(k):
        slot, j = divmod(k, CHUNKS)
        return slot, pl.ds(j * (rows // CHUNKS), rows // CHUNKS)

    def rs_far(k):
        slot, at = cut(k)
        sem = k + 2 * CHUNKS * u
        return rc(rs_stage.at[slot, at, :], rs_in.at[slot + 2 * u, at, :], rs_send.at[0], rs_recv.at[sem], far)

    def rs_near(k):
        slot, at = cut(k)
        sem = 2 * CHUNKS + k
        return rc(rs_stage.at[2, at, :], rs_in.at[2, at, :], rs_send.at[1], rs_recv.at[sem], near)

    def rs_got(k, base):
        slot, at = cut(k)
        p = rs_in.at[slot + base, at, :]
        return rc(p, p, rs_send.at[0], rs_recv.at[k + base * CHUNKS], far)

    def first_send(home, first, count=CHUNKS):
        @pl.when(end)
        def _():
            for k in range(first, first + count):
                slot, at = cut(k)
                rs_stage[slot, at, :] = acc[home, at, :].astype(bf16)
                rs_far(k).start()

    def lead(k):
        @pl.when(mid)
        def _():
            rs_got(k, 0).wait_recv()
            slot, at = cut(k)
            rs_stage[slot, at, :] = (acc[mirror(3 - slot), at, :] + rs_in[slot, at, :].astype(f32)).astype(bf16)
            rs_far(k).start()

    def lag(k):
        @pl.when(mid)
        def _():
            rs_got(k, 2).wait_recv()
            if k < CHUNKS:
                slot, at = cut(k)
                rs_stage[2, at, :] = (acc[mirror(0), at, :] + rs_in[2, at, :].astype(f32)).astype(bf16)
                rs_near(k).start()

    local[8].wait()
    local[9].wait()
    window = 2 + 2 * jnp.minimum(t, 1) + 4 * (t // 2) + 8 * (t // 3)

    def mix_down(j):
        q = (2 * (1 - x) if j < 2 else 2 * x) + (1 - c if j % 2 == 0 else c)
        start = pl.multiple_of(q * rows, rows)
        seg = pooled_in[pl.ds(start, 2 * rows), :]
        i = lax.broadcasted_iota(jnp.int32, (rows, 2 * rows), 0) + rows
        k = lax.broadcasted_iota(jnp.int32, (rows, 2 * rows), 1)
        band = jnp.where((k <= i) & (k > i - window), 1.0, 0.0).astype(bf16)
        sums = jnp.dot(band, seg, preferred_element_type=f32)
        place = lax.broadcasted_iota(jnp.int32, (rows, 1), 0) + (e * blocks + q) * rows + 1
        counts = jnp.minimum(place, window).astype(f32)
        pooled = (sums / counts - seg[rows:, :].astype(f32)).astype(bf16)
        grouped = jnp.dot(pooled, w_group[...], preferred_element_type=f32)
        grouped = (grouped * channel_scale[...].astype(f32).reshape(1, group_width)).astype(bf16)

        @pl.loop(0, width // col)
        def _(n):
            at = pl.ds(pl.multiple_of(n * col, col), col)
            mix_part[j, :, at] = jnp.dot(grouped, w_out[:, at], preferred_element_type=f32).astype(bf16)

    def pair_to(j):
        return rc(mix_part.at[2 * j], mix_pair.at[j], mix_send.at[3], mix_recv.at[4 + j], dev_c)

    def cross(j):
        at = pl.ds(j * half_rows, half_rows)
        return rc(mix_stage.at[at, :], mix_far.at[at, :], mix_send.at[4], mix_recv.at[6 + j], dev_x)

    def mix_relay(j):
        mix_x(t_x, j).wait_recv()
        mix_fwd(t_x, j).start()

    def final(k):
        @pl.when(mid)
        def _():
            _, at = cut(CHUNKS + k)
            expert_out[at, :] = (acc[e, at, :] + rs_in[3, at, :].astype(f32)).astype(bf16)

        @pl.when(end)
        def _():
            _, at = cut(k)
            rs_got(k, 2).wait_recv()
            expert_out[at, :] = (acc[e, at, :] + rs_in[2, at, :].astype(f32)).astype(bf16)

    down(mirror(3), 1 - x, False, part_of[0])
    first_send(mirror(3), 0, CHUNKS // 2)
    gather(5)
    for home in (mirror(2), third, e):
        scale_of(home)
    hidden(mirror(3), x, part_of[1])
    hidden(mirror(3), 1 - x, part_of[1])
    lead(0)
    down(mirror(3), x, True, part_of[1])
    lead(1)
    down(mirror(3), 1 - x, False, part_of[1])
    first_send(mirror(3), CHUNKS // 2, CHUNKS // 2)

    @pl.when(mid)
    def _():
        d2_all(1, d2_half(w_d2, t_x, g)).wait_recv()
        d2_y(1, True).start()
        d2_c(1).start()

    mix_relay(0)
    lead(2)
    hidden(mirror(2), 1 - x)

    @pl.when(rim_relay)
    def _():
        rim_to(1).wait_recv()
        rim_to(2).start()

    lead(3)
    down(mirror(2), 1 - x, False)
    first_send(mirror(2), CHUNKS)
    lead(4)
    mix_relay(1)

    @pl.when(mid)
    def _():
        down(third, 1 - x, False)

    mix_all_in = rc(mix_all.at[t_d], mix_all.at[t_d], mix_send.at[1], mix_recv.at[2], dev_c)
    mix_all_in.wait_recv()
    pool_in(1 - x)

    @pl.when(rim_last)
    def _():
        rim_to(2).wait_recv()

    @pl.when(e > 0)
    def _():
        value = jnp.dot(rim_rows[...], w_in[...], preferred_element_type=f32)
        pooled_in[pl.ds(rows - rim_rows.shape[0], rim_rows.shape[0]), :] = value.astype(bf16)

    lead(5)
    lag(0)
    mix_down(0)
    pair_to(0).start()
    lead(6)
    lag(1)
    mix_down(1)
    lead(7)
    lag(2)
    pair_to(0).wait_recv()
    for j in range(HALVES):
        at = pl.ds(j * half_rows, half_rows)
        mix_stage[at, :] = (mix_part[1, at, :].astype(f32) + mix_pair[0, at, :].astype(f32)).astype(bf16)
        cross(j).start()
    lead(8)
    lag(3)

    hidden(e, 1 - x)
    lead(9)
    lag(4)

    @pl.when(mid)
    def _():
        d2_y(0, False).wait_recv()
        d2_c(2).start()

    down(e, 1 - x, False)
    lead(10)
    lag(5)
    lead(11)
    lag(6)
    mix_down(2)
    pair_to(1).start()
    lead(12)
    lag(7)
    lead(13)
    mix_down(3)
    lead(14)

    @pl.when(mid)
    def _():
        d2_y(1, False).wait_recv()
        d2_c(3).start()

    lead(15)

    @pl.when(mid)
    def _():
        scales[0] = jnp.transpose(jnp.broadcast_to(coefs[e, pl.ds(mirror(0), 1), :], (rows, rows)))
        d2_all(2, hid_far).wait_recv()
        d2_all(4, w_d2.at[pl.ds(0, 2)]).wait_recv()

        @pl.loop(0, width // col)
        def _(n):
            at = pl.ds(pl.multiple_of(n * col, col), col)
            part = acc[e, :, at]
            scale = scales[0][:, :1]
            for xq in range(2):
                w = w_d2[pl.ds(2 * xq, 2), :, at].reshape(4 * ff_half, col)
                part = part + jnp.dot(hid_far[xq], w, preferred_element_type=f32) * scale
            acc[e, :, at] = part

    for k in range(4):
        lag(CHUNKS + k)
        final(k)
    pair_to(1).wait_recv()
    for j in range(HALVES):
        at = pl.ds(j * half_rows, half_rows)
        cross(j).wait_recv()
        mixed_out[at, :] = (
            mix_part[3, at, :].astype(f32) + mix_pair[1, at, :].astype(f32) + mix_far[at, :].astype(f32)
        ).astype(bf16)

    all_gu(x_send, fx_recv).wait_send()
    all_d(x_send, fx_recv, x_rows).wait_send()
    all_gu(y_send, fx_recv).wait_send()
    all_d(y_send, fx_recv, y_rows).wait_send()
    all_gu(fx_send, fx_recv).wait_send()
    all_d(fx_send, fx_recv, x_rows).wait_send()
    all_gu(fy_send, fx_recv).wait_send()
    all_d(fy_send, fx_recv, y_rows).wait_send()
    own_gu(t).wait_send()
    own_d(t).wait_send()

    def sent(sems, k, p):
        rc(p, p, sems.at[k], mix_recv.at[0], dev_c).wait_send()

    sent(mix_send, 0, mix_all.at[t])
    sent(mix_send, 1, mix_all.at[t])
    sent(mix_send, 2, mix_all.at[t])
    sent(mix_send, 3, mix_part.at[pl.ds(0, 2)])
    sent(mix_send, 4, mix_stage)

    @pl.when(rim_source)
    def _():
        rim_to(0).wait_send()

    @pl.when(rim_mine)
    def _():
        rim_to(1).wait_send()
        rim_to(2).wait_send()

    @pl.when(rim_relay)
    def _():
        rim_to(2).wait_send()

    @pl.when(end)
    def _():
        sent(ag_send, 0, tokens.at[e])
        sent(coef_send, 0, coefs.at[e])
        d2_own().wait_send()
        sent(d2_send, 1, d2_half(w_d, t_x, g))
        sent(d2_send, 2, hid_far)

    @pl.when(mid)
    def _():
        sent(ag_send, 0, tokens.at[pl.ds(0, 2)])
        sent(ag_send, 1, tokens.at[pl.ds(0, 3)])
        sent(coef_send, 0, coefs.at[pl.ds(0, 2)])
        sent(coef_send, 1, coefs.at[pl.ds(0, 3)])
        sent(d2_send, 3, w_d2.at[0])
        sent(d2_send, 4, w_d2.at[pl.ds(0, 2)])
        sent(rs_send, 1, rs_stage.at[2])

    for k in range(4, CHUNKS):
        lag(CHUNKS + k)
        final(k)
    sent(rs_send, 0, rs_stage.at[pl.ds(0, 2)])


def fused(*args):
    (mixer_tokens, _, in_weight, group_weight, _, out_weight, _, _, route_ids, _, gate_weight, _, _) = args
    rows, width = mixer_tokens.shape
    group_width = in_weight.shape[1]
    ff = gate_weight.shape[2]
    blocks = lax.axis_size("ep")
    parts = lax.axis_size("tp")
    half = rows // HALVES
    bf16, f32 = jnp.bfloat16, jnp.float32
    vmem = pltpu.VMEM
    dma = pltpu.SemaphoreType.DMA
    anyspace = pl.BlockSpec(memory_space=pl.ANY)
    local_spec = pl.BlockSpec(memory_space=pltpu.VMEM)
    args = list(args)
    for i in (8, 9):
        args[i] = args[i].T
    small = (1, 4, 7, 8, 9)
    scratch = [
        vmem((rows, width), bf16),
        vmem((rows, width), bf16),
        vmem((width, group_width), bf16),
        vmem((group_width, group_width), bf16),
        vmem((group_width, width), bf16),
        vmem((parts, 2, width, ff), bf16),
        vmem((parts, ff, width), bf16),
        vmem((blocks, rows, width), bf16),
        vmem((blocks, 8, rows), f32),
        vmem((blocks, rows, rows), f32),
        vmem((blocks, 2, rows, 2 * ff), bf16),
        vmem((blocks, rows, width), f32),
        vmem((4, rows, width), bf16),
        vmem((3, rows, width), bf16),
        vmem((parts, rows, width), bf16),
        vmem((rows * (parts + 1), group_width), bf16),
        vmem((parts, rows, width), bf16),
        vmem((2, rows, width), bf16),
        vmem((rows, width), bf16),
        vmem((rows, width), bf16),
        vmem((WINDOW_MAX, width), bf16),
        vmem((parts, ff, width), bf16),
        vmem((2, rows, 2 * ff), bf16),
        dma((10,)),
    ]
    for count in (2, X_PIECES, 2, Y_PIECES, 2, 2, 2, 2, 2, 2, 2, 8, 2, 4, 2, 4 * CHUNKS, 5, 8, 3, 3, 5, 6):
        scratch.append(dma((count,)))
    shape = vmem((rows, width), bf16)
    return pl.pallas_call(
        fused_kernel,
        out_shape=(shape, shape),
        in_specs=[local_spec if i in small else anyspace for i in range(len(args))],
        out_specs=(local_spec, local_spec),
        scratch_shapes=scratch,
        compiler_params=pltpu.CompilerParams(
            collective_id=0, has_side_effects=True, vmem_limit_bytes=60 << 20
        ),
        name="fused",
    )(*args)


def fits(mesh):
    sizes = dict(mesh.shape)
    return sizes["grp"] == 2 and sizes["ep"] == 4 and sizes["tp"] == 4


def solution(mesh):
    placed = (
        P(("grp", "ep", "tp"), None),
        P(),
        P(None, "tp"),
        P("tp", None, None),
        P("tp"),
        P("tp", None),
        P(("grp", "ep", "tp"), None),
        P(),
        P(("grp", "ep", "tp"), None),
        P(("grp", "ep", "tp"), None),
        P("ep", None, "tp"),
        P("ep", None, "tp"),
        P("ep", "tp", None),
    )
    return jax.shard_map(
        fused if fits(mesh) else local,
        mesh=mesh,
        in_specs=placed,
        out_specs=(P(("grp", "ep", "tp"), None), P(("grp", "ep", "tp"), None)),
        check_vma=False,
    )
```

```python
import jax
import jax.numpy as jnp
from jax import lax
from jax.experimental import pallas as pl
from jax.experimental.pallas import tpu as pltpu
from jax.sharding import PartitionSpec as P

WINDOW_MAX = 16


def shifted(value, axis, by):
    devices = lax.axis_size(axis)
    pairs = [(i, i + by) for i in range(devices) if 0 <= i + by < devices]
    return lax.ppermute(value, axis, pairs)


def turned(value, axis, by):
    devices = lax.axis_size(axis)
    if by % devices == 0:
        return value
    return lax.ppermute(value, axis, [(i, (i + by) % devices) for i in range(devices)])


def rms_rows(rows, gain):
    values = rows.astype(jnp.float32)
    scaled = values * lax.rsqrt(jnp.mean(values * values, axis=-1, keepdims=True) + 1e-06)
    return (scaled * gain.astype(jnp.float32)).astype(jnp.bfloat16)


def expert_hidden(rows, w_gate, w_up):
    gate = jnp.dot(rows, w_gate, preferred_element_type=jnp.float32)
    upper = jnp.dot(rows, w_up, preferred_element_type=jnp.float32)
    return (jax.nn.silu(gate) * upper).astype(jnp.bfloat16)


def local(
    mixer_tokens,
    mixer_gain,
    in_weight,
    group_weight,
    channel_scale,
    out_weight,
    expert_tokens,
    expert_gain,
    route_ids,
    route_weights,
    gate_weight,
    up_weight,
    down_weight,
):
    normed = rms_rows(mixer_tokens, mixer_gain)
    expert_in = rms_rows(expert_tokens, expert_gain)
    shares = route_weights / jnp.sum(route_weights, axis=1, keepdims=True)
    rows_here, top_k = route_ids.shape
    width = expert_in.shape[1]
    n_experts = lax.axis_size("ep") * gate_weight.shape[0]
    capacity = 4 * rows_here // n_experts
    dense = capacity >= rows_here
    parts_tp = lax.axis_size("tp")
    if dense:
        both = lax.all_gather(jnp.concatenate([normed, expert_in], axis=0), "tp", axis=0, tiled=True)
        both = both.reshape(parts_tp, 2, rows_here, width)
        every = both[:, 0].reshape(parts_tp * rows_here, width)
        own = both[:, 1].reshape(parts_tp * rows_here, width)
    else:
        every = lax.all_gather(normed, "tp", axis=0, tiled=True)
    pooled_in = jnp.dot(
        every,
        in_weight,
        preferred_element_type=jnp.float32,
    ).astype(jnp.bfloat16)
    block_rows = pooled_in.shape[0]
    rim_rows = shifted(pooled_in[block_rows - WINDOW_MAX :], "ep", 1)
    values = pooled_in.astype(jnp.float32)
    extended = jnp.concatenate([rim_rows.astype(jnp.float32), values], axis=0)
    window = jnp.left_shift(jnp.int32(2), lax.axis_index("tp"))
    sums = extended
    span = 1
    total = jnp.zeros_like(values)
    for level in range(WINDOW_MAX.bit_length() - 1):
        sums = sums[span:] + sums[:-span]
        span = span * 2
        total = total + jnp.where(window == span, sums[sums.shape[0] - block_rows :], 0.0)
    positions = lax.axis_index("ep") * block_rows + lax.iota(jnp.int32, block_rows) + 1
    counts = jnp.minimum(positions, window).astype(jnp.float32)
    pooled = (total / counts[:, None] - values).astype(jnp.bfloat16)
    grouped = (
        jnp.dot(pooled, group_weight[0], preferred_element_type=jnp.float32)
        * channel_scale.astype(jnp.float32)
    ).astype(jnp.bfloat16)
    mixed_part = jnp.dot(grouped, out_weight, preferred_element_type=jnp.float32).astype(
        jnp.bfloat16
    )
    if dense:
        experts = jnp.arange(n_experts, dtype=jnp.int32)
        named = (route_ids[:, :, None] == experts[None, None, :]).astype(jnp.float32)
        coefs = jnp.sum(named * shares[:, :, None], axis=1)
        coefs = lax.all_gather(coefs, ("ep", "tp"), axis=0, tiled=True)
        blocks = lax.axis_size("ep")
        here = lax.axis_index("ep")
        mine = (experts == here).astype(jnp.float32)
        coef = jnp.sum(coefs * mine[None, :], axis=1).reshape(blocks, parts_tp, rows_here)
        order = list(range(1, blocks))

        def scale_of(k):
            return lax.dynamic_index_in_dim(coef, lax.rem(here - k + blocks, blocks), 0, False)

        def expert_part(rows, scale):
            hidden = expert_hidden(rows, gate_weight[0], up_weight[0])
            part = jnp.dot(hidden, down_weight[0], preferred_element_type=jnp.float32)
            return (part * scale.reshape(-1)[:, None]).astype(jnp.bfloat16)

        moved = jnp.concatenate([turned(expert_in, "ep", k) for k in order], axis=0)
        moved, own = lax.optimization_barrier((moved, own))
        own_part = expert_part(own, scale_of(0))
        others = lax.all_gather(moved, "tp", axis=0, tiled=True)
        part = expert_part(others, jnp.stack([scale_of(k) for k in order], axis=1))
        back = lax.psum_scatter(part, "tp", scatter_dimension=0, tiled=True)
        back = back.reshape(blocks - 1, rows_here, width)
        pair = jnp.stack(
            [value.reshape(parts_tp, rows_here, width) for value in (mixed_part, own_part)], axis=1
        ).reshape(2 * parts_tp * rows_here, width)
        pair = lax.psum_scatter(pair, "tp", scatter_dimension=0, tiled=True)
        total = pair[rows_here:].astype(jnp.float32)
        for i, k in enumerate(order):
            total = total + turned(back[i], "ep", -k).astype(jnp.float32)
        return (pair[:rows_here], total.astype(jnp.bfloat16))
    mixed_tokens = lax.psum_scatter(mixed_part, "tp", scatter_dimension=0, tiled=True)
    flat_ids = route_ids.reshape(rows_here * top_k)
    one_hot = (flat_ids[:, None] == jnp.arange(n_experts, dtype=jnp.int32)[None, :]).astype(
        jnp.int32
    )
    before = jnp.cumsum(one_hot, axis=0) - one_hot
    slots = jnp.sum(before * one_hot, axis=1)
    targets = flat_ids * capacity + slots
    placement = (
        targets.reshape(rows_here, top_k)[None, :, :]
        == jnp.arange(n_experts * capacity, dtype=jnp.int32)[:, None, None]
    )
    dispatch = jnp.any(placement, axis=2).astype(jnp.bfloat16)
    outgoing = jnp.dot(dispatch, expert_in, preferred_element_type=jnp.float32).astype(jnp.bfloat16)
    outgoing = outgoing.reshape(n_experts, capacity, width)
    arrived = lax.all_to_all(outgoing, "ep", split_axis=0, concat_axis=0, tiled=True)
    sources, held, _ = arrived.shape
    flat = arrived.reshape(sources * held, width)
    hidden = expert_hidden(
        lax.all_gather(flat, "tp", axis=0, tiled=True), gate_weight[0], up_weight[0]
    )
    rows = hidden
    summed = lax.psum_scatter(
        jnp.dot(rows, down_weight[0], preferred_element_type=jnp.float32).astype(jnp.bfloat16),
        "tp",
        scatter_dimension=0,
        tiled=True,
    ).astype(jnp.float32)
    expert_out = lax.all_to_all(
        summed.reshape(sources, held, width).astype(jnp.bfloat16),
        "ep",
        split_axis=0,
        concat_axis=0,
        tiled=True,
    ).astype(jnp.float32)
    flat_out = expert_out.reshape(n_experts * capacity, width)
    picked = jnp.take(flat_out, targets, axis=0).reshape(rows_here, top_k, width)
    expert_mix = jnp.sum(picked * shares[:, :, None], axis=1).astype(jnp.bfloat16)
    return (mixed_tokens, expert_mix)


MESH = pl.DeviceIdType.MESH
GU_CUTS = (0, 1, 2, 4, 6, 8, 10, 12, 14, 16)
PIECES_GU = len(GU_CUTS) - 1
D_CUTS = (0, 2, 4, 5, 6, 8)
PIECES = PIECES_GU + len(D_CUTS) - 1
X_PIECES = PIECES + 1
Y_PIECES = PIECES - 1
WINDOW = 5
LAG = 3
HALVES = 2
CHUNKS = 8


def fused_kernel(
    mixer_tokens,
    mixer_gain,
    in_weight,
    group_weight,
    channel_scale,
    out_weight,
    expert_tokens,
    expert_gain,
    route_ids,
    route_weights,
    gate_weight,
    up_weight,
    down_weight,
    mixed_out,
    expert_out,
    mix_raw,
    exp_raw,
    w_in,
    w_group,
    w_out,
    w_gu,
    w_d,
    tokens,
    coefs,
    scales,
    hid,
    acc,
    rs_in,
    rs_stage,
    mix_all,
    pooled_in,
    mix_part,
    mix_pair,
    mix_stage,
    mix_far,
    rim_rows,
    w_d2,
    hid_far,
    load_sem,
    x_send,
    x_recv,
    y_send,
    y_recv,
    own_send,
    own_recv,
    fx_send,
    fx_recv,
    fy_send,
    fy_recv,
    ag_send,
    ag_recv,
    coef_send,
    coef_recv,
    rs_send,
    rs_recv,
    mix_send,
    mix_recv,
    rim_send,
    rim_recv,
    d2_send,
    d2_recv,
):
    f32, bf16 = jnp.float32, jnp.bfloat16
    rows, width = exp_raw.shape
    half_rows = rows // HALVES
    group_width = w_group.shape[0]
    ff_half = w_d.shape[1] // 2
    blocks = tokens.shape[0]
    parts = mix_all.shape[0]
    g = lax.axis_index("grp")
    e = lax.axis_index("ep")
    t = lax.axis_index("tp")
    x = t // 2
    c = t % 2
    t_c = 2 * x + 1 - c
    t_x = 2 * (1 - x) + c
    t_d = 2 * (1 - x) + 1 - c
    dev_c, dev_x, dev_y = (g, e, t_c), (g, e, t_x), (1 - g, e, t)
    hi = e // 2
    sign = 1 - 2 * hi
    last = blocks - 1

    def mirror(m):
        return hi * last + sign * m

    u = mirror(e)
    end = u == 0
    mid = u == 1
    far = (g, lax.rem(e + sign + blocks, blocks), t)
    near = (g, lax.rem(e - sign + blocks, blocks), t)
    third = mirror(1 - u)

    def rc(src, dst, send, recv, dev):
        return pltpu.make_async_remote_copy(
            src_ref=src, dst_ref=dst, send_sem=send, recv_sem=recv, device_id=dev, device_id_type=MESH
        )

    barrier = pltpu.get_barrier_semaphore()
    for dev in (dev_c, dev_x, dev_y):
        pl.semaphore_signal(barrier, inc=1, device_id=dev, device_id_type=MESH)

    @pl.when(e < last)
    def _():
        dev = (g, lax.rem(e + 1, blocks), t)
        pl.semaphore_signal(barrier, inc=1, device_id=dev, device_id_type=MESH)

    @pl.when(e > 0)
    def _():
        dev = (g, lax.rem(e - 1 + blocks, blocks), t)
        pl.semaphore_signal(barrier, inc=1, device_id=dev, device_id_type=MESH)

    def loads():
        out = []
        for h in range(2):
            hh = g if h == 0 else 1 - g
            lane = pl.multiple_of(hh * ff_half, ff_half)
            out.append((gate_weight.at[0, :, pl.ds(lane, ff_half)], w_gu.at[t, hh, :, pl.ds(0, ff_half)]))
            out.append((up_weight.at[0, :, pl.ds(lane, ff_half)], w_gu.at[t, hh, :, pl.ds(ff_half, ff_half)]))
            if h == 0:
                out.append((expert_tokens, exp_raw))
        out.append((down_weight.at[0], w_d.at[t]))
        out.append((mixer_tokens, mix_raw))
        out.append((in_weight, w_in))
        out.append((group_weight.at[0], w_group))
        out.append((out_weight, w_out))
        return [pltpu.make_async_copy(a, b, load_sem.at[i]) for i, (a, b) in enumerate(out)]

    local = loads()
    for copy in local[:3]:
        copy.start()
    def norm(raw, gain, dst, start, count):
        step = 32
        gain_row = gain[...].astype(f32).reshape(1, width)

        @pl.loop(0, count // step)
        def _(i):
            at = pl.ds(pl.multiple_of(start + i * step, step), step)
            values = raw[at, :].astype(f32)
            scaled = values * lax.rsqrt(jnp.mean(values * values, axis=-1, keepdims=True) + 1e-06)
            dst[at, :] = (scaled * gain_row).astype(bf16)

    ids = route_ids[...]
    weights = route_weights[...]
    shares = weights / jnp.sum(weights, axis=0, keepdims=True)
    numbers = lax.broadcasted_iota(jnp.int32, coefs.shape[1:], 0)
    coef = jnp.zeros(coefs.shape[1:], f32)
    for k in range(ids.shape[0]):
        coef = coef + jnp.where(ids[k : k + 1, :] == numbers, shares[k : k + 1, :], 0.0)
    coefs[e] = coef

    def d_cut(s):
        unit = ff_half // D_CUTS[-1]
        low, high = D_CUTS[s - PIECES_GU], D_CUTS[s - PIECES_GU + 1]
        return low * unit, (high - low) * unit

    def piece(q, h, s):
        if s < PIECES_GU:
            unit = width // GU_CUTS[-1]
            low, high = GU_CUTS[s], GU_CUTS[s + 1]
            return w_gu.at[q, h, pl.ds(low * unit, (high - low) * unit), :]
        start, n = d_cut(s)
        return w_d.at[q, pl.ds(pl.multiple_of(h * ff_half + start, 16), n), :]

    def x_piece(q, s):
        return piece(q, g, s) if s < PIECES else piece(q, 1 - g, PIECES - 1)

    def kind(s):
        return 0 if s < PIECES_GU else 1

    def send_x(s):
        p = x_piece(t, s)
        return rc(p, p, x_send.at[kind(s)], x_recv.at[s], dev_x)

    def got_x(s):
        p = x_piece(t_x, s)
        return rc(p, p, x_send.at[0], x_recv.at[s], dev_x)

    def send_y(s):
        p = piece(t_x, g, s)
        return rc(p, p, y_send.at[kind(s)], y_recv.at[s], dev_y)

    def got_y(s):
        p = piece(t_x, 1 - g, s)
        return rc(p, p, y_send.at[0], y_recv.at[s], dev_y)

    def send_fx(s):
        p = x_piece(t_x, s)
        return rc(p, p, fx_send.at[kind(s)], fx_recv.at[kind(s)], dev_c)

    def send_fy(s):
        p = piece(t_x, 1 - g, s)
        return rc(p, p, fy_send.at[kind(s)], fy_recv.at[kind(s)], dev_c)

    d_last = d_cut(PIECES - 1)
    x_rows, y_rows = ff_half + d_last[1], d_last[0]

    def all_gu(send, recv):
        return rc(w_gu.at[t, g], w_gu.at[t, g], send.at[0], recv.at[0], dev_c)

    def all_d(send, recv, count):
        p = w_d.at[t, pl.ds(0, count), :]
        return rc(p, p, send.at[1], recv.at[1], dev_c)

    def own_gu(q):
        return rc(w_gu.at[q], w_gu.at[q], own_send.at[0], own_recv.at[0], dev_c)

    def own_d(q):
        return rc(w_d.at[q], w_d.at[q], own_send.at[1], own_recv.at[1], dev_c)

    def chunk(home, j):
        return tokens.at[home, pl.ds(j * half_rows, half_rows), :]

    def ag_far(home, j, f):
        p = chunk(home, j)
        return rc(p, p, ag_send.at[0], ag_recv.at[f + 6 * (1 - u)], far)

    def ag_near(home, j, f):
        p = chunk(home, j)
        return rc(p, p, ag_send.at[1], ag_recv.at[f], near)

    def ag_got(home, j, f):
        p = chunk(home, j)
        return rc(p, p, ag_send.at[0], ag_recv.at[f], far)

    rim_source = (t == parts - 1) & (e < last)
    rim_mine = (t == parts - 1) & (e > 0)
    rim_relay = (t == parts // 2 - 1) & (e > 0)
    rim_last = (c == 0) & (e > 0)

    def rim_to(k):
        src = mix_all.at[t, pl.ds(rows - rim_rows.shape[0], rim_rows.shape[0]), :] if k == 0 else rim_rows
        dev = ((g, lax.rem(e + 1, blocks), t), dev_x, dev_c)[k]
        return rc(src, rim_rows, rim_send.at[k], rim_recv.at[k], dev)

    def coef_far(home, k):
        return rc(coefs.at[home], coefs.at[home], coef_send.at[0], coef_recv.at[k + 3 * (1 - u)], far)

    def coef_near(home, k):
        return rc(coefs.at[home], coefs.at[home], coef_send.at[1], coef_recv.at[k], near)

    def coef_got(home, k):
        return rc(coefs.at[home], coefs.at[home], coef_send.at[0], coef_recv.at[k], far)

    def d2_half(ref, q, h):
        return ref.at[q, pl.ds(pl.multiple_of(h * ff_half, ff_half), ff_half), :]

    def d2_piece(ref, s):
        start, n = d_cut(s)
        return ref.at[t_x, pl.ds(pl.multiple_of(g * ff_half + start, 16), n), :]

    def d2_own():
        return rc(d2_half(w_d, t, g), d2_half(w_d2, t, g), d2_send.at[0], d2_recv.at[0], far)

    def d2_relay(s):
        return rc(d2_piece(w_d, s), d2_piece(w_d2, s), d2_send.at[1], d2_recv.at[1], far)

    def d2_hid(xq):
        return rc(hid.at[third, xq], hid_far.at[xq], d2_send.at[2], d2_recv.at[2], far)

    def d2_y(k, mine):
        p = d2_half(w_d2, t if k == 0 else t_x, g if mine else 1 - g)
        return rc(p, p, d2_send.at[3], d2_recv.at[3 + k], dev_y)

    def d2_c(k):
        p = d2_half(w_d2, t if k % 2 == 0 else t_x, g if k < 2 else 1 - g)
        return rc(p, p, d2_send.at[4], d2_recv.at[5], dev_c)

    def d2_all(k, p):
        return rc(p, p, d2_send.at[k], d2_recv.at[min(k, 2) if k < 4 else 5], dev_c)

    def mix_x(q, j):
        p = mix_all.at[q, pl.ds(j * half_rows, half_rows), :]
        return rc(p, p, mix_send.at[0], mix_recv.at[j], dev_x)

    def mix_fwd(q, j):
        p = mix_all.at[q, pl.ds(j * half_rows, half_rows), :]
        return rc(p, p, mix_send.at[1], mix_recv.at[2], dev_c)

    def mix_own(q):
        return rc(mix_all.at[q], mix_all.at[q], mix_send.at[2], mix_recv.at[3], dev_c)

    local[0].wait()
    local[1].wait()
    @pl.when(end)
    def _():
        pl.semaphore_wait(barrier, 4)

    @pl.when(mid)
    def _():
        pl.semaphore_wait(barrier, 5)

    for s in range(WINDOW):
        send_x(s).start()
    for copy in local[3:]:
        copy.start()
    local[2].wait()
    norm(exp_raw, expert_gain, tokens.at[e], 0, rows)
    coef_far(e, 0).start()
    for j in range(HALVES):
        ag_far(e, j, j).start()

    @pl.when(mid)
    def _():
        coef_near(e, 0).start()
        for j in range(HALVES):
            ag_near(e, j, j).start()

    local[3].wait()
    local[4].wait()
    own_gu(t).start()
    local[5].wait()
    own_d(t).start()

    local[6].wait()
    norm(mix_raw, mixer_gain, mix_all.at[t], 0, rows)

    @pl.when(rim_source)
    def _():
        rim_to(0).start()

    @pl.when(end)
    def _():
        d2_own().start()

    mix_own(t).start()

    whole = pl.ds(0, rows)
    part_of = [pl.ds(j * half_rows, half_rows) for j in range(HALVES)]

    def hidden(home, xq, at=whole):
        @pl.loop(0, 4)
        def _(j):
            q = 2 * xq + j // 2
            h = j % 2
            both = jnp.dot(tokens[home, at, :], w_gu[q, h], preferred_element_type=f32)
            gate, upper = both[:, :ff_half], both[:, ff_half:]
            value = gate / (1.0 + jnp.exp(-gate)) * upper
            hid[home, xq, at, pl.ds(pl.multiple_of(j * ff_half, ff_half), ff_half)] = value.astype(bf16)

    col = 2 * width * HALVES // CHUNKS

    def down(home, xq, first, at=whole):
        @pl.loop(0, width // col)
        def _(n):
            cols = pl.ds(pl.multiple_of(n * col, col), col)
            w = w_d[pl.ds(2 * xq, 2), :, cols].reshape(4 * ff_half, col)
            part = jnp.dot(hid[home, xq, at, :], w, preferred_element_type=f32)
            if first:
                acc[home, at, cols] = part
            else:
                scale = scales[home, at, :][:, :1]
                acc[home, at, cols] = (acc[home, at, cols] + part) * scale

    def pool_in(xq):
        @pl.loop(0, 2)
        def _(j):
            q = 2 * xq + j
            value = jnp.dot(mix_all[q], w_in[...], preferred_element_type=f32)
            pooled_in[pl.ds(pl.multiple_of(rows * (q + 1), rows), rows), :] = value.astype(bf16)

    def wait_fgu():
        all_gu(fx_send, fx_recv).wait_recv()
        all_gu(fy_send, fy_recv).wait_recv()

    def relay_y(s):
        got_y(s).wait_recv()
        send_fy(s).start()

    def gather(f):
        @pl.when(end)
        def _():
            home = mirror(1 + f // 2)
            ag_got(home, f % 2, f).wait_recv()
            if f % 2 == 0:
                coef_got(home, f // 2).wait_recv()

        if f < 4:

            @pl.when(mid)
            def _():
                home = mirror(2 + f // 2)
                ag_got(home, f % 2, f).wait_recv()
                ag_near(home, f % 2, f + 2).start()
                if f % 2 == 0:
                    coef_got(home, f // 2).wait_recv()
                    coef_near(home, f // 2 + 1).start()

        if f < 2:

            @pl.when(mid)
            def _():
                home = mirror(0)
                ag_got(home, f % 2, 6 + f).wait_recv()
                ag_far(home, f % 2, 2 + f).start()
                if f % 2 == 0:
                    coef_got(home, 3).wait_recv()
                    coef_far(home, 1).start()

    def scale_of(home):
        scales[home] = jnp.transpose(jnp.broadcast_to(coefs[home, pl.ds(e, 1), :], (rows, rows)))

    for s in range(X_PIECES):
        got_x(s).wait_recv()
        if s < Y_PIECES:
            send_y(s).start()
        send_fx(s).start()
        if PIECES_GU <= s < PIECES:

            @pl.when(end)
            def _():
                d2_relay(s).start()

        if s + WINDOW == X_PIECES:

            @pl.when(rim_mine)
            def _():
                rim_to(1).start()

        if s + WINDOW < X_PIECES:
            send_x(s + WINDOW).start()
        elif s + WINDOW < X_PIECES + HALVES:
            mix_x(t, s + WINDOW - X_PIECES).start()
        if s >= LAG:
            relay_y(s - LAG)
        if s in (3, 5, 7, 9, 11):
            gather(s // 2 - 1)
        if s == 3:
            own_gu(t_c).wait_recv()
            hidden(e, x)
        if s == 8:

            @pl.when(rim_mine)
            def _():
                rim_to(0).wait_recv()
                rim_to(2).start()

        if s == 4:
            own_d(t_c).wait_recv()
            down(e, x, True)
        if s == 5:
            pooled_in[pl.ds(0, rows), :] = jnp.zeros((rows, group_width), bf16)
        if s == 6:
            hidden(third, x)

            @pl.when(end)
            def _():
                d2_hid(x).start()

        if s == 7:

            @pl.when(mid)
            def _():
                down(third, x, True)

        if s == 8:
            mix_own(t_c).wait_recv()
            local[7].wait()
            pool_in(x)
        if s == 10:
            hidden(mirror(2), x)
            down(mirror(2), x, True)
        if s == 11:
            hidden(mirror(3), x, part_of[0])
        if s == 12:
            wait_fgu()
            hidden(third, 1 - x)

            @pl.when(end)
            def _():
                d2_hid(1 - x).start()

        if s == Y_PIECES:

            @pl.when(mid)
            def _():
                d2_own().wait_recv()
                d2_y(0, True).start()
                d2_c(0).start()

            hidden(mirror(3), 1 - x, part_of[0])
            down(mirror(3), x, True, part_of[0])
            scale_of(mirror(3))

    for s in range(X_PIECES - LAG, Y_PIECES):
        relay_y(s)
    all_d(fx_send, fx_recv, x_rows).wait_recv()
    all_d(fy_send, fy_recv, y_rows).wait_recv()

    def cut(k):
        slot, j = divmod(k, CHUNKS)
        return slot, pl.ds(j * (rows // CHUNKS), rows // CHUNKS)

    def rs_far(k):
        slot, at = cut(k)
        sem = k + 2 * CHUNKS * u
        return rc(rs_stage.at[slot, at, :], rs_in.at[slot + 2 * u, at, :], rs_send.at[0], rs_recv.at[sem], far)

    def rs_near(k):
        slot, at = cut(k)
        sem = 2 * CHUNKS + k
        return rc(rs_stage.at[2, at, :], rs_in.at[2, at, :], rs_send.at[1], rs_recv.at[sem], near)

    def rs_got(k, base):
        slot, at = cut(k)
        p = rs_in.at[slot + base, at, :]
        return rc(p, p, rs_send.at[0], rs_recv.at[k + base * CHUNKS], far)

    def first_send(home, first, count=CHUNKS):
        @pl.when(end)
        def _():
            for k in range(first, first + count):
                slot, at = cut(k)
                rs_stage[slot, at, :] = acc[home, at, :].astype(bf16)
                rs_far(k).start()

    def lead(k):
        @pl.when(mid)
        def _():
            rs_got(k, 0).wait_recv()
            slot, at = cut(k)
            rs_stage[slot, at, :] = (acc[mirror(3 - slot), at, :] + rs_in[slot, at, :].astype(f32)).astype(bf16)
            rs_far(k).start()

    def lag(k):
        @pl.when(mid)
        def _():
            rs_got(k, 2).wait_recv()
            if k < CHUNKS:
                slot, at = cut(k)
                rs_stage[2, at, :] = (acc[mirror(0), at, :] + rs_in[2, at, :].astype(f32)).astype(bf16)
                rs_near(k).start()

    local[8].wait()
    local[9].wait()
    window = 2 + 2 * jnp.minimum(t, 1) + 4 * (t // 2) + 8 * (t // 3)

    def mix_down(j):
        q = (2 * (1 - x) if j < 2 else 2 * x) + (1 - c if j % 2 == 0 else c)
        start = pl.multiple_of(q * rows, rows)
        seg = pooled_in[pl.ds(start, 2 * rows), :]
        i = lax.broadcasted_iota(jnp.int32, (rows, 2 * rows), 0) + rows
        k = lax.broadcasted_iota(jnp.int32, (rows, 2 * rows), 1)
        band = jnp.where((k <= i) & (k > i - window), 1.0, 0.0).astype(bf16)
        sums = jnp.dot(band, seg, preferred_element_type=f32)
        place = lax.broadcasted_iota(jnp.int32, (rows, 1), 0) + (e * blocks + q) * rows + 1
        counts = jnp.minimum(place, window).astype(f32)
        pooled = (sums / counts - seg[rows:, :].astype(f32)).astype(bf16)
        grouped = jnp.dot(pooled, w_group[...], preferred_element_type=f32)
        grouped = (grouped * channel_scale[...].astype(f32).reshape(1, group_width)).astype(bf16)

        @pl.loop(0, width // col)
        def _(n):
            at = pl.ds(pl.multiple_of(n * col, col), col)
            mix_part[j, :, at] = jnp.dot(grouped, w_out[:, at], preferred_element_type=f32).astype(bf16)

    def pair_to(j):
        return rc(mix_part.at[2 * j], mix_pair.at[j], mix_send.at[3], mix_recv.at[4 + j], dev_c)

    def cross(j):
        at = pl.ds(j * half_rows, half_rows)
        return rc(mix_stage.at[at, :], mix_far.at[at, :], mix_send.at[4], mix_recv.at[6 + j], dev_x)

    def mix_relay(j):
        mix_x(t_x, j).wait_recv()
        mix_fwd(t_x, j).start()

    def final(k):
        @pl.when(mid)
        def _():
            _, at = cut(CHUNKS + k)
            expert_out[at, :] = (acc[e, at, :] + rs_in[3, at, :].astype(f32)).astype(bf16)

        @pl.when(end)
        def _():
            _, at = cut(k)
            rs_got(k, 2).wait_recv()
            expert_out[at, :] = (acc[e, at, :] + rs_in[2, at, :].astype(f32)).astype(bf16)

    down(mirror(3), 1 - x, False, part_of[0])
    first_send(mirror(3), 0, CHUNKS // 2)
    gather(5)
    for home in (mirror(2), third, e):
        scale_of(home)
    hidden(mirror(3), x, part_of[1])
    hidden(mirror(3), 1 - x, part_of[1])
    lead(0)
    down(mirror(3), x, True, part_of[1])
    lead(1)
    down(mirror(3), 1 - x, False, part_of[1])
    first_send(mirror(3), CHUNKS // 2, CHUNKS // 2)

    @pl.when(mid)
    def _():
        d2_all(1, d2_half(w_d2, t_x, g)).wait_recv()
        d2_y(1, True).start()
        d2_c(1).start()

    mix_relay(0)
    lead(2)
    hidden(mirror(2), 1 - x)

    @pl.when(rim_relay)
    def _():
        rim_to(1).wait_recv()
        rim_to(2).start()

    lead(3)
    down(mirror(2), 1 - x, False)
    first_send(mirror(2), CHUNKS)
    lead(4)
    mix_relay(1)

    @pl.when(mid)
    def _():
        down(third, 1 - x, False)

    mix_all_in = rc(mix_all.at[t_d], mix_all.at[t_d], mix_send.at[1], mix_recv.at[2], dev_c)
    mix_all_in.wait_recv()
    pool_in(1 - x)

    @pl.when(rim_last)
    def _():
        rim_to(2).wait_recv()

    @pl.when(e > 0)
    def _():
        value = jnp.dot(rim_rows[...], w_in[...], preferred_element_type=f32)
        pooled_in[pl.ds(rows - rim_rows.shape[0], rim_rows.shape[0]), :] = value.astype(bf16)

    lead(5)
    lag(0)
    mix_down(0)
    pair_to(0).start()
    lead(6)
    lag(1)
    mix_down(1)
    lead(7)
    lag(2)
    pair_to(0).wait_recv()
    for j in range(HALVES):
        at = pl.ds(j * half_rows, half_rows)
        mix_stage[at, :] = (mix_part[1, at, :].astype(f32) + mix_pair[0, at, :].astype(f32)).astype(bf16)
        cross(j).start()
    lead(8)
    lag(3)

    hidden(e, 1 - x)
    lead(9)
    lag(4)

    @pl.when(mid)
    def _():
        d2_y(0, False).wait_recv()
        d2_c(2).start()

    down(e, 1 - x, False)
    lead(10)
    lag(5)
    lead(11)
    lag(6)
    mix_down(2)
    pair_to(1).start()
    lead(12)
    lag(7)
    lead(13)
    mix_down(3)
    lead(14)

    @pl.when(mid)
    def _():
        d2_y(1, False).wait_recv()
        d2_c(3).start()

    lead(15)

    @pl.when(mid)
    def _():
        scales[0] = jnp.transpose(jnp.broadcast_to(coefs[e, pl.ds(mirror(0), 1), :], (rows, rows)))
        d2_all(2, hid_far).wait_recv()
        d2_all(4, w_d2.at[pl.ds(0, 2)]).wait_recv()

        @pl.loop(0, width // col)
        def _(n):
            at = pl.ds(pl.multiple_of(n * col, col), col)
            part = acc[e, :, at]
            scale = scales[0][:, :1]
            for xq in range(2):
                w = w_d2[pl.ds(2 * xq, 2), :, at].reshape(4 * ff_half, col)
                part = part + jnp.dot(hid_far[xq], w, preferred_element_type=f32) * scale
            acc[e, :, at] = part

    for k in range(4):
        lag(CHUNKS + k)
        final(k)
    pair_to(1).wait_recv()
    for j in range(HALVES):
        at = pl.ds(j * half_rows, half_rows)
        cross(j).wait_recv()
        mixed_out[at, :] = (
            mix_part[3, at, :].astype(f32) + mix_pair[1, at, :].astype(f32) + mix_far[at, :].astype(f32)
        ).astype(bf16)

    all_gu(x_send, fx_recv).wait_send()
    all_d(x_send, fx_recv, x_rows).wait_send()
    all_gu(y_send, fx_recv).wait_send()
    all_d(y_send, fx_recv, y_rows).wait_send()
    all_gu(fx_send, fx_recv).wait_send()
    all_d(fx_send, fx_recv, x_rows).wait_send()
    all_gu(fy_send, fx_recv).wait_send()
    all_d(fy_send, fx_recv, y_rows).wait_send()
    own_gu(t).wait_send()
    own_d(t).wait_send()

    def sent(sems, k, p):
        rc(p, p, sems.at[k], mix_recv.at[0], dev_c).wait_send()

    sent(mix_send, 0, mix_all.at[t])
    sent(mix_send, 1, mix_all.at[t])
    sent(mix_send, 2, mix_all.at[t])
    sent(mix_send, 3, mix_part.at[pl.ds(0, 2)])
    sent(mix_send, 4, mix_stage)

    @pl.when(rim_source)
    def _():
        rim_to(0).wait_send()

    @pl.when(rim_mine)
    def _():
        rim_to(1).wait_send()
        rim_to(2).wait_send()

    @pl.when(rim_relay)
    def _():
        rim_to(2).wait_send()

    @pl.when(end)
    def _():
        sent(ag_send, 0, tokens.at[e])
        sent(coef_send, 0, coefs.at[e])
        d2_own().wait_send()
        sent(d2_send, 1, d2_half(w_d, t_x, g))
        sent(d2_send, 2, hid_far)

    @pl.when(mid)
    def _():
        sent(ag_send, 0, tokens.at[pl.ds(0, 2)])
        sent(ag_send, 1, tokens.at[pl.ds(0, 3)])
        sent(coef_send, 0, coefs.at[pl.ds(0, 2)])
        sent(coef_send, 1, coefs.at[pl.ds(0, 3)])
        sent(d2_send, 3, w_d2.at[0])
        sent(d2_send, 4, w_d2.at[pl.ds(0, 2)])
        sent(rs_send, 1, rs_stage.at[2])

    for k in range(4, CHUNKS):
        lag(CHUNKS + k)
        final(k)
    sent(rs_send, 0, rs_stage.at[pl.ds(0, 2)])


def fused(*args):
    (mixer_tokens, _, in_weight, group_weight, _, out_weight, _, _, route_ids, _, gate_weight, _, _) = args
    rows, width = mixer_tokens.shape
    group_width = in_weight.shape[1]
    ff = gate_weight.shape[2]
    blocks = lax.axis_size("ep")
    parts = lax.axis_size("tp")
    half = rows // HALVES
    bf16, f32 = jnp.bfloat16, jnp.float32
    vmem = pltpu.VMEM
    dma = pltpu.SemaphoreType.DMA
    anyspace = pl.BlockSpec(memory_space=pl.ANY)
    local_spec = pl.BlockSpec(memory_space=pltpu.VMEM)
    args = list(args)
    for i in (8, 9):
        args[i] = args[i].T
    small = (1, 4, 7, 8, 9)
    scratch = [
        vmem((rows, width), bf16),
        vmem((rows, width), bf16),
        vmem((width, group_width), bf16),
        vmem((group_width, group_width), bf16),
        vmem((group_width, width), bf16),
        vmem((parts, 2, width, ff), bf16),
        vmem((parts, ff, width), bf16),
        vmem((blocks, rows, width), bf16),
        vmem((blocks, 8, rows), f32),
        vmem((blocks, rows, rows), f32),
        vmem((blocks, 2, rows, 2 * ff), bf16),
        vmem((blocks, rows, width), f32),
        vmem((4, rows, width), bf16),
        vmem((3, rows, width), bf16),
        vmem((parts, rows, width), bf16),
        vmem((rows * (parts + 1), group_width), bf16),
        vmem((parts, rows, width), bf16),
        vmem((2, rows, width), bf16),
        vmem((rows, width), bf16),
        vmem((rows, width), bf16),
        vmem((WINDOW_MAX, width), bf16),
        vmem((parts, ff, width), bf16),
        vmem((2, rows, 2 * ff), bf16),
        dma((10,)),
    ]
    for count in (2, X_PIECES, 2, Y_PIECES, 2, 2, 2, 2, 2, 2, 2, 8, 2, 4, 2, 4 * CHUNKS, 5, 8, 3, 3, 5, 6):
        scratch.append(dma((count,)))
    shape = vmem((rows, width), bf16)
    return pl.pallas_call(
        fused_kernel,
        out_shape=(shape, shape),
        in_specs=[local_spec if i in small else anyspace for i in range(len(args))],
        out_specs=(local_spec, local_spec),
        scratch_shapes=scratch,
        compiler_params=pltpu.CompilerParams(
            collective_id=0, has_side_effects=True, vmem_limit_bytes=60 << 20
        ),
        name="fused",
    )(*args)


def fits(mesh):
    sizes = dict(mesh.shape)
    return sizes["grp"] == 2 and sizes["ep"] == 4 and sizes["tp"] == 4


def solution(mesh):
    placed = (
        P(("grp", "ep", "tp"), None),
        P(),
        P(None, "tp"),
        P("tp", None, None),
        P("tp"),
        P("tp", None),
        P(("grp", "ep", "tp"), None),
        P(),
        P(("grp", "ep", "tp"), None),
        P(("grp", "ep", "tp"), None),
        P("ep", None, "tp"),
        P("ep", None, "tp"),
        P("ep", "tp", None),
    )
    return jax.shard_map(
        fused if fits(mesh) else local,
        mesh=mesh,
        in_specs=placed,
        out_specs=(P(("grp", "ep", "tp"), None), P(("grp", "ep", "tp"), None)),
        check_vma=False,
    )
```

```python
import jax
import jax.numpy as jnp
from jax import lax
from jax.experimental import pallas as pl
from jax.experimental.pallas import tpu as pltpu
from jax.sharding import PartitionSpec as P

WINDOW_MAX = 16


def shifted(value, axis, by):
    devices = lax.axis_size(axis)
    pairs = [(i, i + by) for i in range(devices) if 0 <= i + by < devices]
    return lax.ppermute(value, axis, pairs)


def turned(value, axis, by):
    devices = lax.axis_size(axis)
    if by % devices == 0:
        return value
    return lax.ppermute(value, axis, [(i, (i + by) % devices) for i in range(devices)])


def rms_rows(rows, gain):
    values = rows.astype(jnp.float32)
    scaled = values * lax.rsqrt(jnp.mean(values * values, axis=-1, keepdims=True) + 1e-06)
    return (scaled * gain.astype(jnp.float32)).astype(jnp.bfloat16)


def expert_hidden(rows, w_gate, w_up):
    gate = jnp.dot(rows, w_gate, preferred_element_type=jnp.float32)
    upper = jnp.dot(rows, w_up, preferred_element_type=jnp.float32)
    return (jax.nn.silu(gate) * upper).astype(jnp.bfloat16)


def local(
    mixer_tokens,
    mixer_gain,
    in_weight,
    group_weight,
    channel_scale,
    out_weight,
    expert_tokens,
    expert_gain,
    route_ids,
    route_weights,
    gate_weight,
    up_weight,
    down_weight,
):
    normed = rms_rows(mixer_tokens, mixer_gain)
    expert_in = rms_rows(expert_tokens, expert_gain)
    shares = route_weights / jnp.sum(route_weights, axis=1, keepdims=True)
    rows_here, top_k = route_ids.shape
    width = expert_in.shape[1]
    n_experts = lax.axis_size("ep") * gate_weight.shape[0]
    capacity = 4 * rows_here // n_experts
    dense = capacity >= rows_here
    parts_tp = lax.axis_size("tp")
    if dense:
        both = lax.all_gather(jnp.concatenate([normed, expert_in], axis=0), "tp", axis=0, tiled=True)
        both = both.reshape(parts_tp, 2, rows_here, width)
        every = both[:, 0].reshape(parts_tp * rows_here, width)
        own = both[:, 1].reshape(parts_tp * rows_here, width)
    else:
        every = lax.all_gather(normed, "tp", axis=0, tiled=True)
    pooled_in = jnp.dot(
        every,
        in_weight,
        preferred_element_type=jnp.float32,
    ).astype(jnp.bfloat16)
    block_rows = pooled_in.shape[0]
    rim_rows = shifted(pooled_in[block_rows - WINDOW_MAX :], "ep", 1)
    values = pooled_in.astype(jnp.float32)
    extended = jnp.concatenate([rim_rows.astype(jnp.float32), values], axis=0)
    window = jnp.left_shift(jnp.int32(2), lax.axis_index("tp"))
    sums = extended
    span = 1
    total = jnp.zeros_like(values)
    for level in range(WINDOW_MAX.bit_length() - 1):
        sums = sums[span:] + sums[:-span]
        span = span * 2
        total = total + jnp.where(window == span, sums[sums.shape[0] - block_rows :], 0.0)
    positions = lax.axis_index("ep") * block_rows + lax.iota(jnp.int32, block_rows) + 1
    counts = jnp.minimum(positions, window).astype(jnp.float32)
    pooled = (total / counts[:, None] - values).astype(jnp.bfloat16)
    grouped = (
        jnp.dot(pooled, group_weight[0], preferred_element_type=jnp.float32)
        * channel_scale.astype(jnp.float32)
    ).astype(jnp.bfloat16)
    mixed_part = jnp.dot(grouped, out_weight, preferred_element_type=jnp.float32).astype(
        jnp.bfloat16
    )
    if dense:
        experts = jnp.arange(n_experts, dtype=jnp.int32)
        named = (route_ids[:, :, None] == experts[None, None, :]).astype(jnp.float32)
        coefs = jnp.sum(named * shares[:, :, None], axis=1)
        coefs = lax.all_gather(coefs, ("ep", "tp"), axis=0, tiled=True)
        blocks = lax.axis_size("ep")
        here = lax.axis_index("ep")
        mine = (experts == here).astype(jnp.float32)
        coef = jnp.sum(coefs * mine[None, :], axis=1).reshape(blocks, parts_tp, rows_here)
        order = list(range(1, blocks))

        def scale_of(k):
            return lax.dynamic_index_in_dim(coef, lax.rem(here - k + blocks, blocks), 0, False)

        def expert_part(rows, scale):
            hidden = expert_hidden(rows, gate_weight[0], up_weight[0])
            part = jnp.dot(hidden, down_weight[0], preferred_element_type=jnp.float32)
            return (part * scale.reshape(-1)[:, None]).astype(jnp.bfloat16)

        moved = jnp.concatenate([turned(expert_in, "ep", k) for k in order], axis=0)
        moved, own = lax.optimization_barrier((moved, own))
        own_part = expert_part(own, scale_of(0))
        others = lax.all_gather(moved, "tp", axis=0, tiled=True)
        part = expert_part(others, jnp.stack([scale_of(k) for k in order], axis=1))
        back = lax.psum_scatter(part, "tp", scatter_dimension=0, tiled=True)
        back = back.reshape(blocks - 1, rows_here, width)
        pair = jnp.stack(
            [value.reshape(parts_tp, rows_here, width) for value in (mixed_part, own_part)], axis=1
        ).reshape(2 * parts_tp * rows_here, width)
        pair = lax.psum_scatter(pair, "tp", scatter_dimension=0, tiled=True)
        total = pair[rows_here:].astype(jnp.float32)
        for i, k in enumerate(order):
            total = total + turned(back[i], "ep", -k).astype(jnp.float32)
        return (pair[:rows_here], total.astype(jnp.bfloat16))
    mixed_tokens = lax.psum_scatter(mixed_part, "tp", scatter_dimension=0, tiled=True)
    flat_ids = route_ids.reshape(rows_here * top_k)
    one_hot = (flat_ids[:, None] == jnp.arange(n_experts, dtype=jnp.int32)[None, :]).astype(
        jnp.int32
    )
    before = jnp.cumsum(one_hot, axis=0) - one_hot
    slots = jnp.sum(before * one_hot, axis=1)
    targets = flat_ids * capacity + slots
    placement = (
        targets.reshape(rows_here, top_k)[None, :, :]
        == jnp.arange(n_experts * capacity, dtype=jnp.int32)[:, None, None]
    )
    dispatch = jnp.any(placement, axis=2).astype(jnp.bfloat16)
    outgoing = jnp.dot(dispatch, expert_in, preferred_element_type=jnp.float32).astype(jnp.bfloat16)
    outgoing = outgoing.reshape(n_experts, capacity, width)
    arrived = lax.all_to_all(outgoing, "ep", split_axis=0, concat_axis=0, tiled=True)
    sources, held, _ = arrived.shape
    flat = arrived.reshape(sources * held, width)
    hidden = expert_hidden(
        lax.all_gather(flat, "tp", axis=0, tiled=True), gate_weight[0], up_weight[0]
    )
    rows = hidden
    summed = lax.psum_scatter(
        jnp.dot(rows, down_weight[0], preferred_element_type=jnp.float32).astype(jnp.bfloat16),
        "tp",
        scatter_dimension=0,
        tiled=True,
    ).astype(jnp.float32)
    expert_out = lax.all_to_all(
        summed.reshape(sources, held, width).astype(jnp.bfloat16),
        "ep",
        split_axis=0,
        concat_axis=0,
        tiled=True,
    ).astype(jnp.float32)
    flat_out = expert_out.reshape(n_experts * capacity, width)
    picked = jnp.take(flat_out, targets, axis=0).reshape(rows_here, top_k, width)
    expert_mix = jnp.sum(picked * shares[:, :, None], axis=1).astype(jnp.bfloat16)
    return (mixed_tokens, expert_mix)


MESH = pl.DeviceIdType.MESH
GU_CUTS = (0, 1, 2, 4, 6, 8, 10, 12, 14, 16)
PIECES_GU = len(GU_CUTS) - 1
D_CUTS = (0, 2, 4, 5, 6, 8)
PIECES = PIECES_GU + len(D_CUTS) - 1
X_PIECES = PIECES + 1
Y_PIECES = PIECES - 1
WINDOW = 5
LAG = 3
HALVES = 2
CHUNKS = 8


def fused_kernel(
    mixer_tokens,
    mixer_gain,
    in_weight,
    group_weight,
    channel_scale,
    out_weight,
    expert_tokens,
    expert_gain,
    route_ids,
    route_weights,
    gate_weight,
    up_weight,
    down_weight,
    mixed_out,
    expert_out,
    mix_raw,
    exp_raw,
    w_in,
    w_group,
    w_out,
    w_gu,
    w_d,
    tokens,
    coefs,
    scales,
    hid,
    acc,
    rs_in,
    rs_stage,
    mix_all,
    pooled_in,
    mix_part,
    mix_pair,
    mix_stage,
    mix_far,
    rim_rows,
    w_d2,
    hid_far,
    load_sem,
    x_send,
    x_recv,
    y_send,
    y_recv,
    own_send,
    own_recv,
    fx_send,
    fx_recv,
    fy_send,
    fy_recv,
    ag_send,
    ag_recv,
    coef_send,
    coef_recv,
    rs_send,
    rs_recv,
    mix_send,
    mix_recv,
    rim_send,
    rim_recv,
    d2_send,
    d2_recv,
):
    f32, bf16 = jnp.float32, jnp.bfloat16
    rows, width = exp_raw.shape
    half_rows = rows // HALVES
    group_width = w_group.shape[0]
    ff_half = w_d.shape[1] // 2
    blocks = tokens.shape[0]
    parts = mix_all.shape[0]
    g = lax.axis_index("grp")
    e = lax.axis_index("ep")
    t = lax.axis_index("tp")
    x = t // 2
    c = t % 2
    t_c = 2 * x + 1 - c
    t_x = 2 * (1 - x) + c
    t_d = 2 * (1 - x) + 1 - c
    dev_c, dev_x, dev_y = (g, e, t_c), (g, e, t_x), (1 - g, e, t)
    hi = e // 2
    sign = 1 - 2 * hi
    last = blocks - 1

    def mirror(m):
        return hi * last + sign * m

    u = mirror(e)
    end = u == 0
    mid = u == 1
    far = (g, lax.rem(e + sign + blocks, blocks), t)
    near = (g, lax.rem(e - sign + blocks, blocks), t)
    third = mirror(1 - u)

    def rc(src, dst, send, recv, dev):
        return pltpu.make_async_remote_copy(
            src_ref=src, dst_ref=dst, send_sem=send, recv_sem=recv, device_id=dev, device_id_type=MESH
        )

    barrier = pltpu.get_barrier_semaphore()
    for dev in (dev_c, dev_x, dev_y):
        pl.semaphore_signal(barrier, inc=1, device_id=dev, device_id_type=MESH)

    @pl.when(e < last)
    def _():
        dev = (g, lax.rem(e + 1, blocks), t)
        pl.semaphore_signal(barrier, inc=1, device_id=dev, device_id_type=MESH)

    @pl.when(e > 0)
    def _():
        dev = (g, lax.rem(e - 1 + blocks, blocks), t)
        pl.semaphore_signal(barrier, inc=1, device_id=dev, device_id_type=MESH)

    def loads():
        out = []
        for h in range(2):
            hh = g if h == 0 else 1 - g
            lane = pl.multiple_of(hh * ff_half, ff_half)
            out.append((gate_weight.at[0, :, pl.ds(lane, ff_half)], w_gu.at[t, hh, :, pl.ds(0, ff_half)]))
            out.append((up_weight.at[0, :, pl.ds(lane, ff_half)], w_gu.at[t, hh, :, pl.ds(ff_half, ff_half)]))
            if h == 0:
                out.append((expert_tokens, exp_raw))
        out.append((down_weight.at[0], w_d.at[t]))
        out.append((mixer_tokens, mix_raw))
        out.append((in_weight, w_in))
        out.append((group_weight.at[0], w_group))
        out.append((out_weight, w_out))
        return [pltpu.make_async_copy(a, b, load_sem.at[i]) for i, (a, b) in enumerate(out)]

    local = loads()
    for copy in local[:3]:
        copy.start()
    def norm(raw, gain, dst, start, count):
        step = 64
        gain_row = gain[...].astype(f32).reshape(1, width)

        @pl.loop(0, count // step)
        def _(i):
            at = pl.ds(pl.multiple_of(start + i * step, step), step)
            values = raw[at, :].astype(f32)
            scaled = values * lax.rsqrt(jnp.mean(values * values, axis=-1, keepdims=True) + 1e-06)
            dst[at, :] = (scaled * gain_row).astype(bf16)

    ids = route_ids[...]
    weights = route_weights[...]
    shares = weights / jnp.sum(weights, axis=0, keepdims=True)
    numbers = lax.broadcasted_iota(jnp.int32, coefs.shape[1:], 0)
    coef = jnp.zeros(coefs.shape[1:], f32)
    for k in range(ids.shape[0]):
        coef = coef + jnp.where(ids[k : k + 1, :] == numbers, shares[k : k + 1, :], 0.0)
    coefs[e] = coef

    def d_cut(s):
        unit = ff_half // D_CUTS[-1]
        low, high = D_CUTS[s - PIECES_GU], D_CUTS[s - PIECES_GU + 1]
        return low * unit, (high - low) * unit

    def piece(q, h, s):
        if s < PIECES_GU:
            unit = width // GU_CUTS[-1]
            low, high = GU_CUTS[s], GU_CUTS[s + 1]
            return w_gu.at[q, h, pl.ds(low * unit, (high - low) * unit), :]
        start, n = d_cut(s)
        return w_d.at[q, pl.ds(pl.multiple_of(h * ff_half + start, 16), n), :]

    def x_piece(q, s):
        return piece(q, g, s) if s < PIECES else piece(q, 1 - g, PIECES - 1)

    def kind(s):
        return 0 if s < PIECES_GU else 1

    def send_x(s):
        p = x_piece(t, s)
        return rc(p, p, x_send.at[kind(s)], x_recv.at[s], dev_x)

    def got_x(s):
        p = x_piece(t_x, s)
        return rc(p, p, x_send.at[0], x_recv.at[s], dev_x)

    def send_y(s):
        p = piece(t_x, g, s)
        return rc(p, p, y_send.at[kind(s)], y_recv.at[s], dev_y)

    def got_y(s):
        p = piece(t_x, 1 - g, s)
        return rc(p, p, y_send.at[0], y_recv.at[s], dev_y)

    def send_fx(s):
        p = x_piece(t_x, s)
        return rc(p, p, fx_send.at[kind(s)], fx_recv.at[kind(s)], dev_c)

    def send_fy(s):
        p = piece(t_x, 1 - g, s)
        return rc(p, p, fy_send.at[kind(s)], fy_recv.at[kind(s)], dev_c)

    d_last = d_cut(PIECES - 1)
    x_rows, y_rows = ff_half + d_last[1], d_last[0]

    def all_gu(send, recv):
        return rc(w_gu.at[t, g], w_gu.at[t, g], send.at[0], recv.at[0], dev_c)

    def all_d(send, recv, count):
        p = w_d.at[t, pl.ds(0, count), :]
        return rc(p, p, send.at[1], recv.at[1], dev_c)

    def own_gu(q):
        return rc(w_gu.at[q], w_gu.at[q], own_send.at[0], own_recv.at[0], dev_c)

    def own_d(q):
        return rc(w_d.at[q], w_d.at[q], own_send.at[1], own_recv.at[1], dev_c)

    def chunk(home, j):
        return tokens.at[home, pl.ds(j * half_rows, half_rows), :]

    def ag_far(home, j, f):
        p = chunk(home, j)
        return rc(p, p, ag_send.at[0], ag_recv.at[f + 6 * (1 - u)], far)

    def ag_near(home, j, f):
        p = chunk(home, j)
        return rc(p, p, ag_send.at[1], ag_recv.at[f], near)

    def ag_got(home, j, f):
        p = chunk(home, j)
        return rc(p, p, ag_send.at[0], ag_recv.at[f], far)

    rim_source = (t == parts - 1) & (e < last)
    rim_mine = (t == parts - 1) & (e > 0)
    rim_relay = (t == parts // 2 - 1) & (e > 0)
    rim_last = (c == 0) & (e > 0)

    def rim_to(k):
        src = mix_all.at[t, pl.ds(rows - rim_rows.shape[0], rim_rows.shape[0]), :] if k == 0 else rim_rows
        dev = ((g, lax.rem(e + 1, blocks), t), dev_x, dev_c)[k]
        return rc(src, rim_rows, rim_send.at[k], rim_recv.at[k], dev)

    def coef_far(home, k):
        return rc(coefs.at[home], coefs.at[home], coef_send.at[0], coef_recv.at[k + 3 * (1 - u)], far)

    def coef_near(home, k):
        return rc(coefs.at[home], coefs.at[home], coef_send.at[1], coef_recv.at[k], near)

    def coef_got(home, k):
        return rc(coefs.at[home], coefs.at[home], coef_send.at[0], coef_recv.at[k], far)

    def d2_half(ref, q, h):
        return ref.at[q, pl.ds(pl.multiple_of(h * ff_half, ff_half), ff_half), :]

    def d2_piece(ref, s):
        start, n = d_cut(s)
        return ref.at[t_x, pl.ds(pl.multiple_of(g * ff_half + start, 16), n), :]

    def d2_own():
        return rc(d2_half(w_d, t, g), d2_half(w_d2, t, g), d2_send.at[0], d2_recv.at[0], far)

    def d2_relay(s):
        return rc(d2_piece(w_d, s), d2_piece(w_d2, s), d2_send.at[1], d2_recv.at[1], far)

    def d2_hid(xq):
        return rc(hid.at[third, xq], hid_far.at[xq], d2_send.at[2], d2_recv.at[2], far)

    def d2_y(k, mine):
        p = d2_half(w_d2, t if k == 0 else t_x, g if mine else 1 - g)
        return rc(p, p, d2_send.at[3], d2_recv.at[3 + k], dev_y)

    def d2_c(k):
        p = d2_half(w_d2, t if k % 2 == 0 else t_x, g if k < 2 else 1 - g)
        return rc(p, p, d2_send.at[4], d2_recv.at[5], dev_c)

    def d2_all(k, p):
        return rc(p, p, d2_send.at[k], d2_recv.at[min(k, 2) if k < 4 else 5], dev_c)

    def mix_x(q, j):
        p = mix_all.at[q, pl.ds(j * half_rows, half_rows), :]
        return rc(p, p, mix_send.at[0], mix_recv.at[j], dev_x)

    def mix_fwd(q, j):
        p = mix_all.at[q, pl.ds(j * half_rows, half_rows), :]
        return rc(p, p, mix_send.at[1], mix_recv.at[2], dev_c)

    def mix_own(q):
        return rc(mix_all.at[q], mix_all.at[q], mix_send.at[2], mix_recv.at[3], dev_c)

    local[0].wait()
    local[1].wait()
    @pl.when(end)
    def _():
        pl.semaphore_wait(barrier, 4)

    @pl.when(mid)
    def _():
        pl.semaphore_wait(barrier, 5)

    for s in range(WINDOW):
        send_x(s).start()
    for copy in local[3:]:
        copy.start()
    local[2].wait()
    norm(exp_raw, expert_gain, tokens.at[e], 0, rows)
    coef_far(e, 0).start()
    for j in range(HALVES):
        ag_far(e, j, j).start()

    @pl.when(mid)
    def _():
        coef_near(e, 0).start()
        for j in range(HALVES):
            ag_near(e, j, j).start()

    local[3].wait()
    local[4].wait()
    own_gu(t).start()
    local[5].wait()
    own_d(t).start()

    local[6].wait()
    norm(mix_raw, mixer_gain, mix_all.at[t], 0, rows)

    @pl.when(rim_source)
    def _():
        rim_to(0).start()

    @pl.when(end)
    def _():
        d2_own().start()

    mix_own(t).start()

    whole = pl.ds(0, rows)
    part_of = [pl.ds(j * half_rows, half_rows) for j in range(HALVES)]

    def hidden(home, xq, at=whole):
        @pl.loop(0, 4)
        def _(j):
            q = 2 * xq + j // 2
            h = j % 2
            both = jnp.dot(tokens[home, at, :], w_gu[q, h], preferred_element_type=f32)
            gate, upper = both[:, :ff_half], both[:, ff_half:]
            value = gate / (1.0 + jnp.exp(-gate)) * upper
            hid[home, xq, at, pl.ds(pl.multiple_of(j * ff_half, ff_half), ff_half)] = value.astype(bf16)

    col = 512

    def down(home, xq, first, at=whole):
        @pl.loop(0, width // col)
        def _(n):
            cols = pl.ds(pl.multiple_of(n * col, col), col)
            w = w_d[pl.ds(2 * xq, 2), :, cols].reshape(4 * ff_half, col)
            part = jnp.dot(hid[home, xq, at, :], w, preferred_element_type=f32)
            if first:
                acc[home, at, cols] = part
            else:
                scale = scales[home, at, :][:, :1]
                acc[home, at, cols] = (acc[home, at, cols] + part) * scale

    def pool_in(xq):
        @pl.loop(0, 2)
        def _(j):
            q = 2 * xq + j
            value = jnp.dot(mix_all[q], w_in[...], preferred_element_type=f32)
            pooled_in[pl.ds(pl.multiple_of(rows * (q + 1), rows), rows), :] = value.astype(bf16)

    def wait_fgu():
        all_gu(fx_send, fx_recv).wait_recv()
        all_gu(fy_send, fy_recv).wait_recv()

    def relay_y(s):
        got_y(s).wait_recv()
        send_fy(s).start()

    def gather(f):
        @pl.when(end)
        def _():
            home = mirror(1 + f // 2)
            ag_got(home, f % 2, f).wait_recv()
            if f % 2 == 0:
                coef_got(home, f // 2).wait_recv()

        if f < 4:

            @pl.when(mid)
            def _():
                home = mirror(2 + f // 2)
                ag_got(home, f % 2, f).wait_recv()
                ag_near(home, f % 2, f + 2).start()
                if f % 2 == 0:
                    coef_got(home, f // 2).wait_recv()
                    coef_near(home, f // 2 + 1).start()

        if f < 2:

            @pl.when(mid)
            def _():
                home = mirror(0)
                ag_got(home, f % 2, 6 + f).wait_recv()
                ag_far(home, f % 2, 2 + f).start()
                if f % 2 == 0:
                    coef_got(home, 3).wait_recv()
                    coef_far(home, 1).start()

    def scale_of(home):
        scales[home] = jnp.transpose(jnp.broadcast_to(coefs[home, pl.ds(e, 1), :], (rows, rows)))

    for s in range(X_PIECES):
        got_x(s).wait_recv()
        if s < Y_PIECES:
            send_y(s).start()
        send_fx(s).start()
        if PIECES_GU <= s < PIECES:

            @pl.when(end)
            def _():
                d2_relay(s).start()

        if s + WINDOW == X_PIECES:

            @pl.when(rim_mine)
            def _():
                rim_to(1).start()

        if s + WINDOW < X_PIECES:
            send_x(s + WINDOW).start()
        elif s + WINDOW < X_PIECES + HALVES:
            mix_x(t, s + WINDOW - X_PIECES).start()
        if s >= LAG:
            relay_y(s - LAG)
        if s in (3, 5, 7, 9, 11):
            gather(s // 2 - 1)
        if s == 3:
            own_gu(t_c).wait_recv()
            hidden(e, x)
        if s == 8:

            @pl.when(rim_mine)
            def _():
                rim_to(0).wait_recv()
                rim_to(2).start()

        if s == 4:
            own_d(t_c).wait_recv()
            down(e, x, True)
        if s == 5:
            pooled_in[pl.ds(0, rows), :] = jnp.zeros((rows, group_width), bf16)
        if s == 6:
            hidden(third, x)

            @pl.when(end)
            def _():
                d2_hid(x).start()

        if s == 7:

            @pl.when(mid)
            def _():
                down(third, x, True)

        if s == 8:
            mix_own(t_c).wait_recv()
            local[7].wait()
            pool_in(x)
        if s == 10:
            hidden(mirror(2), x)
            down(mirror(2), x, True)
        if s == 11:
            hidden(mirror(3), x, part_of[0])
        if s == 12:
            wait_fgu()
            hidden(third, 1 - x)

            @pl.when(end)
            def _():
                d2_hid(1 - x).start()

        if s == Y_PIECES:

            @pl.when(mid)
            def _():
                d2_own().wait_recv()
                d2_y(0, True).start()
                d2_c(0).start()

            hidden(mirror(3), 1 - x, part_of[0])
            down(mirror(3), x, True, part_of[0])
            scale_of(mirror(3))

    for s in range(X_PIECES - LAG, Y_PIECES):
        relay_y(s)
    all_d(fx_send, fx_recv, x_rows).wait_recv()
    all_d(fy_send, fy_recv, y_rows).wait_recv()

    def cut(k):
        slot, j = divmod(k, CHUNKS)
        return slot, pl.ds(j * (rows // CHUNKS), rows // CHUNKS)

    def rs_far(k):
        slot, at = cut(k)
        sem = k + 2 * CHUNKS * u
        return rc(rs_stage.at[slot, at, :], rs_in.at[slot + 2 * u, at, :], rs_send.at[0], rs_recv.at[sem], far)

    def rs_near(k):
        slot, at = cut(k)
        sem = 2 * CHUNKS + k
        return rc(rs_stage.at[2, at, :], rs_in.at[2, at, :], rs_send.at[1], rs_recv.at[sem], near)

    def rs_got(k, base):
        slot, at = cut(k)
        p = rs_in.at[slot + base, at, :]
        return rc(p, p, rs_send.at[0], rs_recv.at[k + base * CHUNKS], far)

    def first_send(home, first, count=CHUNKS):
        @pl.when(end)
        def _():
            for k in range(first, first + count):
                slot, at = cut(k)
                rs_stage[slot, at, :] = acc[home, at, :].astype(bf16)
                rs_far(k).start()

    def lead(k):
        @pl.when(mid)
        def _():
            rs_got(k, 0).wait_recv()
            slot, at = cut(k)
            rs_stage[slot, at, :] = (acc[mirror(3 - slot), at, :] + rs_in[slot, at, :].astype(f32)).astype(bf16)
            rs_far(k).start()

    def lag(k):
        @pl.when(mid)
        def _():
            rs_got(k, 2).wait_recv()
            if k < CHUNKS:
                slot, at = cut(k)
                rs_stage[2, at, :] = (acc[mirror(0), at, :] + rs_in[2, at, :].astype(f32)).astype(bf16)
                rs_near(k).start()

    local[8].wait()
    local[9].wait()
    window = 2 + 2 * jnp.minimum(t, 1) + 4 * (t // 2) + 8 * (t // 3)

    def mix_down(j):
        q = (2 * (1 - x) if j < 2 else 2 * x) + (1 - c if j % 2 == 0 else c)
        start = pl.multiple_of(q * rows, rows)
        seg = pooled_in[pl.ds(start, 2 * rows), :]
        i = lax.broadcasted_iota(jnp.int32, (rows, 2 * rows), 0) + rows
        k = lax.broadcasted_iota(jnp.int32, (rows, 2 * rows), 1)
        band = jnp.where((k <= i) & (k > i - window), 1.0, 0.0).astype(bf16)
        sums = jnp.dot(band, seg, preferred_element_type=f32)
        place = lax.broadcasted_iota(jnp.int32, (rows, 1), 0) + (e * blocks + q) * rows + 1
        counts = jnp.minimum(place, window).astype(f32)
        pooled = (sums / counts - seg[rows:, :].astype(f32)).astype(bf16)
        grouped = jnp.dot(pooled, w_group[...], preferred_element_type=f32)
        grouped = (grouped * channel_scale[...].astype(f32).reshape(1, group_width)).astype(bf16)

        @pl.loop(0, width // col)
        def _(n):
            at = pl.ds(pl.multiple_of(n * col, col), col)
            mix_part[j, :, at] = jnp.dot(grouped, w_out[:, at], preferred_element_type=f32).astype(bf16)

    def pair_to(j):
        return rc(mix_part.at[2 * j], mix_pair.at[j], mix_send.at[3], mix_recv.at[4 + j], dev_c)

    def cross(j):
        at = pl.ds(j * half_rows, half_rows)
        return rc(mix_stage.at[at, :], mix_far.at[at, :], mix_send.at[4], mix_recv.at[6 + j], dev_x)

    def mix_relay(j):
        mix_x(t_x, j).wait_recv()
        mix_fwd(t_x, j).start()

    def final(k):
        @pl.when(mid)
        def _():
            _, at = cut(CHUNKS + k)
            expert_out[at, :] = (acc[e, at, :] + rs_in[3, at, :].astype(f32)).astype(bf16)

        @pl.when(end)
        def _():
            _, at = cut(k)
            rs_got(k, 2).wait_recv()
            expert_out[at, :] = (acc[e, at, :] + rs_in[2, at, :].astype(f32)).astype(bf16)

    down(mirror(3), 1 - x, False, part_of[0])
    first_send(mirror(3), 0, CHUNKS // 2)
    gather(5)
    for home in (mirror(2), third, e):
        scale_of(home)
    hidden(mirror(3), x, part_of[1])
    hidden(mirror(3), 1 - x, part_of[1])
    lead(0)
    down(mirror(3), x, True, part_of[1])
    lead(1)
    down(mirror(3), 1 - x, False, part_of[1])
    first_send(mirror(3), CHUNKS // 2, CHUNKS // 2)

    @pl.when(mid)
    def _():
        d2_all(1, d2_half(w_d2, t_x, g)).wait_recv()
        d2_y(1, True).start()
        d2_c(1).start()

    mix_relay(0)
    lead(2)
    hidden(mirror(2), 1 - x)

    @pl.when(rim_relay)
    def _():
        rim_to(1).wait_recv()
        rim_to(2).start()

    lead(3)
    down(mirror(2), 1 - x, False)
    first_send(mirror(2), CHUNKS)
    lead(4)
    mix_relay(1)

    @pl.when(mid)
    def _():
        down(third, 1 - x, False)

    mix_all_in = rc(mix_all.at[t_d], mix_all.at[t_d], mix_send.at[1], mix_recv.at[2], dev_c)
    mix_all_in.wait_recv()
    pool_in(1 - x)

    @pl.when(rim_last)
    def _():
        rim_to(2).wait_recv()

    @pl.when(e > 0)
    def _():
        value = jnp.dot(rim_rows[...], w_in[...], preferred_element_type=f32)
        pooled_in[pl.ds(rows - rim_rows.shape[0], rim_rows.shape[0]), :] = value.astype(bf16)

    lead(5)
    lag(0)
    mix_down(0)
    pair_to(0).start()
    lead(6)
    lag(1)
    mix_down(1)
    lead(7)
    lag(2)
    pair_to(0).wait_recv()
    for j in range(HALVES):
        at = pl.ds(j * half_rows, half_rows)
        mix_stage[at, :] = (mix_part[1, at, :].astype(f32) + mix_pair[0, at, :].astype(f32)).astype(bf16)
        cross(j).start()
    lead(8)
    lag(3)

    hidden(e, 1 - x)
    lead(9)
    lag(4)

    @pl.when(mid)
    def _():
        d2_y(0, False).wait_recv()
        d2_c(2).start()

    down(e, 1 - x, False)
    lead(10)
    lag(5)
    lead(11)
    lag(6)
    mix_down(2)
    pair_to(1).start()
    lead(12)
    lag(7)
    lead(13)
    mix_down(3)
    lead(14)

    @pl.when(mid)
    def _():
        d2_y(1, False).wait_recv()
        d2_c(3).start()

    lead(15)

    @pl.when(mid)
    def _():
        scales[0] = jnp.transpose(jnp.broadcast_to(coefs[e, pl.ds(mirror(0), 1), :], (rows, rows)))
        d2_all(2, hid_far).wait_recv()
        d2_all(4, w_d2.at[pl.ds(0, 2)]).wait_recv()

        @pl.loop(0, width // col)
        def _(n):
            at = pl.ds(pl.multiple_of(n * col, col), col)
            part = acc[e, :, at]
            scale = scales[0][:, :1]
            for xq in range(2):
                w = w_d2[pl.ds(2 * xq, 2), :, at].reshape(4 * ff_half, col)
                part = part + jnp.dot(hid_far[xq], w, preferred_element_type=f32) * scale
            acc[e, :, at] = part

    for k in range(4):
        lag(CHUNKS + k)
        final(k)
    pair_to(1).wait_recv()
    for j in range(HALVES):
        at = pl.ds(j * half_rows, half_rows)
        cross(j).wait_recv()
        mixed_out[at, :] = (
            mix_part[3, at, :].astype(f32) + mix_pair[1, at, :].astype(f32) + mix_far[at, :].astype(f32)
        ).astype(bf16)

    all_gu(x_send, fx_recv).wait_send()
    all_d(x_send, fx_recv, x_rows).wait_send()
    all_gu(y_send, fx_recv).wait_send()
    all_d(y_send, fx_recv, y_rows).wait_send()
    all_gu(fx_send, fx_recv).wait_send()
    all_d(fx_send, fx_recv, x_rows).wait_send()
    all_gu(fy_send, fx_recv).wait_send()
    all_d(fy_send, fx_recv, y_rows).wait_send()
    own_gu(t).wait_send()
    own_d(t).wait_send()

    def sent(sems, k, p):
        rc(p, p, sems.at[k], mix_recv.at[0], dev_c).wait_send()

    sent(mix_send, 0, mix_all.at[t])
    sent(mix_send, 1, mix_all.at[t])
    sent(mix_send, 2, mix_all.at[t])
    sent(mix_send, 3, mix_part.at[pl.ds(0, 2)])
    sent(mix_send, 4, mix_stage)

    @pl.when(rim_source)
    def _():
        rim_to(0).wait_send()

    @pl.when(rim_mine)
    def _():
        rim_to(1).wait_send()
        rim_to(2).wait_send()

    @pl.when(rim_relay)
    def _():
        rim_to(2).wait_send()

    @pl.when(end)
    def _():
        sent(ag_send, 0, tokens.at[e])
        sent(coef_send, 0, coefs.at[e])
        d2_own().wait_send()
        sent(d2_send, 1, d2_half(w_d, t_x, g))
        sent(d2_send, 2, hid_far)

    @pl.when(mid)
    def _():
        sent(ag_send, 0, tokens.at[pl.ds(0, 2)])
        sent(ag_send, 1, tokens.at[pl.ds(0, 3)])
        sent(coef_send, 0, coefs.at[pl.ds(0, 2)])
        sent(coef_send, 1, coefs.at[pl.ds(0, 3)])
        sent(d2_send, 3, w_d2.at[0])
        sent(d2_send, 4, w_d2.at[pl.ds(0, 2)])
        sent(rs_send, 1, rs_stage.at[2])

    for k in range(4, CHUNKS):
        lag(CHUNKS + k)
        final(k)
    sent(rs_send, 0, rs_stage.at[pl.ds(0, 2)])


def fused(*args):
    (mixer_tokens, _, in_weight, group_weight, _, out_weight, _, _, route_ids, _, gate_weight, _, _) = args
    rows, width = mixer_tokens.shape
    group_width = in_weight.shape[1]
    ff = gate_weight.shape[2]
    blocks = lax.axis_size("ep")
    parts = lax.axis_size("tp")
    half = rows // HALVES
    bf16, f32 = jnp.bfloat16, jnp.float32
    vmem = pltpu.VMEM
    dma = pltpu.SemaphoreType.DMA
    anyspace = pl.BlockSpec(memory_space=pl.ANY)
    local_spec = pl.BlockSpec(memory_space=pltpu.VMEM)
    args = list(args)
    for i in (8, 9):
        args[i] = args[i].T
    small = (1, 4, 7, 8, 9)
    scratch = [
        vmem((rows, width), bf16),
        vmem((rows, width), bf16),
        vmem((width, group_width), bf16),
        vmem((group_width, group_width), bf16),
        vmem((group_width, width), bf16),
        vmem((parts, 2, width, ff), bf16),
        vmem((parts, ff, width), bf16),
        vmem((blocks, rows, width), bf16),
        vmem((blocks, 8, rows), f32),
        vmem((blocks, rows, rows), f32),
        vmem((blocks, 2, rows, 2 * ff), bf16),
        vmem((blocks, rows, width), f32),
        vmem((4, rows, width), bf16),
        vmem((3, rows, width), bf16),
        vmem((parts, rows, width), bf16),
        vmem((rows * (parts + 1), group_width), bf16),
        vmem((parts, rows, width), bf16),
        vmem((2, rows, width), bf16),
        vmem((rows, width), bf16),
        vmem((rows, width), bf16),
        vmem((WINDOW_MAX, width), bf16),
        vmem((parts, ff, width), bf16),
        vmem((2, rows, 2 * ff), bf16),
        dma((10,)),
    ]
    for count in (2, X_PIECES, 2, Y_PIECES, 2, 2, 2, 2, 2, 2, 2, 8, 2, 4, 2, 4 * CHUNKS, 5, 8, 3, 3, 5, 6):
        scratch.append(dma((count,)))
    shape = vmem((rows, width), bf16)
    return pl.pallas_call(
        fused_kernel,
        out_shape=(shape, shape),
        in_specs=[local_spec if i in small else anyspace for i in range(len(args))],
        out_specs=(local_spec, local_spec),
        scratch_shapes=scratch,
        compiler_params=pltpu.CompilerParams(
            collective_id=0, has_side_effects=True, vmem_limit_bytes=60 << 20
        ),
        name="fused",
    )(*args)


def fits(mesh):
    sizes = dict(mesh.shape)
    return sizes["grp"] == 2 and sizes["ep"] == 4 and sizes["tp"] == 4


def solution(mesh):
    placed = (
        P(("grp", "ep", "tp"), None),
        P(),
        P(None, "tp"),
        P("tp", None, None),
        P("tp"),
        P("tp", None),
        P(("grp", "ep", "tp"), None),
        P(),
        P(("grp", "ep", "tp"), None),
        P(("grp", "ep", "tp"), None),
        P("ep", None, "tp"),
        P("ep", None, "tp"),
        P("ep", "tp", None),
    )
    return jax.shard_map(
        fused if fits(mesh) else local,
        mesh=mesh,
        in_specs=placed,
        out_specs=(P(("grp", "ep", "tp"), None), P(("grp", "ep", "tp"), None)),
        check_vma=False,
    )
```
